32 devices in a mesh: grp: 2 (over y), ep: 8 (over z, core), tp: 2 (over x).
Axes of the slice: x: 2, y: 2, z: 4, core: 2. Of those that a mesh axis runs over, the one named last changes fastest.
Arguments:
- tokens: bfloat16 [3072, 2048], P(('grp', 'ep')), parts along dimension 0, may hold values from -6 to 6
- norm_gain: float32 [2048], replicated, may hold values from 0.1 to 1.9
- w_gate: bfloat16 [8, 2048, 1024], P('ep', None, 'tp'), may hold values from -0.3125 to 0.3125
- w_up: bfloat16 [8, 2048, 1024], P('ep', None, 'tp'), may hold values from -0.3125 to 0.3125
- w_down: bfloat16 [8, 1024, 2048], P('ep', 'tp'), may hold values from -0.09375 to 0.09375
- expert_ids: int32 [3072, 4], P(('grp', 'ep')), parts along dimension 0, may hold values from 0 to 7, all different within a row; in each aligned block of 192 rows (0 to 191, 192 to 383, ...) at most 128 rows name the same one
- gate_weights: float32 [3072, 4], P(('grp', 'ep')), parts along dimension 0, may hold values from 0.1 to 1
Outputs:
- mixed: bfloat16 [3072, 2048], P(('grp', 'ep'), 'tp'), parts along dimension 0
The draws below stay inside these ranges and needn't reach their ends.
There are 2 independent parts, one for each index of `grp`. The reference program is written for one: setup_inputs(seed, part) draws one part's arguments, and reference() takes and returns one part's arrays. A program takes and returns all parts, laid end to end along the dimension named above; an argument that names none is the same for every part. Nothing has to cross between parts.
Inputs may be any that keep to these rules, and one draw needn't show every extreme that they name: `expert_ids`: each row names 4 different experts; among the rows of one index of ep, no expert is named by more than 128 rows, a bound that some block reaches.
All inputs are finite; a program needn't handle non-finite values.
Results may differ from the reference program's by a relative error of at most 0.012.
Values may be sent and summed in bfloat16 or wider, within the bound.
A program may use at most 64 MiB of HBM per device.

```python
import math
import jax
import jax.numpy as jnp
import numpy as np
from jax import lax

D = 2048
FF = 1024
TOP_K = 4
TOK_DEV = 192
EXPERTS = 8
CAP = 128
TOKENS = 1536
N_EP = 8
N_TP = 2


def shard_levels(own_key, shape, cuts, least, largest):
    def one(dim, parts):
        steps = jax.random.uniform(jax.random.fold_in(jax.random.fold_in(own_key, 6), dim), (parts,), jnp.float32, least / len(cuts), largest / len(cuts))
        return jnp.repeat(jnp.exp(steps), shape[dim] // parts).reshape((-1,) + (1,) * (len(shape) - dim - 1))

    factor_of = one(*cuts[0])
    for cut in cuts[1:]:
        factor_of = factor_of * one(*cut)
    return factor_of


def deal_out(own_key, own, number, rows, count, top, most, skew):
    order = jax.random.permutation(own_key, count)
    heavy_load, ordinary = portions_of(count, rows * top, most, skew, True), portions_of(count, rows * top, most, skew, False)
    places = jnp.arange(count)

    def named(lengths, offset_by):
        used = int((lengths > 0).sum())
        fixed = max(1, used // 4)
        moved = fixed + (places - fixed + offset_by * (used - fixed)) % max(1, count - fixed)
        return jnp.zeros((count,), jnp.int32).at[order[jnp.where(places < fixed, places, moved)]].set(jnp.asarray(lengths, jnp.int32))

    lengths = jnp.where(number % 4 == 0, named(heavy_load, number // 4), named(ordinary, number - number // 4 - 1))
    mixed = jax.random.permutation(jax.random.fold_in(own, 3), count)
    donor, taker = mixed[0:count // 2 * 2:2], mixed[1:count // 2 * 2:2]
    room = jnp.minimum(lengths[donor] - 1, most - lengths[taker]) // 2
    room = jnp.where((donor == order[0]) | (taker == order[0]) | (lengths[taker] == 0), 0, jnp.maximum(room, 0))
    moved = jax.random.randint(jax.random.fold_in(own, 4), (count // 2,), 0, 1 << 20) % (room + 1)
    lengths = lengths.at[donor].add(-moved).at[taker].add(moved)
    items = jnp.searchsorted(jnp.cumsum(lengths), jnp.arange(rows * top), side="right").astype(jnp.int32)
    table = items.reshape(top, rows).T
    table = table[jax.random.permutation(jax.random.fold_in(own, 1), rows)]
    offset_by = jax.random.randint(jax.random.fold_in(own, 2), (rows, 1), 0, top)
    return jnp.take_along_axis(table, (jnp.arange(top)[None, :] + offset_by) % top, axis=1)


def portions_of(amount, total, bound, skew, full):
    portions = [(1 << 20) // math.isqrt(standing ** skew) + 1 for standing in range(1, amount + 1)]
    largest = bound if full else min(bound, max(-(-total // amount), total * portions[0] // sum(portions)))
    least = 1 if total - largest >= amount - 1 else 0
    holding, spare = [largest] + [least] * (amount - 1), total - largest - least * (amount - 1)
    while spare > 0:
        candidates = [i for i in range(1, amount) if holding[i] < largest] or [i for i in range(1, amount) if holding[i] < bound]
        whole, left = sum([portions[i] for i in candidates]), spare
        for i in candidates:
            addition = min(bound - holding[i], max(1, left * portions[i] // whole), spare)
            holding[i] = holding[i] + addition
            spare = spare - addition
    return np.array(holding)


def normal_values(key, shape, spread, limit, pieces=(), kind=jnp.bfloat16):
    drawn = spread * jax.random.normal(key, shape, jnp.float32)
    if pieces:
        drawn = drawn * shard_levels(key, shape, pieces, -0.22, 0.18)
    return jnp.clip(drawn, -limit, limit).astype(kind)


def setup_inputs(seed: int = 0, part: int = 0) -> dict:
    key_list = jax.random.split(jax.random.key(seed), 8)
    part_keys = jax.random.split(jax.random.fold_in(key_list[7], part), 8)
    tokens = normal_values(part_keys[0], (TOKENS, D), 1.0, 6.0, ((0, 8),))
    norm_gain = jnp.clip(1.0 + 0.18 * jax.random.normal(key_list[1], (D,), jnp.float32), 0.1, 1.9)
    w_gate = normal_values(key_list[2], (EXPERTS, D, FF), (D // 6) ** -0.5, 0.3125, ((0, 8), (2, 2)))
    w_up = normal_values(key_list[3], (EXPERTS, D, FF), (D // 6) ** -0.5, 0.3125, ((0, 8), (2, 2)))
    w_down = normal_values(key_list[4], (EXPERTS, FF, D), (FF * 4) ** -0.5, 0.09375, ((0, 8), (1, 2)))
    expert_ids_keys = jax.random.split(jax.random.fold_in(part_keys[5], 1), TOKENS // TOK_DEV)
    expert_ids_turns = jax.random.permutation(jax.random.fold_in(part_keys[5], 3), TOKENS // TOK_DEV)
    expert_ids = jax.vmap(lambda own, number: deal_out(jax.random.fold_in(part_keys[5], 2), own, number, TOK_DEV, EXPERTS, TOP_K, CAP, 1))(expert_ids_keys, expert_ids_turns).reshape((TOKENS, TOP_K))
    gate_weights = jnp.clip(0.1 + 0.9 * jax.random.uniform(part_keys[6], (TOKENS, TOP_K), jnp.float32) ** shard_levels(part_keys[6], (TOKENS, TOP_K), ((0, 8),), -0.2, 0.2), 0.1, 1.0)
    return {"tokens": tokens, "norm_gain": norm_gain, "w_gate": w_gate, "w_up": w_up, "w_down": w_down, "expert_ids": expert_ids, "gate_weights": gate_weights}


epsilon = 1e-06
clamp_limit = 7.0
swish_alpha = 1.702

def rms_norm(tokens, norm_gain):
    widened = tokens.astype(jnp.float32)
    scaled = widened * lax.rsqrt(lax.optimization_barrier(jnp.mean(widened * widened, axis=-1, keepdims=True)) + epsilon)
    return (scaled * norm_gain).astype(jnp.bfloat16)

def reference(tokens, norm_gain, w_gate, w_up, w_down, expert_ids, gate_weights):
    normed = rms_norm(tokens, norm_gain)
    src_ids = expert_ids.reshape(N_EP, TOK_DEV * TOP_K).astype(jnp.int32)
    onehot = (src_ids[:, :, None] == jnp.arange(EXPERTS, dtype=jnp.int32)[None, None, :]).astype(jnp.int32)
    before = jnp.cumsum(onehot, axis=1) - onehot
    slot_index = lax.optimization_barrier(jnp.sum(before * onehot, axis=2)).astype(jnp.int32)
    source = jnp.arange(N_EP, dtype=jnp.int32)[:, None]
    row_index = (src_ids * (N_EP * CAP) + source * CAP + slot_index).astype(jnp.int32)
    owner_tok = (source * TOK_DEV + jnp.arange(TOK_DEV * TOP_K, dtype=jnp.int32)[None, :] // TOP_K).astype(jnp.int32)
    slot_table = jnp.full((EXPERTS * N_EP * CAP,), TOKENS, jnp.int32)
    slot_table = slot_table.at[row_index.reshape(-1)].set(owner_tok.reshape(-1)).reshape(EXPERTS, N_EP * CAP)
    padded = jnp.concatenate([normed, jnp.zeros((1, D), jnp.bfloat16)], axis=0)

    def expert_fn(packed):
        slot_rows, gate_mat, up_mat, down_mat = packed
        expert_rows = padded[slot_rows]
        gate_pre = jnp.dot(expert_rows, gate_mat, preferred_element_type=jnp.float32)
        up_pre = jnp.dot(expert_rows, up_mat, preferred_element_type=jnp.float32)
        gated = jnp.minimum(gate_pre, clamp_limit)
        linear = jnp.clip(up_pre, -clamp_limit, clamp_limit)
        activated = (gated * jax.nn.sigmoid(swish_alpha * gated) * (linear + 1.0)).astype(jnp.bfloat16)
        act_blocks = activated.reshape(-1, N_TP, FF // N_TP).astype(jnp.float32)
        down_blocks = down_mat.reshape(N_TP, FF // N_TP, D).astype(jnp.float32)
        partial_value = jnp.einsum('rtf,tfd->rtd', act_blocks, down_blocks).astype(jnp.bfloat16)
        partial_value = lax.optimization_barrier(partial_value)
        return lax.optimization_barrier(jnp.sum(partial_value.astype(jnp.float32), axis=1)).astype(jnp.bfloat16)
    expert_out = lax.map(expert_fn, (slot_table, w_gate, w_up, w_down))
    picked = expert_out.reshape(EXPERTS * N_EP * CAP, D)[row_index.reshape(-1)]
    picked = picked.reshape(TOKENS, TOP_K, D).astype(jnp.float32)
    return lax.optimization_barrier(jnp.sum(picked * gate_weights[:, :, None], axis=1)).astype(jnp.bfloat16)
```

```python
import functools

import jax
import jax.numpy as jnp
from jax import lax
from jax.experimental import pallas as pl
from jax.experimental.pallas import tpu as pltpu
from jax.sharding import PartitionSpec as P

epsilon = 1e-06
clamp_limit = 7.0
swish_alpha = 1.702


def rms_norm(tokens, norm_gain):
    widened = tokens.astype(jnp.float32)
    scaled = widened * lax.rsqrt(jnp.mean(widened * widened, axis=-1, keepdims=True) + epsilon)
    return (scaled * norm_gain).astype(jnp.bfloat16)


def body(tokens, norm_gain, w_gate, w_up, w_down, expert_ids, gate_weights):
    tok_rows, model_width = tokens.shape
    top_count = expert_ids.shape[1]
    ep_count = lax.axis_size("ep")
    local_experts = w_gate.shape[0]
    experts_all = local_experts * ep_count
    capacity = min(tok_rows, tok_rows * top_count * 4 // (3 * experts_all))
    normed = rms_norm(tokens, norm_gain)
    flat_ids = expert_ids.reshape(-1)
    onehot = (flat_ids[:, None] == jnp.arange(experts_all, dtype=jnp.int32)[None, :]).astype(
        jnp.int32
    )
    before = jnp.cumsum(onehot, axis=0) - onehot
    slot_index = jnp.sum(before * onehot, axis=1)
    dest_row = flat_ids * capacity + slot_index
    owner_tok = jnp.arange(tok_rows * top_count, dtype=jnp.int32) // top_count
    slot_table = (
        jnp.full((experts_all * capacity,), tok_rows, jnp.int32).at[dest_row].set(owner_tok)
    )
    padded = jnp.concatenate([normed, jnp.zeros((1, model_width), jnp.bfloat16)], axis=0)
    send_buffer = padded[slot_table].reshape(experts_all, capacity, model_width)
    received = lax.all_to_all(send_buffer, "ep", split_axis=0, concat_axis=0, tiled=True)
    expert_rows = received.reshape(ep_count, local_experts, capacity, model_width)
    gate_pre = jnp.einsum("sjcd,jdf->sjcf", expert_rows, w_gate, preferred_element_type=jnp.float32)
    up_pre = jnp.einsum("sjcd,jdf->sjcf", expert_rows, w_up, preferred_element_type=jnp.float32)
    gated = jnp.minimum(gate_pre, clamp_limit)
    linear = jnp.clip(up_pre, -clamp_limit, clamp_limit)
    activated = (gated * jax.nn.sigmoid(swish_alpha * gated) * (linear + 1.0)).astype(jnp.bfloat16)
    partial_value = jnp.einsum(
        "sjcf,jfd->sjcd", activated, w_down, preferred_element_type=jnp.float32
    ).astype(jnp.bfloat16)
    summed = (
        lax.psum_scatter(partial_value, "tp", scatter_dimension=3, tiled=True)
        .astype(jnp.float32)
        .astype(jnp.bfloat16)
    )
    returned = lax.all_to_all(summed, "ep", split_axis=0, concat_axis=0, tiled=True)
    returned = returned.reshape(experts_all * capacity, returned.shape[3])
    picked = returned[dest_row].reshape(tok_rows, top_count, returned.shape[1]).astype(jnp.float32)
    return jnp.sum(picked * gate_weights[:, :, None], axis=1).astype(jnp.bfloat16)


MESH = pl.DeviceIdType.MESH
CORES = 2
PIECES = 3
SPLIT = 3
HIDDEN_TILE = 256
COLUMN_TILE = 512


def fused_kernel(
    chips,
    tok_ref,
    gain_ref,
    ids_ref,
    gates_ref,
    wg_hbm,
    wu_hbm,
    wd_hbm,
    out_ref,
    rows_all,
    codes,
    wg,
    wu,
    wd,
    act,
    kept,
    part,
    merge_out,
    merge_in,
    side_out,
    side_in,
    far_out,
    far_in,
    agg_in,
    weight_sem,
    pair_sem,
    code_send,
    code_recv,
    z_send,
    z_recv,
    x_send,
    x_recv,
    merge_sem,
    side_sem,
    far_send,
    far_recv,
):
    ep, tp = lax.axis_index("ep"), lax.axis_index("tp")
    z, core = lax.div(ep, CORES), lax.rem(ep, CORES)
    rows, width = tok_ref.shape
    half = rows // 2
    piece = half // PIECES
    out_width = width // 2
    hidden = wg.shape[2]
    last = chips - 1
    partner = {"ep": z * CORES + 1 - core}
    peer = {"tp": 1 - tp}
    onward = ({"ep": (z + 1) * CORES + core}, {"ep": (z - 1) * CORES + core})
    has_next = (z < last, z > 0)

    sources = (wg_hbm.at[0], wu_hbm.at[0], wd_hbm.at[0])
    loads = [
        pltpu.make_async_copy(source, target, weight_sem.at[i])
        for i, (source, target) in enumerate(
            zip(sources, (wg.at[0], wu.at[0], wd.at[pl.ds(0, hidden)]))
        )
    ]
    for load in loads:
        load.start()

    barrier = pltpu.get_barrier_semaphore()
    for target in (partner, peer):
        pl.semaphore_signal(barrier, inc=1, device_id=target, device_id_type=MESH)
    for side in range(2):

        @pl.when(has_next[side])
        def _(side=side):
            pl.semaphore_signal(barrier, inc=1, device_id=onward[side], device_id_type=MESH)

    def block_at(side, distance):
        return z - distance if side == 0 else z + distance

    def valid(side, distance):
        return z >= distance if side == 0 else z + distance < chips

    def remote(source, target, send, recv, device):
        return pltpu.make_async_remote_copy(
            src_ref=source,
            dst_ref=target,
            send_sem=send,
            recv_sem=recv,
            device_id=device,
            device_id_type=MESH,
        )

    def chip_of(block):
        return {"ep": block * CORES + core}

    gives = [
        remote(source, target, pair_sem.at[0, i], pair_sem.at[1, i], partner)
        for i, (source, target) in enumerate(
            zip(sources, (wg.at[1], wu.at[1], wd.at[pl.ds(hidden, hidden)]))
        )
    ]

    def normed(start):
        span = pl.ds(pl.multiple_of(start, 16), half)
        widened = tok_ref[span].astype(jnp.float32)
        scaled = widened * lax.rsqrt(jnp.mean(widened * widened, axis=-1, keepdims=True) + epsilon)
        rows_all[z, span] = (scaled * gain_ref[...]).astype(jnp.bfloat16)

    normed(tp * half)
    line = lax.broadcasted_iota(jnp.int32, codes.shape[1:], 0)
    gate = jnp.zeros(codes.shape[1:], jnp.float32)
    for k in range(ids_ref.shape[0]):
        gate = gate + jnp.where(line == ids_ref[k : k + 1, :], gates_ref[k : k + 1, :], 0.0)
    codes[z] = gate

    neighbours = 2 + jnp.where(z > 0, 1, 0) + jnp.where(z < last, 1, 0)
    pl.semaphore_wait(barrier, neighbours)

    def rows_of(block, which, q):
        start = pl.multiple_of(which * half + q * piece, 16)
        return rows_all.at[block, pl.ds(start, piece), :]

    def z_copy(side, distance, q):
        ref = rows_of(block_at(side, distance), tp, q)
        return remote(
            ref, ref, z_send.at[side, distance, q], z_recv.at[side, distance, q], onward[side]
        )

    def z_arrival(side, distance, q):
        ref = rows_of(block_at(side, distance), tp, q)
        return remote(
            ref,
            ref,
            z_send.at[side, distance - 1, q],
            z_recv.at[side, distance - 1, q],
            onward[side],
        )

    def code_copy(side, distance, hop):
        ref = codes.at[block_at(side, distance)]
        return remote(ref, ref, code_send.at[side, hop], code_recv.at[side, hop], onward[side])

    def x_copy(side, distance, q, which):
        ref = rows_of(block_at(side, distance), which, q)
        return remote(
            ref, ref, x_send.at[side, distance - 1, q], x_recv.at[side, distance - 1, q], peer
        )

    for q in range(PIECES):
        for side in range(2):

            @pl.when(has_next[side])
            def _(side=side, q=q):
                z_copy(side, 0, q).start()
                if q == 0:
                    code_copy(side, 0, 0).start()

    for give in gives:
        give.start()
    normed((1 - tp) * half)

    def gather_z(distance, pieces):
        for q in pieces:
            for side in range(2):

                @pl.when(valid(side, distance))
                def _(side=side, q=q):
                    z_arrival(side, distance, q).wait_recv()
                    if q == 0:
                        code_copy(side, distance, distance - 1).wait_recv()
                    if distance < last:

                        @pl.when(has_next[side])
                        def _():
                            z_copy(side, distance, q).start()
                            if q == 0:
                                code_copy(side, distance, distance).start()

                    x_copy(side, distance, q, tp).start()

    def gather_x(distance):
        for q in range(PIECES):
            for side in range(2):

                @pl.when(valid(side, distance))
                def _(side=side, q=q):
                    x_copy(side, distance, q, 1 - tp).wait_recv()

    theirs = pl.multiple_of((1 - tp) * out_width, 128)
    mine = pl.multiple_of(tp * out_width, 128)

    def span_of(q):
        return pl.ds(q * (rows // SPLIT), rows // SPLIT)

    def activate(block, slot):
        turned = jnp.transpose(codes[block])
        lane = lax.broadcasted_iota(jnp.int32, turned.shape, 1)
        owner = ep if slot == 0 else z * CORES + 1 - core
        weight = jnp.sum(jnp.where(lane == owner, turned, 0.0), axis=1, keepdims=True)[:rows]
        held = rows_all[block]
        for start in range(0, hidden, HIDDEN_TILE):
            columns = slice(start, start + HIDDEN_TILE)
            gate_pre = jnp.dot(held, wg[slot, :, columns], preferred_element_type=jnp.float32)
            up_pre = jnp.dot(held, wu[slot, :, columns], preferred_element_type=jnp.float32)
            gated = jnp.minimum(gate_pre, clamp_limit)
            linear = jnp.clip(up_pre, -clamp_limit, clamp_limit)
            value = gated * jax.nn.sigmoid(swish_alpha * gated) * (linear + 1.0) * weight
            act[:, slot * hidden + start : slot * hidden + start + HIDDEN_TILE] = value.astype(
                jnp.bfloat16
            )

    def project(start):
        return jnp.dot(
            act[...], wd[:, pl.ds(start, COLUMN_TILE)], preferred_element_type=jnp.float32
        )

    def merge_copy(side, other, q, block):
        return remote(
            merge_out.at[side, span_of(q)],
            merge_in.at[other, span_of(q)],
            merge_sem.at[0, side, q],
            merge_sem.at[1, other, q],
            chip_of(block),
        )

    def side_copy(block, q):
        return remote(
            side_out.at[block, span_of(q)],
            side_in.at[block, span_of(q)],
            side_sem.at[0, block, q],
            side_sem.at[1, block, q],
            peer,
        )

    def far_copy(side, distance, q):
        dest = block_at(side, distance)
        sender = far_send.at[side, distance - 2, q]
        if distance == 2:
            target, receiver = far_in.at[1 - side, span_of(q)], far_recv.at[1 - side, 0, q]
            device = chip_of(dest)
        else:
            target = agg_in.at[side, distance - 3, span_of(q)]
            receiver = far_recv.at[side, distance - 2, q]
            device = onward[1 - side]
        return remote(far_out.at[dest, span_of(q)], target, sender, receiver, device)

    def far_arrival(side, q):
        return remote(
            far_in.at[side, span_of(q)],
            far_in.at[side, span_of(q)],
            far_send.at[side, 0, q],
            far_recv.at[side, 0, q],
            peer,
        )

    def agg_arrival(side, distance, q):
        ref = agg_in.at[side, distance - 2, span_of(q)]
        return remote(
            ref, ref, far_send.at[side, 0, q], far_recv.at[side, distance - 1, q], peer
        )

    def experts_at(distance):
        def one(side, carry):
            block = z + distance * (2 * side - 1)

            @pl.when((block >= 0) & (block < chips))
            def _():
                activate(block, 0)
                activate(block, 1)
                if distance == 1:
                    for start in range(0, width, COLUMN_TILE):
                        merge_out[side, :, start : start + COLUMN_TILE] = project(start).astype(
                            jnp.bfloat16
                        )
                    for q in range(SPLIT):
                        merge_copy(side, 1 - side, q, block).start()
                else:
                    for start in range(0, out_width, COLUMN_TILE):
                        side_out[block, :, start : start + COLUMN_TILE] = project(
                            pl.multiple_of(theirs + start, 128)
                        ).astype(jnp.bfloat16)
                    for q in range(SPLIT):
                        side_copy(block, q).start()
                    for start in range(0, out_width, COLUMN_TILE):
                        part[block, :, start : start + COLUMN_TILE] = project(
                            pl.multiple_of(mine + start, 128)
                        )

            return carry

        lax.fori_loop(0, 2, one, 0)

    def far_sum(side, distance, more):
        block = block_at(side, distance)
        for q in range(SPLIT):
            span = span_of(q)
            side_copy(block, q).wait_recv()
            total = part[block, span] + side_in[block, span].astype(jnp.float32)
            if more:
                agg_arrival(side, distance, q).wait_recv()
                total = total + agg_in[side, distance - 2, span].astype(jnp.float32)
            far_out[block, span] = total.astype(jnp.bfloat16)
            far_copy(side, distance, q).start()

    def far_sums(distance, more):
        for side in range(2):
            through = has_next[side]

            @pl.when(valid(side, distance) & (through if more else jnp.logical_not(through)))
            def _(side=side):
                far_sum(side, distance, more)

    def own_exchange():
        for q in range(SPLIT):
            span = span_of(q)
            for side in range(2):

                @pl.when(valid(side, 1))
                def _(side=side, q=q):
                    merge_copy(1 - side, side, q, block_at(side, 1)).wait_recv()
                    kept[span] = kept[span] + merge_in[side, span].astype(jnp.float32)

            side_out[z, span] = kept[span, pl.ds(theirs, out_width)].astype(jnp.bfloat16)
            side_copy(z, q).start()

    def finish():
        for q in range(SPLIT):
            span = span_of(q)
            side_copy(z, q).wait_recv()
            part[z, span] = kept[span, pl.ds(mine, out_width)] + side_in[z, span].astype(
                jnp.float32
            )
            if chips > 2:
                for side in range(2):

                    @pl.when(valid(side, 2))
                    def _(side=side, q=q):
                        far_arrival(side, q).wait_recv()
                        part[z, span] = part[z, span] + far_in[side, span].astype(jnp.float32)

            out_ref[span] = part[z, span].astype(jnp.bfloat16)

    for load in loads:
        load.wait()
    activate(z, 0)
    gather_z(1, range(PIECES - 1))
    for give in gives[:2]:
        give.wait_recv()
    activate(z, 1)
    gather_z(1, range(PIECES - 1, PIECES))
    gives[2].wait_recv()
    for start in range(0, width, COLUMN_TILE):
        kept[:, start : start + COLUMN_TILE] = project(start)
    if last >= 2:
        gather_z(2, range(PIECES))
    for turn in range(1, last + 1):
        gather_x(turn)
        experts_at(turn)
        if turn + 2 <= last:
            gather_z(turn + 2, range(PIECES))
    for distance in range(2, last):
        far_sums(distance, False)
    own_exchange()
    if last >= 2:
        far_sums(last, False)
    for distance in range(last - 1, 1, -1):
        far_sums(distance, True)
    finish()

    for give in gives:
        give.wait_send()
    for q in range(PIECES):
        for side in range(2):
            for distance in range(chips):
                if distance < last:

                    @pl.when(valid(side, distance) & has_next[side])
                    def _(side=side, distance=distance, q=q):
                        z_copy(side, distance, q).wait_send()
                        if q == 0:
                            code_copy(side, distance, distance).wait_send()

                if distance > 0:

                    @pl.when(valid(side, distance))
                    def _(side=side, distance=distance, q=q):
                        x_copy(side, distance, q, tp).wait_send()

    for q in range(SPLIT):
        side_copy(z, q).wait_send()
        for side in range(2):
            for distance in range(1, chips):

                @pl.when(valid(side, distance))
                def _(side=side, distance=distance, q=q):
                    if distance == 1:
                        merge_copy(side, 1 - side, q, block_at(side, 1)).wait_send()
                    else:
                        side_copy(block_at(side, distance), q).wait_send()
                        far_copy(side, distance, q).wait_send()


def fused(tokens, norm_gain, w_gate, w_up, w_down, expert_ids, gate_weights):
    rows, width = tokens.shape
    chips = lax.axis_size("ep") // CORES
    experts_all = chips * CORES
    hidden = w_gate.shape[2]
    out_width = width // 2
    last = chips - 1
    hops = max(last - 1, 1)
    lanes = -rows % 128
    vmem = pl.BlockSpec(memory_space=pltpu.VMEM)
    anywhere = pl.BlockSpec(memory_space=pl.ANY)
    dma = pltpu.SemaphoreType.DMA
    ids = jnp.pad(expert_ids.T, ((0, 0), (0, lanes)), constant_values=-1)
    gates = jnp.pad(gate_weights.T, ((0, 0), (0, lanes)))
    return pl.pallas_call(
        functools.partial(fused_kernel, chips),
        out_shape=jax.ShapeDtypeStruct((rows, out_width), jnp.bfloat16),
        in_specs=[vmem] * 4 + [anywhere] * 3,
        out_specs=vmem,
        scratch_shapes=[
            pltpu.VMEM((chips, rows, width), jnp.bfloat16),
            pltpu.VMEM((chips, experts_all + -experts_all % 8, rows + lanes), jnp.float32),
            pltpu.VMEM((CORES, width, hidden), jnp.bfloat16),
            pltpu.VMEM((CORES, width, hidden), jnp.bfloat16),
            pltpu.VMEM((CORES * hidden, width), jnp.bfloat16),
            pltpu.VMEM((rows, CORES * hidden), jnp.bfloat16),
            pltpu.VMEM((rows, width), jnp.float32),
            pltpu.VMEM((chips, rows, out_width), jnp.float32),
            pltpu.VMEM((2, rows, width), jnp.bfloat16),
            pltpu.VMEM((2, rows, width), jnp.bfloat16),
            pltpu.VMEM((chips, rows, out_width), jnp.bfloat16),
            pltpu.VMEM((chips, rows, out_width), jnp.bfloat16),
            pltpu.VMEM((chips, rows, out_width), jnp.bfloat16),
            pltpu.VMEM((2, rows, out_width), jnp.bfloat16),
            pltpu.VMEM((2, hops, rows, out_width), jnp.bfloat16),
            dma((3,)),
            dma((2, 3)),
            dma((2, last)),
            dma((2, last)),
            dma((2, last, PIECES)),
            dma((2, last, PIECES)),
            dma((2, last, PIECES)),
            dma((2, last, PIECES)),
            dma((2, 2, SPLIT)),
            dma((2, chips, SPLIT)),
            dma((2, hops, SPLIT)),
            dma((2, hops + 1, SPLIT)),
        ],
        compiler_params=pltpu.CompilerParams(collective_id=0, has_side_effects=True),
    )(tokens, norm_gain[None, :], ids, gates, w_gate, w_up, w_down)


def step(mesh, *arrays):
    tokens, norm_gain, w_gate, w_up, w_down, expert_ids, gate_weights = arrays
    ep_count, tp_count = mesh.shape["ep"], mesh.shape["tp"]
    rows, top_count = expert_ids.shape
    experts_all = ep_count * w_gate.shape[0]
    capacity = min(rows, rows * top_count * 4 // (3 * experts_all))
    dense = (
        w_gate.shape[0] == 1
        and tp_count == 2
        and ep_count % CORES == 0
        and ep_count > CORES
        and rows <= 2 * capacity
        and rows % (32 * PIECES) == 0
        and rows % (16 * SPLIT) == 0
    )
    return fused(*arrays) if dense else body(*arrays)


def solution(mesh):
    placed = (
        P(("grp", "ep"), None),
        P(),
        P("ep", None, "tp"),
        P("ep", None, "tp"),
        P("ep", "tp", None),
        P(("grp", "ep"), None),
        P(("grp", "ep"), None),
    )
    return jax.shard_map(
        functools.partial(step, mesh), mesh=mesh, in_specs=placed, out_specs=P(("grp", "ep"), "tp"), check_vma=False
    )
```

```python
import functools

import jax
import jax.numpy as jnp
from jax import lax
from jax.experimental import pallas as pl
from jax.experimental.pallas import tpu as pltpu
from jax.sharding import PartitionSpec as P

epsilon = 1e-06
clamp_limit = 7.0
swish_alpha = 1.702


def rms_norm(tokens, norm_gain):
    widened = tokens.astype(jnp.float32)
    scaled = widened * lax.rsqrt(jnp.mean(widened * widened, axis=-1, keepdims=True) + epsilon)
    return (scaled * norm_gain).astype(jnp.bfloat16)


def body(tokens, norm_gain, w_gate, w_up, w_down, expert_ids, gate_weights):
    tok_rows, model_width = tokens.shape
    top_count = expert_ids.shape[1]
    ep_count = lax.axis_size("ep")
    local_experts = w_gate.shape[0]
    experts_all = local_experts * ep_count
    capacity = min(tok_rows, tok_rows * top_count * 4 // (3 * experts_all))
    normed = rms_norm(tokens, norm_gain)
    flat_ids = expert_ids.reshape(-1)
    onehot = (flat_ids[:, None] == jnp.arange(experts_all, dtype=jnp.int32)[None, :]).astype(
        jnp.int32
    )
    before = jnp.cumsum(onehot, axis=0) - onehot
    slot_index = jnp.sum(before * onehot, axis=1)
    dest_row = flat_ids * capacity + slot_index
    owner_tok = jnp.arange(tok_rows * top_count, dtype=jnp.int32) // top_count
    slot_table = (
        jnp.full((experts_all * capacity,), tok_rows, jnp.int32).at[dest_row].set(owner_tok)
    )
    padded = jnp.concatenate([normed, jnp.zeros((1, model_width), jnp.bfloat16)], axis=0)
    send_buffer = padded[slot_table].reshape(experts_all, capacity, model_width)
    received = lax.all_to_all(send_buffer, "ep", split_axis=0, concat_axis=0, tiled=True)
    expert_rows = received.reshape(ep_count, local_experts, capacity, model_width)
    gate_pre = jnp.einsum("sjcd,jdf->sjcf", expert_rows, w_gate, preferred_element_type=jnp.float32)
    up_pre = jnp.einsum("sjcd,jdf->sjcf", expert_rows, w_up, preferred_element_type=jnp.float32)
    gated = jnp.minimum(gate_pre, clamp_limit)
    linear = jnp.clip(up_pre, -clamp_limit, clamp_limit)
    activated = (gated * jax.nn.sigmoid(swish_alpha * gated) * (linear + 1.0)).astype(jnp.bfloat16)
    partial_value = jnp.einsum(
        "sjcf,jfd->sjcd", activated, w_down, preferred_element_type=jnp.float32
    ).astype(jnp.bfloat16)
    summed = (
        lax.psum_scatter(partial_value, "tp", scatter_dimension=3, tiled=True)
        .astype(jnp.float32)
        .astype(jnp.bfloat16)
    )
    returned = lax.all_to_all(summed, "ep", split_axis=0, concat_axis=0, tiled=True)
    returned = returned.reshape(experts_all * capacity, returned.shape[3])
    picked = returned[dest_row].reshape(tok_rows, top_count, returned.shape[1]).astype(jnp.float32)
    return jnp.sum(picked * gate_weights[:, :, None], axis=1).astype(jnp.bfloat16)


MESH = pl.DeviceIdType.MESH
CORES = 2
PIECES = 6
SPLIT = 3
HIDDEN_TILE = 256
COLUMN_TILE = 512


def fused_kernel(
    chips,
    tok_hbm,
    gain_hbm,
    ids_hbm,
    gates_hbm,
    wg_hbm,
    wu_hbm,
    wd_hbm,
    out_ref,
    tok_ref,
    gain_ref,
    ids_ref,
    gates_ref,
    rows_all,
    codes,
    wg,
    wu,
    wd,
    act,
    kept,
    part,
    merge_out,
    merge_in,
    side_out,
    side_in,
    far_out,
    far_in,
    agg_in,
    input_sem,
    weight_sem,
    pair_sem,
    code_send,
    code_recv,
    z_send,
    z_recv,
    x_send,
    x_recv,
    merge_sem,
    side_sem,
    far_send,
    far_recv,
):
    ep, tp = lax.axis_index("ep"), lax.axis_index("tp")
    z, core = lax.div(ep, CORES), lax.rem(ep, CORES)
    rows, width = tok_hbm.shape
    half = rows // 2
    piece = half // PIECES
    out_width = width // 2
    hidden = wg.shape[2]
    last = chips - 1
    partner = {"ep": z * CORES + 1 - core}
    peer = {"tp": 1 - tp}
    onward = ({"ep": (z + 1) * CORES + core}, {"ep": (z - 1) * CORES + core})
    has_next = (z < last, z > 0)

    def half_of(which):
        return pl.ds(pl.multiple_of(which * half, 16), half)

    small = [
        pltpu.make_async_copy(source, target, input_sem.at[i])
        for i, (source, target) in enumerate(
            (
                (gain_hbm, gain_ref),
                (ids_hbm, ids_ref),
                (gates_hbm, gates_ref),
                (tok_hbm.at[half_of(tp)], tok_ref.at[half_of(tp)]),
                (tok_hbm.at[half_of(1 - tp)], tok_ref.at[half_of(1 - tp)]),
            )
        )
    ]
    sources = (wg_hbm.at[0], wu_hbm.at[0], wd_hbm.at[0])
    loads = [
        pltpu.make_async_copy(source, target, weight_sem.at[i])
        for i, (source, target) in enumerate(
            zip(sources, (wg.at[0], wu.at[0], wd.at[pl.ds(0, hidden)]))
        )
    ]

    barrier = pltpu.get_barrier_semaphore()
    for target in (partner, peer):
        pl.semaphore_signal(barrier, inc=1, device_id=target, device_id_type=MESH)
    for side in range(2):

        @pl.when(has_next[side])
        def _(side=side):
            pl.semaphore_signal(barrier, inc=1, device_id=onward[side], device_id_type=MESH)

    for load in small + loads:
        load.start()

    def block_at(side, distance):
        return z - distance if side == 0 else z + distance

    def valid(side, distance):
        return z >= distance if side == 0 else z + distance < chips

    def remote(source, target, send, recv, device):
        return pltpu.make_async_remote_copy(
            src_ref=source,
            dst_ref=target,
            send_sem=send,
            recv_sem=recv,
            device_id=device,
            device_id_type=MESH,
        )

    def chip_of(block):
        return {"ep": block * CORES + core}

    gives = [
        remote(source, target, pair_sem.at[0, i], pair_sem.at[1, i], partner)
        for i, (source, target) in enumerate(
            zip(sources, (wg.at[1], wu.at[1], wd.at[pl.ds(hidden, hidden)]))
        )
    ]

    def normed(which):
        span = half_of(which)
        widened = tok_ref[span].astype(jnp.float32)
        scaled = widened * lax.rsqrt(jnp.mean(widened * widened, axis=-1, keepdims=True) + epsilon)
        rows_all[z, span] = (scaled * gain_ref[...]).astype(jnp.bfloat16)

    for load in small[:4]:
        load.wait()
    normed(tp)
    line = lax.broadcasted_iota(jnp.int32, (codes.shape[1], rows), 0)
    gate = jnp.zeros(line.shape, jnp.float32)
    for k in range(ids_ref.shape[0]):
        gate = gate + jnp.where(line == ids_ref[k : k + 1, :], gates_ref[k : k + 1, :], 0.0)
    codes[z] = jnp.zeros(codes.shape[1:], jnp.float32)
    codes[z, :, :rows] = gate

    neighbours = 2 + jnp.where(z > 0, 1, 0) + jnp.where(z < last, 1, 0)
    pl.semaphore_wait(barrier, neighbours)

    def rows_of(block, which, q):
        start = pl.multiple_of(which * half + q * piece, 16)
        return rows_all.at[block, pl.ds(start, piece), :]

    def z_copy(side, distance, q):
        ref = rows_of(block_at(side, distance), tp, q)
        return remote(
            ref, ref, z_send.at[side, distance, q], z_recv.at[side, distance, q], onward[side]
        )

    def z_arrival(side, distance, q):
        ref = rows_of(block_at(side, distance), tp, q)
        return remote(
            ref,
            ref,
            z_send.at[side, distance - 1, q],
            z_recv.at[side, distance - 1, q],
            onward[side],
        )

    def code_copy(side, distance, hop):
        ref = codes.at[block_at(side, distance)]
        return remote(ref, ref, code_send.at[side, hop], code_recv.at[side, hop], onward[side])

    def x_copy(side, distance, q, which):
        ref = rows_of(block_at(side, distance), which, q)
        return remote(
            ref, ref, x_send.at[side, distance - 1, q], x_recv.at[side, distance - 1, q], peer
        )

    for q in range(PIECES):
        for side in range(2):

            @pl.when(has_next[side])
            def _(side=side, q=q):
                z_copy(side, 0, q).start()
                if q == 0:
                    code_copy(side, 0, 0).start()

    for give in gives:
        give.start()
    small[4].wait()
    normed(1 - tp)

    centre = jnp.where(2 * z < last, 1, 0)
    is_centre = (centre == 0, centre == 1)

    def gather_z(distance, pieces):
        if distance > last:
            return
        for q in pieces:
            for side in range(2):

                @pl.when(valid(side, distance))
                def _(side=side, q=q):
                    z_arrival(side, distance, q).wait_recv()
                    if q == 0:
                        code_copy(side, distance, distance - 1).wait_recv()
                    if distance < last:

                        @pl.when(has_next[side])
                        def _():
                            z_copy(side, distance, q).start()
                            if q == 0:
                                code_copy(side, distance, distance).start()

                    if distance > 1:
                        x_copy(side, distance, q, tp).start()
                    else:

                        @pl.when(is_centre[side])
                        def _():
                            x_copy(side, distance, q, tp).start()

    def outer_x():
        for side in range(2):

            @pl.when(valid(side, 1) & jnp.logical_not(is_centre[side]))
            def _(side=side):
                for q in range(PIECES):
                    x_copy(side, 1, q, tp).start()

    def in_turn(distance, turn):
        side = centre if turn == 0 else 1 - centre
        block = z + distance * (2 * side - 1)
        return side, block, (block >= 0) & (block < chips)

    def wait_x(distance, turn):
        side, block, there = in_turn(distance, turn)

        @pl.when(there)
        def _():
            for q in range(PIECES):
                ref = rows_of(block, 1 - tp, q)
                remote(
                    ref,
                    ref,
                    x_send.at[side, distance - 1, q],
                    x_recv.at[side, distance - 1, q],
                    peer,
                ).wait_recv()

    theirs = pl.multiple_of((1 - tp) * out_width, 128)
    mine = pl.multiple_of(tp * out_width, 128)

    def span_of(q):
        return pl.ds(q * (rows // SPLIT), rows // SPLIT)

    def activate(block, slot):
        turned = jnp.transpose(codes[block])
        lane = lax.broadcasted_iota(jnp.int32, turned.shape, 1)
        owner = ep if slot == 0 else z * CORES + 1 - core
        weight = jnp.sum(jnp.where(lane == owner, turned, 0.0), axis=1, keepdims=True)[:rows]
        held = rows_all[block]
        for start in range(0, hidden, HIDDEN_TILE):
            columns = slice(start, start + HIDDEN_TILE)
            gate_pre = jnp.dot(held, wg[slot, :, columns], preferred_element_type=jnp.float32)
            up_pre = jnp.dot(held, wu[slot, :, columns], preferred_element_type=jnp.float32)
            gated = jnp.minimum(gate_pre, clamp_limit)
            linear = jnp.clip(up_pre, -clamp_limit, clamp_limit)
            value = gated * jax.nn.sigmoid(swish_alpha * gated) * (linear + 1.0) * weight
            act[:, slot * hidden + start : slot * hidden + start + HIDDEN_TILE] = value.astype(
                jnp.bfloat16
            )

    def project(start):
        return jnp.dot(
            act[...], wd[:, pl.ds(start, COLUMN_TILE)], preferred_element_type=jnp.float32
        )

    def merge_copy(side, other, q, block):
        return remote(
            merge_out.at[side, span_of(q)],
            merge_in.at[other, span_of(q)],
            merge_sem.at[0, side, q],
            merge_sem.at[1, other, q],
            chip_of(block),
        )

    def side_copy(block, q):
        return remote(
            side_out.at[block, span_of(q)],
            side_in.at[block, span_of(q)],
            side_sem.at[0, block, q],
            side_sem.at[1, block, q],
            peer,
        )

    def far_copy(side, distance, q):
        dest = block_at(side, distance)
        sender = far_send.at[side, distance - 2, q]
        if distance == 2:
            target, receiver = far_in.at[1 - side, span_of(q)], far_recv.at[1 - side, 0, q]
            device = chip_of(dest)
        else:
            target = agg_in.at[side, distance - 3, span_of(q)]
            receiver = far_recv.at[side, distance - 2, q]
            device = onward[1 - side]
        return remote(far_out.at[dest, span_of(q)], target, sender, receiver, device)

    def far_arrival(side, q):
        return remote(
            far_in.at[side, span_of(q)],
            far_in.at[side, span_of(q)],
            far_send.at[side, 0, q],
            far_recv.at[side, 0, q],
            peer,
        )

    def agg_arrival(side, distance, q):
        ref = agg_in.at[side, distance - 2, span_of(q)]
        return remote(
            ref, ref, far_send.at[side, 0, q], far_recv.at[side, distance - 1, q], peer
        )

    def hidden_at(distance, turn, slot):
        side, block, there = in_turn(distance, turn)

        @pl.when(there)
        def _():
            activate(block, slot)

    def project_at(distance, turn):
        side, block, there = in_turn(distance, turn)

        @pl.when(there)
        def _():
            if distance == 1:
                for start in range(0, width, COLUMN_TILE):
                    merge_out[side, :, start : start + COLUMN_TILE] = project(start).astype(
                        jnp.bfloat16
                    )
                for q in range(SPLIT):
                    merge_copy(side, 1 - side, q, block).start()
            else:
                for start in range(0, out_width, COLUMN_TILE):
                    side_out[block, :, start : start + COLUMN_TILE] = project(
                        pl.multiple_of(theirs + start, 128)
                    ).astype(jnp.bfloat16)
                for start in range(0, out_width, COLUMN_TILE):
                    part[block, :, start : start + COLUMN_TILE] = project(
                        pl.multiple_of(mine + start, 128)
                    )

    def sides_at(distance, turn):
        side, block, there = in_turn(distance, turn)

        @pl.when(there)
        def _():
            for q in range(SPLIT):
                side_copy(block, q).start()

    def far_sum(side, distance, more):
        block = block_at(side, distance)
        for q in range(SPLIT):
            span = span_of(q)
            side_copy(block, q).wait_recv()
            total = part[block, span] + side_in[block, span].astype(jnp.float32)
            if more:
                agg_arrival(side, distance, q).wait_recv()
                total = total + agg_in[side, distance - 2, span].astype(jnp.float32)
            far_out[block, span] = total.astype(jnp.bfloat16)
            far_copy(side, distance, q).start()

    def far_sums(distance, more):
        for side in range(2):
            through = has_next[side]

            @pl.when(valid(side, distance) & (through if more else jnp.logical_not(through)))
            def _(side=side):
                far_sum(side, distance, more)

    def own_exchange():
        for q in range(SPLIT):
            span = span_of(q)
            for side in range(2):

                @pl.when(valid(side, 1))
                def _(side=side, q=q):
                    merge_copy(1 - side, side, q, block_at(side, 1)).wait_recv()
                    kept[span] = kept[span] + merge_in[side, span].astype(jnp.float32)

            side_out[z, span] = kept[span, pl.ds(theirs, out_width)].astype(jnp.bfloat16)
            side_copy(z, q).start()

    def finish():
        for q in range(SPLIT):
            span = span_of(q)
            side_copy(z, q).wait_recv()
            part[z, span] = kept[span, pl.ds(mine, out_width)] + side_in[z, span].astype(
                jnp.float32
            )
            if chips > 2:
                for side in range(2):

                    @pl.when(valid(side, 2))
                    def _(side=side, q=q):
                        far_arrival(side, q).wait_recv()
                        part[z, span] = part[z, span] + far_in[side, span].astype(jnp.float32)

            out_ref[span] = part[z, span].astype(jnp.bfloat16)

    third = PIECES // 3

    def pieces_of(distance, first, count):
        gather_z(distance, range(first * third, (first + count) * third))

    for load in loads[:2]:
        load.wait()
    gather_z(1, range(0, 1))
    activate(z, 0)
    gather_z(1, range(1, 2 * third))
    for give in gives[:2]:
        give.wait_recv()
    activate(z, 1)
    pieces_of(1, 2, 1)
    outer_x()
    loads[2].wait()
    gives[2].wait_recv()
    for start in range(0, width, COLUMN_TILE):
        kept[:, start : start + COLUMN_TILE] = project(start)
    for distance in range(1, chips):
        for turn in range(2):
            if 2 * distance + turn > chips and turn == 1:
                continue
            first = turn == 0
            if first:
                gather_z(distance + 1, range(0, 1))
            wait_x(distance, turn)
            hidden_at(distance, turn, 0)
            if first:
                gather_z(distance + 1, range(1, third))
            hidden_at(distance, turn, 1)
            if first:
                pieces_of(distance + 1, 1, 1)
            project_at(distance, turn)
            if first:
                pieces_of(distance + 1, 2, 1)
            if distance > 1:
                sides_at(distance, turn)
    for distance in range(2, last):
        far_sums(distance, False)
    own_exchange()
    if last >= 2:
        far_sums(last, False)
    for distance in range(last - 1, 1, -1):
        far_sums(distance, True)
    finish()

    for give in gives:
        give.wait_send()
    for q in range(PIECES):
        for side in range(2):
            for distance in range(chips):
                if distance < last:

                    @pl.when(valid(side, distance) & has_next[side])
                    def _(side=side, distance=distance, q=q):
                        z_copy(side, distance, q).wait_send()
                        if q == 0:
                            code_copy(side, distance, distance).wait_send()

                if distance > 0:

                    @pl.when(valid(side, distance))
                    def _(side=side, distance=distance, q=q):
                        x_copy(side, distance, q, tp).wait_send()

    for q in range(SPLIT):
        side_copy(z, q).wait_send()
        for side in range(2):
            for distance in range(1, chips):

                @pl.when(valid(side, distance))
                def _(side=side, distance=distance, q=q):
                    if distance == 1:
                        merge_copy(side, 1 - side, q, block_at(side, 1)).wait_send()
                    else:
                        side_copy(block_at(side, distance), q).wait_send()
                        far_copy(side, distance, q).wait_send()


def fused(tokens, norm_gain, w_gate, w_up, w_down, expert_ids, gate_weights):
    rows, width = tokens.shape
    top_count = expert_ids.shape[1]
    chips = lax.axis_size("ep") // CORES
    experts_all = chips * CORES
    hidden = w_gate.shape[2]
    out_width = width // 2
    last = chips - 1
    hops = max(last - 1, 1)
    lanes = -rows % 128
    vmem = pl.BlockSpec(memory_space=pltpu.VMEM)
    anywhere = pl.BlockSpec(memory_space=pl.ANY)
    dma = pltpu.SemaphoreType.DMA
    return pl.pallas_call(
        functools.partial(fused_kernel, chips),
        out_shape=jax.ShapeDtypeStruct((rows, out_width), jnp.bfloat16),
        in_specs=[anywhere] * 7,
        out_specs=vmem,
        scratch_shapes=[
            pltpu.VMEM((rows, width), jnp.bfloat16),
            pltpu.VMEM((1, width), jnp.float32),
            pltpu.VMEM((top_count, rows), jnp.int32),
            pltpu.VMEM((top_count, rows), jnp.float32),
            pltpu.VMEM((chips, rows, width), jnp.bfloat16),
            pltpu.VMEM((chips, experts_all + -experts_all % 8, rows + lanes), jnp.float32),
            pltpu.VMEM((CORES, width, hidden), jnp.bfloat16),
            pltpu.VMEM((CORES, width, hidden), jnp.bfloat16),
            pltpu.VMEM((CORES * hidden, width), jnp.bfloat16),
            pltpu.VMEM((rows, CORES * hidden), jnp.bfloat16),
            pltpu.VMEM((rows, width), jnp.float32),
            pltpu.VMEM((chips, rows, out_width), jnp.float32),
            pltpu.VMEM((2, rows, width), jnp.bfloat16),
            pltpu.VMEM((2, rows, width), jnp.bfloat16),
            pltpu.VMEM((chips, rows, out_width), jnp.bfloat16),
            pltpu.VMEM((chips, rows, out_width), jnp.bfloat16),
            pltpu.VMEM((chips, rows, out_width), jnp.bfloat16),
            pltpu.VMEM((2, rows, out_width), jnp.bfloat16),
            pltpu.VMEM((2, hops, rows, out_width), jnp.bfloat16),
            dma((5,)),
            dma((3,)),
            dma((2, 3)),
            dma((2, last)),
            dma((2, last)),
            dma((2, last, PIECES)),
            dma((2, last, PIECES)),
            dma((2, last, PIECES)),
            dma((2, last, PIECES)),
            dma((2, 2, SPLIT)),
            dma((2, chips, SPLIT)),
            dma((2, hops, SPLIT)),
            dma((2, hops + 1, SPLIT)),
        ],
        compiler_params=pltpu.CompilerParams(collective_id=0, has_side_effects=True),
    )(tokens, norm_gain[None, :], expert_ids.T, gate_weights.T, w_gate, w_up, w_down)


def step(mesh, *arrays):
    tokens, norm_gain, w_gate, w_up, w_down, expert_ids, gate_weights = arrays
    ep_count, tp_count = mesh.shape["ep"], mesh.shape["tp"]
    rows, top_count = expert_ids.shape
    experts_all = ep_count * w_gate.shape[0]
    capacity = min(rows, rows * top_count * 4 // (3 * experts_all))
    dense = (
        w_gate.shape[0] == 1
        and tp_count == 2
        and ep_count % CORES == 0
        and ep_count > CORES
        and rows <= 2 * capacity
        and rows % (32 * PIECES) == 0
        and rows % (16 * SPLIT) == 0
    )
    return fused(*arrays) if dense else body(*arrays)


def solution(mesh):
    placed = (
        P(("grp", "ep"), None),
        P(),
        P("ep", None, "tp"),
        P("ep", None, "tp"),
        P("ep", "tp", None),
        P(("grp", "ep"), None),
        P(("grp", "ep"), None),
    )
    return jax.shard_map(
        functools.partial(step, mesh), mesh=mesh, in_specs=placed, out_specs=P(("grp", "ep"), "tp"), check_vma=False
    )
```

```python
import functools

import jax
import jax.numpy as jnp
from jax import lax
from jax.experimental import pallas as pl
from jax.experimental.pallas import tpu as pltpu
from jax.sharding import PartitionSpec as P

epsilon = 1e-06
clamp_limit = 7.0
swish_alpha = 1.702


def rms_norm(tokens, norm_gain):
    widened = tokens.astype(jnp.float32)
    scaled = widened * lax.rsqrt(jnp.mean(widened * widened, axis=-1, keepdims=True) + epsilon)
    return (scaled * norm_gain).astype(jnp.bfloat16)


def body(tokens, norm_gain, w_gate, w_up, w_down, expert_ids, gate_weights):
    tok_rows, model_width = tokens.shape
    top_count = expert_ids.shape[1]
    ep_count = lax.axis_size("ep")
    local_experts = w_gate.shape[0]
    experts_all = local_experts * ep_count
    capacity = min(tok_rows, tok_rows * top_count * 4 // (3 * experts_all))
    normed = rms_norm(tokens, norm_gain)
    flat_ids = expert_ids.reshape(-1)
    onehot = (flat_ids[:, None] == jnp.arange(experts_all, dtype=jnp.int32)[None, :]).astype(
        jnp.int32
    )
    before = jnp.cumsum(onehot, axis=0) - onehot
    slot_index = jnp.sum(before * onehot, axis=1)
    dest_row = flat_ids * capacity + slot_index
    owner_tok = jnp.arange(tok_rows * top_count, dtype=jnp.int32) // top_count
    slot_table = (
        jnp.full((experts_all * capacity,), tok_rows, jnp.int32).at[dest_row].set(owner_tok)
    )
    padded = jnp.concatenate([normed, jnp.zeros((1, model_width), jnp.bfloat16)], axis=0)
    send_buffer = padded[slot_table].reshape(experts_all, capacity, model_width)
    received = lax.all_to_all(send_buffer, "ep", split_axis=0, concat_axis=0, tiled=True)
    expert_rows = received.reshape(ep_count, local_experts, capacity, model_width)
    gate_pre = jnp.einsum("sjcd,jdf->sjcf", expert_rows, w_gate, preferred_element_type=jnp.float32)
    up_pre = jnp.einsum("sjcd,jdf->sjcf", expert_rows, w_up, preferred_element_type=jnp.float32)
    gated = jnp.minimum(gate_pre, clamp_limit)
    linear = jnp.clip(up_pre, -clamp_limit, clamp_limit)
    activated = (gated * jax.nn.sigmoid(swish_alpha * gated) * (linear + 1.0)).astype(jnp.bfloat16)
    partial_value = jnp.einsum(
        "sjcf,jfd->sjcd", activated, w_down, preferred_element_type=jnp.float32
    ).astype(jnp.bfloat16)
    summed = (
        lax.psum_scatter(partial_value, "tp", scatter_dimension=3, tiled=True)
        .astype(jnp.float32)
        .astype(jnp.bfloat16)
    )
    returned = lax.all_to_all(summed, "ep", split_axis=0, concat_axis=0, tiled=True)
    returned = returned.reshape(experts_all * capacity, returned.shape[3])
    picked = returned[dest_row].reshape(tok_rows, top_count, returned.shape[1]).astype(jnp.float32)
    return jnp.sum(picked * gate_weights[:, :, None], axis=1).astype(jnp.bfloat16)


MESH = pl.DeviceIdType.MESH
CORES = 2
PIECES = 6
SPLIT = 3
OVER = 1
HIDDEN_TILE = 256
COLUMN_TILE = 512


def fused_kernel(
    chips,
    tok_hbm,
    gain_hbm,
    ids_hbm,
    gates_hbm,
    wg_hbm,
    wu_hbm,
    wd_hbm,
    out_ref,
    tok_ref,
    gain_ref,
    ids_ref,
    gates_ref,
    rows_all,
    codes,
    wg,
    wu,
    wd,
    act,
    kept,
    part,
    merge_out,
    merge_in,
    side_out,
    side_in,
    far_out,
    far_in,
    agg_in,
    over_in,
    input_sem,
    weight_sem,
    pair_sem,
    code_send,
    code_recv,
    z_send,
    z_recv,
    x_send,
    x_recv,
    merge_sem,
    side_sem,
    far_send,
    far_recv,
    over_sem,
):
    ep, tp = lax.axis_index("ep"), lax.axis_index("tp")
    z, core = lax.div(ep, CORES), lax.rem(ep, CORES)
    rows, width = tok_hbm.shape
    half = rows // 2
    piece = half // PIECES
    out_width = width // 2
    hidden = wg.shape[2]
    last = chips - 1
    partner = {"ep": z * CORES + 1 - core}
    peer = {"tp": 1 - tp}
    onward = ({"ep": (z + 1) * CORES + core}, {"ep": (z - 1) * CORES + core})
    has_next = (z < last, z > 0)
    centre = jnp.where(2 * z < last, 1, 0)

    def half_of(which):
        return pl.ds(pl.multiple_of(which * half, 16), half)

    small = [
        pltpu.make_async_copy(source, target, input_sem.at[i])
        for i, (source, target) in enumerate(
            (
                (gain_hbm, gain_ref),
                (ids_hbm, ids_ref),
                (gates_hbm, gates_ref),
                (tok_hbm.at[half_of(tp)], tok_ref.at[half_of(tp)]),
                (tok_hbm.at[half_of(1 - tp)], tok_ref.at[half_of(1 - tp)]),
            )
        )
    ]
    sources = (wg_hbm.at[0], wu_hbm.at[0], wd_hbm.at[0])
    loads = [
        pltpu.make_async_copy(source, target, weight_sem.at[i])
        for i, (source, target) in enumerate(
            zip(sources, (wg.at[0], wu.at[0], wd.at[pl.ds(0, hidden)]))
        )
    ]

    barrier = pltpu.get_barrier_semaphore()
    for target in (partner, peer):
        pl.semaphore_signal(barrier, inc=1, device_id=target, device_id_type=MESH)
    for side in range(2):

        @pl.when(has_next[side])
        def _(side=side):
            pl.semaphore_signal(barrier, inc=1, device_id=onward[side], device_id_type=MESH)

    for load in small + loads:
        load.start()

    def block_at(side, distance):
        return z - distance if side == 0 else z + distance

    def valid(side, distance):
        return z >= distance if side == 0 else z + distance < chips

    def remote(source, target, send, recv, device):
        return pltpu.make_async_remote_copy(
            src_ref=source,
            dst_ref=target,
            send_sem=send,
            recv_sem=recv,
            device_id=device,
            device_id_type=MESH,
        )

    def chip_of(block):
        return {"ep": block * CORES + core}

    gives = [
        remote(source, target, pair_sem.at[0, i], pair_sem.at[1, i], partner)
        for i, (source, target) in enumerate(
            zip(sources, (wg.at[1], wu.at[1], wd.at[pl.ds(hidden, hidden)]))
        )
    ]

    def normed(which):
        span = half_of(which)
        widened = tok_ref[span].astype(jnp.float32)
        scaled = widened * lax.rsqrt(jnp.mean(widened * widened, axis=-1, keepdims=True) + epsilon)
        rows_all[z, span] = (scaled * gain_ref[...]).astype(jnp.bfloat16)

    for load in small[:4]:
        load.wait()
    normed(tp)
    line = lax.broadcasted_iota(jnp.int32, (codes.shape[1], rows), 0)
    gate = jnp.zeros(line.shape, jnp.float32)
    for k in range(ids_ref.shape[0]):
        gate = gate + jnp.where(line == ids_ref[k : k + 1, :], gates_ref[k : k + 1, :], 0.0)
    codes[z] = jnp.zeros(codes.shape[1:], jnp.float32)
    codes[z, :, :rows] = gate

    neighbours = 2 + jnp.where(z > 0, 1, 0) + jnp.where(z < last, 1, 0)
    pl.semaphore_wait(barrier, neighbours)

    def rows_of(block, which, q):
        start = pl.multiple_of(which * half + q * piece, 16)
        return rows_all.at[block, pl.ds(start, piece), :]

    def flow(turn):
        side = centre if turn == 0 else 1 - centre
        ahead = z + 1 - 2 * side
        return side, {"ep": ahead * CORES + core}, (ahead >= 0) & (ahead < chips)

    def at(turn, distance):
        block = z + distance * (2 * flow(turn)[0] - 1)
        return block, (block >= 0) & (block < chips)

    def z_copy(turn, distance, q):
        side, device, _ = flow(turn)
        ref = rows_of(at(turn, distance)[0], tp, q)
        return remote(ref, ref, z_send.at[side, distance, q], z_recv.at[side, distance, q], device)

    def z_arrival(turn, distance, q):
        side, device, _ = flow(turn)
        ref = rows_of(at(turn, distance)[0], tp, q)
        return remote(
            ref, ref, z_send.at[side, distance - 1, q], z_recv.at[side, distance - 1, q], device
        )

    def code_copy(turn, distance, hop):
        side, device, _ = flow(turn)
        ref = codes.at[at(turn, distance)[0]]
        return remote(ref, ref, code_send.at[side, hop], code_recv.at[side, hop], device)

    def x_copy(turn, distance, q, which):
        side = flow(turn)[0]
        ref = rows_of(at(turn, distance)[0], which, q)
        return remote(
            ref, ref, x_send.at[side, distance - 1, q], x_recv.at[side, distance - 1, q], peer
        )

    for q in range(PIECES):
        for turn in range(2):

            @pl.when(flow(turn)[2])
            def _(turn=turn, q=q):
                z_copy(turn, 0, q).start()
                if q == 0:
                    code_copy(turn, 0, 0).start()

    for give in gives:
        give.start()
    small[4].wait()
    normed(1 - tp)

    def gather_z(distance, pieces):
        if distance > last:
            return
        for q in pieces:
            for turn in range(2):

                @pl.when(at(turn, distance)[1])
                def _(turn=turn, q=q):
                    z_arrival(turn, distance, q).wait_recv()
                    if q == 0:
                        code_copy(turn, distance, distance - 1).wait_recv()
                    if distance < last:

                        @pl.when(flow(turn)[2])
                        def _():
                            z_copy(turn, distance, q).start()
                            if q == 0:
                                code_copy(turn, distance, distance).start()

                    if distance > 1 or turn == 0:
                        x_copy(turn, distance, q, tp).start()

    def outer_x():
        @pl.when(at(1, 1)[1])
        def _():
            for q in range(PIECES):
                x_copy(1, 1, q, tp).start()

    def in_turn(distance, turn):
        side = centre if turn == 0 else 1 - centre
        block = z + distance * (2 * side - 1)
        return side, block, (block >= 0) & (block < chips)

    def wait_x(distance, turn):
        @pl.when(at(turn, distance)[1])
        def _():
            for q in range(PIECES):
                x_copy(turn, distance, q, 1 - tp).wait_recv()

    theirs = pl.multiple_of((1 - tp) * out_width, 128)
    mine = pl.multiple_of(tp * out_width, 128)

    def span_of(q):
        return pl.ds(q * (rows // SPLIT), rows // SPLIT)

    def activate(block, slot):
        turned = jnp.transpose(codes[block])
        lane = lax.broadcasted_iota(jnp.int32, turned.shape, 1)
        owner = ep if slot == 0 else z * CORES + 1 - core
        weight = jnp.sum(jnp.where(lane == owner, turned, 0.0), axis=1, keepdims=True)[:rows]
        held = rows_all[block]
        for start in range(0, hidden, HIDDEN_TILE):
            columns = slice(start, start + HIDDEN_TILE)
            gate_pre = jnp.dot(held, wg[slot, :, columns], preferred_element_type=jnp.float32)
            up_pre = jnp.dot(held, wu[slot, :, columns], preferred_element_type=jnp.float32)
            gated = jnp.minimum(gate_pre, clamp_limit)
            linear = jnp.clip(up_pre, -clamp_limit, clamp_limit)
            value = gated * jax.nn.sigmoid(swish_alpha * gated) * (linear + 1.0) * weight
            act[:, slot * hidden + start : slot * hidden + start + HIDDEN_TILE] = value.astype(
                jnp.bfloat16
            )

    def project(start):
        return jnp.dot(
            act[...], wd[:, pl.ds(start, COLUMN_TILE)], preferred_element_type=jnp.float32
        )

    def merge_copy(side, other, q, block):
        return remote(
            merge_out.at[side, span_of(q)],
            merge_in.at[other, span_of(q)],
            merge_sem.at[0, side, q],
            merge_sem.at[1, other, q],
            chip_of(block),
        )

    def side_copy(block, q):
        return remote(
            side_out.at[block, span_of(q)],
            side_in.at[block, span_of(q)],
            side_sem.at[0, block, q],
            side_sem.at[1, block, q],
            peer,
        )

    def far_copy(side, distance, q):
        dest = block_at(side, distance)
        sender = far_send.at[side, distance - 2, q]
        if distance == 2:
            target, receiver = far_in.at[1 - side, span_of(q)], far_recv.at[1 - side, 0, q]
            device = chip_of(dest)
        else:
            target = agg_in.at[side, distance - 3, span_of(q)]
            receiver = far_recv.at[side, distance - 2, q]
            device = onward[1 - side]
        return remote(far_out.at[dest, span_of(q)], target, sender, receiver, device)

    def over_copy(side, block, q):
        return remote(
            side_out.at[block, span_of(q)],
            over_in.at[1 - side, span_of(q)],
            over_sem.at[0, side, q],
            over_sem.at[1, 1 - side, q],
            chip_of(block),
        )

    def last_copy(side, block, q):
        return remote(
            far_out.at[block, span_of(q)],
            far_in.at[1 - side, span_of(q)],
            far_send.at[side, 0, q],
            far_recv.at[1 - side, 0, q],
            chip_of(block),
        )

    def far_arrival(side, q):
        return remote(
            far_in.at[side, span_of(q)],
            far_in.at[side, span_of(q)],
            far_send.at[side, 0, q],
            far_recv.at[side, 0, q],
            peer,
        )

    def agg_arrival(side, distance, q):
        ref = agg_in.at[side, distance - 2, span_of(q)]
        return remote(
            ref, ref, far_send.at[side, 0, q], far_recv.at[side, distance - 1, q], peer
        )

    def hidden_at(distance, turn, slot):
        side, block, there = in_turn(distance, turn)

        @pl.when(there)
        def _():
            activate(block, slot)

    def project_at(distance, turn):
        side, block, there = in_turn(distance, turn)

        @pl.when(there)
        def _():
            if distance == 1:
                for start in range(0, width, COLUMN_TILE):
                    merge_out[side, :, start : start + COLUMN_TILE] = project(start).astype(
                        jnp.bfloat16
                    )
                for q in range(SPLIT):
                    merge_copy(side, 1 - side, q, block).start()
            else:
                for start in range(0, out_width, COLUMN_TILE):
                    side_out[block, :, start : start + COLUMN_TILE] = project(
                        pl.multiple_of(theirs + start, 128)
                    ).astype(jnp.bfloat16)
                for start in range(0, out_width, COLUMN_TILE):
                    part[block, :, start : start + COLUMN_TILE] = project(
                        pl.multiple_of(mine + start, 128)
                    )

    def sides_at(distance, turn):
        side, block, there = in_turn(distance, turn)
        over = OVER if distance == 2 else 0
        through = flow(turn)[2]

        @pl.when(there & jnp.logical_not(through))
        def _():
            for q in range(over):
                over_copy(side, block, q).start()
                far_out[block, span_of(q)] = part[block, span_of(q)].astype(jnp.bfloat16)
                last_copy(side, block, q).start()

        @pl.when(there & through)
        def _():
            for q in range(over):
                side_copy(block, q).start()

        @pl.when(there)
        def _():
            for q in range(over, SPLIT):
                side_copy(block, q).start()

    def far_sum(side, distance, more):
        block = block_at(side, distance)
        for q in range(OVER if distance == 2 and not more else 0, SPLIT):
            span = span_of(q)
            side_copy(block, q).wait_recv()
            total = part[block, span] + side_in[block, span].astype(jnp.float32)
            if more:
                agg_arrival(side, distance, q).wait_recv()
                total = total + agg_in[side, distance - 2, span].astype(jnp.float32)
            far_out[block, span] = total.astype(jnp.bfloat16)
            far_copy(side, distance, q).start()

    def far_sums(distance, more):
        for side in range(2):
            through = has_next[side]

            @pl.when(valid(side, distance) & (through if more else jnp.logical_not(through)))
            def _(side=side):
                far_sum(side, distance, more)

    def own_exchange():
        for q in range(SPLIT):
            span = span_of(q)
            for side in range(2):

                @pl.when(valid(side, 1))
                def _(side=side, q=q):
                    merge_copy(1 - side, side, q, block_at(side, 1)).wait_recv()
                    kept[span] = kept[span] + merge_in[side, span].astype(jnp.float32)

            if q < OVER and chips > 2:
                for side in range(2):

                    @pl.when((z == 2) if side == 0 else (z + 2 == last))
                    def _(side=side, q=q):
                        over_copy(1 - side, block_at(side, 2), q).wait_recv()
                        here = (span, pl.ds(theirs, out_width))
                        kept[here] = kept[here] + over_in[side, span].astype(jnp.float32)

            side_out[z, span] = kept[span, pl.ds(theirs, out_width)].astype(jnp.bfloat16)
            side_copy(z, q).start()

    def finish():
        for q in range(SPLIT):
            span = span_of(q)
            side_copy(z, q).wait_recv()
            part[z, span] = kept[span, pl.ds(mine, out_width)] + side_in[z, span].astype(
                jnp.float32
            )
            if chips > 2:
                for side in range(2):

                    @pl.when(valid(side, 2))
                    def _(side=side, q=q):
                        far_arrival(side, q).wait_recv()
                        part[z, span] = part[z, span] + far_in[side, span].astype(jnp.float32)

            out_ref[span] = part[z, span].astype(jnp.bfloat16)

    third = PIECES // 3

    def pieces_of(distance, first, count):
        gather_z(distance, range(first * third, (first + count) * third))

    for load in loads[:2]:
        load.wait()
    gather_z(1, range(0, 1))
    activate(z, 0)
    gather_z(1, range(1, 2 * third))
    for give in gives[:2]:
        give.wait_recv()
    activate(z, 1)
    pieces_of(1, 2, 1)
    outer_x()
    loads[2].wait()
    gives[2].wait_recv()
    for start in range(0, width, COLUMN_TILE):
        kept[:, start : start + COLUMN_TILE] = project(start)
    for distance in range(1, chips):
        for turn in range(2):
            if 2 * distance + turn > chips and turn == 1:
                continue
            first = turn == 0
            if first:
                gather_z(distance + 1, range(0, 1))
            wait_x(distance, turn)
            hidden_at(distance, turn, 0)
            if first:
                gather_z(distance + 1, range(1, third))
            hidden_at(distance, turn, 1)
            if first:
                pieces_of(distance + 1, 1, 1)
            project_at(distance, turn)
            if first:
                pieces_of(distance + 1, 2, 1)
            if distance > 1:
                sides_at(distance, turn)
    for distance in range(2, last):
        far_sums(distance, False)
    own_exchange()
    if last >= 2:
        far_sums(last, False)
    for distance in range(last - 1, 1, -1):
        far_sums(distance, True)
    for give in gives:
        give.wait_send()
    for q in range(PIECES):
        for turn in range(2):
            for distance in range(chips):
                if distance < last:

                    @pl.when(at(turn, distance)[1] & flow(turn)[2])
                    def _(turn=turn, distance=distance, q=q):
                        z_copy(turn, distance, q).wait_send()
                        if q == 0:
                            code_copy(turn, distance, distance).wait_send()

                if distance > 0:

                    @pl.when(at(turn, distance)[1])
                    def _(turn=turn, distance=distance, q=q):
                        x_copy(turn, distance, q, tp).wait_send()

    for q in range(SPLIT):
        for side in range(2):

            @pl.when(valid(side, 1))
            def _(side=side, q=q):
                merge_copy(side, 1 - side, q, block_at(side, 1)).wait_send()

            for distance in range(2, chips):
                over = distance == 2 and q < OVER
                through = has_next[side] if over else True

                @pl.when(valid(side, distance) & through)
                def _(side=side, distance=distance, q=q):
                    side_copy(block_at(side, distance), q).wait_send()

                if over:

                    @pl.when(valid(side, distance) & jnp.logical_not(has_next[side]))
                    def _(side=side, distance=distance, q=q):
                        over_copy(side, block_at(side, distance), q).wait_send()

    finish()
    for q in range(SPLIT):
        side_copy(z, q).wait_send()
        for side in range(2):
            for distance in range(2, chips):

                @pl.when(valid(side, distance))
                def _(side=side, distance=distance, q=q):
                    far_copy(side, distance, q).wait_send()


def fused(tokens, norm_gain, w_gate, w_up, w_down, expert_ids, gate_weights):
    rows, width = tokens.shape
    top_count = expert_ids.shape[1]
    chips = lax.axis_size("ep") // CORES
    experts_all = chips * CORES
    hidden = w_gate.shape[2]
    out_width = width // 2
    last = chips - 1
    hops = max(last - 1, 1)
    lanes = -rows % 128
    vmem = pl.BlockSpec(memory_space=pltpu.VMEM)
    anywhere = pl.BlockSpec(memory_space=pl.ANY)
    dma = pltpu.SemaphoreType.DMA
    return pl.pallas_call(
        functools.partial(fused_kernel, chips),
        out_shape=pltpu.VMEM((rows, out_width), jnp.bfloat16),
        in_specs=[anywhere] * 7,
        out_specs=vmem,
        scratch_shapes=[
            pltpu.VMEM((rows, width), jnp.bfloat16),
            pltpu.VMEM((1, width), jnp.float32),
            pltpu.VMEM((top_count, rows), jnp.int32),
            pltpu.VMEM((top_count, rows), jnp.float32),
            pltpu.VMEM((chips, rows, width), jnp.bfloat16),
            pltpu.VMEM((chips, experts_all + -experts_all % 8, rows + lanes), jnp.float32),
            pltpu.VMEM((CORES, width, hidden), jnp.bfloat16),
            pltpu.VMEM((CORES, width, hidden), jnp.bfloat16),
            pltpu.VMEM((CORES * hidden, width), jnp.bfloat16),
            pltpu.VMEM((rows, CORES * hidden), jnp.bfloat16),
            pltpu.VMEM((rows, width), jnp.float32),
            pltpu.VMEM((chips, rows, out_width), jnp.float32),
            pltpu.VMEM((2, rows, width), jnp.bfloat16),
            pltpu.VMEM((2, rows, width), jnp.bfloat16),
            pltpu.VMEM((chips, rows, out_width), jnp.bfloat16),
            pltpu.VMEM((chips, rows, out_width), jnp.bfloat16),
            pltpu.VMEM((chips, rows, out_width), jnp.bfloat16),
            pltpu.VMEM((2, rows, out_width), jnp.bfloat16),
            pltpu.VMEM((2, hops, rows, out_width), jnp.bfloat16),
            pltpu.VMEM((2, rows, out_width), jnp.bfloat16),
            dma((5,)),
            dma((3,)),
            dma((2, 3)),
            dma((2, last)),
            dma((2, last)),
            dma((2, last, PIECES)),
            dma((2, last, PIECES)),
            dma((2, last, PIECES)),
            dma((2, last, PIECES)),
            dma((2, 2, SPLIT)),
            dma((2, chips, SPLIT)),
            dma((2, hops, SPLIT)),
            dma((2, hops + 1, SPLIT)),
            dma((2, 2, SPLIT)),
        ],
        compiler_params=pltpu.CompilerParams(collective_id=0, has_side_effects=True),
    )(tokens, norm_gain[None, :], expert_ids.T, gate_weights.T, w_gate, w_up, w_down)


def step(mesh, *arrays):
    tokens, norm_gain, w_gate, w_up, w_down, expert_ids, gate_weights = arrays
    ep_count, tp_count = mesh.shape["ep"], mesh.shape["tp"]
    rows, top_count = expert_ids.shape
    experts_all = ep_count * w_gate.shape[0]
    capacity = min(rows, rows * top_count * 4 // (3 * experts_all))
    dense = (
        w_gate.shape[0] == 1
        and tp_count == 2
        and ep_count % CORES == 0
        and ep_count > CORES
        and rows <= 2 * capacity
        and rows % (32 * PIECES) == 0
        and rows % (16 * SPLIT) == 0
    )
    return fused(*arrays) if dense else body(*arrays)


def solution(mesh):
    placed = (
        P(("grp", "ep"), None),
        P(),
        P("ep", None, "tp"),
        P("ep", None, "tp"),
        P("ep", "tp", None),
        P(("grp", "ep"), None),
        P(("grp", "ep"), None),
    )
    return jax.shard_map(
        functools.partial(step, mesh), mesh=mesh, in_specs=placed, out_specs=P(("grp", "ep"), "tp"), check_vma=False
    )
```

```python
import functools

import jax
import jax.numpy as jnp
from jax import lax
from jax.experimental import pallas as pl
from jax.experimental.pallas import tpu as pltpu
from jax.sharding import PartitionSpec as P

epsilon = 1e-06
clamp_limit = 7.0
swish_alpha = 1.702


def rms_norm(tokens, norm_gain):
    widened = tokens.astype(jnp.float32)
    scaled = widened * lax.rsqrt(jnp.mean(widened * widened, axis=-1, keepdims=True) + epsilon)
    return (scaled * norm_gain).astype(jnp.bfloat16)


def body(tokens, norm_gain, w_gate, w_up, w_down, expert_ids, gate_weights):
    tok_rows, model_width = tokens.shape
    top_count = expert_ids.shape[1]
    ep_count = lax.axis_size("ep")
    local_experts = w_gate.shape[0]
    experts_all = local_experts * ep_count
    capacity = min(tok_rows, tok_rows * top_count * 4 // (3 * experts_all))
    normed = rms_norm(tokens, norm_gain)
    flat_ids = expert_ids.reshape(-1)
    onehot = (flat_ids[:, None] == jnp.arange(experts_all, dtype=jnp.int32)[None, :]).astype(
        jnp.int32
    )
    before = jnp.cumsum(onehot, axis=0) - onehot
    slot_index = jnp.sum(before * onehot, axis=1)
    dest_row = flat_ids * capacity + slot_index
    owner_tok = jnp.arange(tok_rows * top_count, dtype=jnp.int32) // top_count
    slot_table = (
        jnp.full((experts_all * capacity,), tok_rows, jnp.int32).at[dest_row].set(owner_tok)
    )
    padded = jnp.concatenate([normed, jnp.zeros((1, model_width), jnp.bfloat16)], axis=0)
    send_buffer = padded[slot_table].reshape(experts_all, capacity, model_width)
    received = lax.all_to_all(send_buffer, "ep", split_axis=0, concat_axis=0, tiled=True)
    expert_rows = received.reshape(ep_count, local_experts, capacity, model_width)
    gate_pre = jnp.einsum("sjcd,jdf->sjcf", expert_rows, w_gate, preferred_element_type=jnp.float32)
    up_pre = jnp.einsum("sjcd,jdf->sjcf", expert_rows, w_up, preferred_element_type=jnp.float32)
    gated = jnp.minimum(gate_pre, clamp_limit)
    linear = jnp.clip(up_pre, -clamp_limit, clamp_limit)
    activated = (gated * jax.nn.sigmoid(swish_alpha * gated) * (linear + 1.0)).astype(jnp.bfloat16)
    partial_value = jnp.einsum(
        "sjcf,jfd->sjcd", activated, w_down, preferred_element_type=jnp.float32
    ).astype(jnp.bfloat16)
    summed = (
        lax.psum_scatter(partial_value, "tp", scatter_dimension=3, tiled=True)
        .astype(jnp.float32)
        .astype(jnp.bfloat16)
    )
    returned = lax.all_to_all(summed, "ep", split_axis=0, concat_axis=0, tiled=True)
    returned = returned.reshape(experts_all * capacity, returned.shape[3])
    picked = returned[dest_row].reshape(tok_rows, top_count, returned.shape[1]).astype(jnp.float32)
    return jnp.sum(picked * gate_weights[:, :, None], axis=1).astype(jnp.bfloat16)


MESH = pl.DeviceIdType.MESH
CORES = 2
PIECES = (0, 1, 3, 5, 6)
SPANS = (0, 1, 3)
OVER = 1
HIDDEN_TILE = 256
COLUMN_TILE = 512


def fused_kernel(
    chips,
    tok_hbm,
    gain_hbm,
    ids_hbm,
    gates_hbm,
    wg_hbm,
    wu_hbm,
    wd_hbm,
    out_ref,
    tok_ref,
    gain_ref,
    ids_ref,
    gates_ref,
    rows_all,
    codes,
    gate_cols,
    wg,
    wu,
    wd,
    act,
    kept,
    part,
    merge_out,
    merge_in,
    side_out,
    side_in,
    far_out,
    far_in,
    agg_in,
    over_in,
    input_sem,
    weight_sem,
    pair_sem,
    code_send,
    code_recv,
    z_send,
    z_recv,
    x_send,
    x_recv,
    merge_send,
    merge_recv,
    side_send,
    side_recv,
    far_send,
    far_recv,
    agg_recv,
    over_send,
    over_recv,
):
    ep, tp = lax.axis_index("ep"), lax.axis_index("tp")
    z, core = lax.div(ep, CORES), lax.rem(ep, CORES)
    rows, width = tok_hbm.shape
    half = rows // 2
    out_width = width // 2
    hidden = wg.shape[2]
    last = chips - 1
    partner = {"ep": z * CORES + 1 - core}
    peer = {"tp": 1 - tp}
    centre = jnp.where(2 * z < last, 1, 0)

    def chip_of(block):
        return {"ep": block * CORES + core}

    def within(block):
        return (block >= 0) & (block < chips)

    def flow(turn):
        side = centre if turn == 0 else 1 - centre
        ahead = z + 1 - 2 * side
        return side, ahead, within(ahead)

    def at(turn, distance):
        block = z + distance * (2 * flow(turn)[0] - 1)
        return block, within(block)

    def half_of(which):
        return pl.ds(pl.multiple_of(which * half, 16), half)

    small = [
        pltpu.make_async_copy(source, target, input_sem.at[i])
        for i, (source, target) in enumerate(
            (
                (gain_hbm, gain_ref),
                (ids_hbm, ids_ref),
                (gates_hbm, gates_ref),
                (tok_hbm.at[half_of(tp)], tok_ref.at[half_of(tp)]),
                (tok_hbm.at[half_of(1 - tp)], tok_ref.at[half_of(1 - tp)]),
            )
        )
    ]
    sources = (wg_hbm.at[0], wu_hbm.at[0], wd_hbm.at[0])
    loads = [
        pltpu.make_async_copy(source, target, weight_sem.at[i])
        for i, (source, target) in enumerate(
            zip(sources, (wg.at[0], wu.at[0], wd.at[pl.ds(0, hidden)]))
        )
    ]

    barrier = pltpu.get_barrier_semaphore()
    for target in (partner, peer):
        pl.semaphore_signal(barrier, inc=1, device_id=target, device_id_type=MESH)
    for turn in range(2):

        @pl.when(flow(turn)[2])
        def _(turn=turn):
            target = chip_of(flow(turn)[1])
            pl.semaphore_signal(barrier, inc=1, device_id=target, device_id_type=MESH)

    for load in small + loads:
        load.start()

    def remote(source, target, send, recv, device):
        return pltpu.make_async_remote_copy(
            src_ref=source,
            dst_ref=target,
            send_sem=send,
            recv_sem=recv,
            device_id=device,
            device_id_type=MESH,
        )

    gives = [
        remote(source, target, pair_sem.at[0, i], pair_sem.at[1, i], partner)
        for i, (source, target) in enumerate(
            zip(sources, (wg.at[1], wu.at[1], wd.at[pl.ds(hidden, hidden)]))
        )
    ]

    def normed(which):
        span = half_of(which)
        widened = tok_ref[span].astype(jnp.float32)
        scaled = widened * lax.rsqrt(jnp.mean(widened * widened, axis=-1, keepdims=True) + epsilon)
        rows_all[z, span] = (scaled * gain_ref[...]).astype(jnp.bfloat16)

    for load in small[:4]:
        load.wait()
    normed(tp)
    line = lax.broadcasted_iota(jnp.int32, (codes.shape[1], rows), 0)
    gate = jnp.zeros(line.shape, jnp.float32)
    for k in range(ids_ref.shape[0]):
        gate = gate + jnp.where(line == ids_ref[k : k + 1, :], gates_ref[k : k + 1, :], 0.0)
    codes[z] = jnp.zeros(codes.shape[1:], jnp.float32)
    codes[z, :, :rows] = gate

    neighbours = 2 + jnp.where(z > 0, 1, 0) + jnp.where(z < last, 1, 0)
    pl.semaphore_wait(barrier, neighbours)

    count = len(PIECES) - 1

    def rows_of(block, which, q):
        unit = half // PIECES[-1]
        start = pl.multiple_of(which * half + PIECES[q] * unit, 16)
        return rows_all.at[block, pl.ds(start, (PIECES[q + 1] - PIECES[q]) * unit)]

    def sender(turn, distance):
        side, _, _ = flow(turn)
        return jnp.where(side == 1, chips, z) if distance == 0 else at(turn, distance)[0]

    def z_copy(turn, distance, q):
        block = at(turn, distance)[0]
        ref = rows_of(block, tp, q)
        device = chip_of(flow(turn)[1])
        return remote(
            ref, ref, z_send.at[sender(turn, distance)], z_recv.at[block, q], device
        )

    def z_sent(turn, distance):
        ref = rows_all.at[z, half_of(tp)]
        return remote(ref, ref, z_send.at[sender(turn, distance)], z_recv.at[z, 0], peer)

    def code_copy(turn, distance):
        block = at(turn, distance)[0]
        device = chip_of(flow(turn)[1])
        return remote(
            codes.at[block],
            codes.at[block],
            code_send.at[sender(turn, distance)],
            code_recv.at[block],
            device,
        )

    def x_copy(block, which, q):
        ref = rows_of(block, which, q)
        return remote(ref, ref, x_send.at[block], x_recv.at[block], peer)

    def x_whole(block, which):
        ref = rows_all.at[block, half_of(which)]
        return remote(ref, ref, x_send.at[block], x_recv.at[block], peer)

    for q in range(count):
        for turn in range(2):

            @pl.when(flow(turn)[2])
            def _(turn=turn, q=q):
                z_copy(turn, 0, q).start()
                if q == 0:
                    code_copy(turn, 0).start()

    for give in gives:
        give.start()
    small[4].wait()
    normed(1 - tp)

    def gather_z(distance, q):
        for turn in range(2):

            @pl.when(at(turn, distance)[1])
            def _(turn=turn):
                z_copy(turn, distance, q).wait_recv()
                if q == 0:
                    code_copy(turn, distance).wait_recv()
                if distance < last:

                    @pl.when(flow(turn)[2])
                    def _():
                        z_copy(turn, distance, q).start()
                        if q == 0:
                            code_copy(turn, distance).start()

                if distance > 1 or turn == 0:
                    x_copy(at(turn, distance)[0], tp, q).start()

    waiting = [(distance, q) for distance in range(1, chips) for q in range(count)]

    def pump():
        if waiting:
            gather_z(*waiting.pop(0))

    def pump_all(distance):
        while waiting and waiting[0][0] <= distance:
            pump()

    def outer_x():
        @pl.when(at(1, 1)[1])
        def _():
            for q in range(count):
                x_copy(at(1, 1)[0], tp, q).start()

    def wait_x(distance, turn):
        @pl.when(at(turn, distance)[1])
        def _():
            x_whole(at(turn, distance)[0], 1 - tp).wait_recv()

    theirs = pl.multiple_of((1 - tp) * out_width, 128)
    mine = pl.multiple_of(tp * out_width, 128)
    parts = len(SPANS) - 1
    unit = half // SPANS[-1]
    first_half, second_half = tp, 1 - tp

    def span_of(which, s):
        start = pl.multiple_of(which * half + SPANS[s] * unit, 16)
        return pl.ds(start, (SPANS[s + 1] - SPANS[s]) * unit)

    def activate(block, start, size, slot):
        if slot == 0:
            gate_cols[...] = jnp.transpose(codes[block])
        span = pl.ds(start, size)
        turned = gate_cols[span]
        lane = lax.broadcasted_iota(jnp.int32, turned.shape, 1)
        owner = ep if slot == 0 else z * CORES + 1 - core
        weight = jnp.sum(jnp.where(lane == owner, turned, 0.0), axis=1, keepdims=True)
        held = rows_all[block, span]
        for begin in range(0, hidden, HIDDEN_TILE):
            columns = slice(begin, begin + HIDDEN_TILE)
            gate_pre = jnp.dot(held, wg[slot, :, columns], preferred_element_type=jnp.float32)
            up_pre = jnp.dot(held, wu[slot, :, columns], preferred_element_type=jnp.float32)
            gated = jnp.minimum(gate_pre, clamp_limit)
            linear = jnp.clip(up_pre, -clamp_limit, clamp_limit)
            value = gated * jax.nn.sigmoid(swish_alpha * gated) * (linear + 1.0) * weight
            act[:size, slot * hidden + begin : slot * hidden + begin + HIDDEN_TILE] = value.astype(
                jnp.bfloat16
            )

    def project(start, size):
        return jnp.dot(
            act[:size], wd[:, pl.ds(start, COLUMN_TILE)], preferred_element_type=jnp.float32
        )

    def merge_copy(side, other, which, s, block):
        span = span_of(which, s)
        return remote(
            merge_out.at[side, span],
            merge_in.at[other, span],
            merge_send.at[side],
            merge_recv.at[other, which * parts + s],
            chip_of(block),
        )

    def side_copy(block, which, s):
        span = span_of(which, s)
        return remote(
            side_out.at[block, span],
            side_in.at[block, span],
            side_send.at[block],
            side_recv.at[block, which * parts + s],
            peer,
        )

    def over_copy(side, block, which, s):
        span = span_of(which, s)
        return remote(
            side_out.at[block, span],
            over_in.at[1 - side, span],
            over_send.at[side],
            over_recv.at[1 - side, which * OVER + s],
            chip_of(block),
        )

    def far_copy(side, distance, block, which, s):
        span = span_of(which, s)
        if distance == 2:
            target = far_in.at[1 - side, span]
            receiver = far_recv.at[1 - side, which * parts + s]
            device = chip_of(block)
        else:
            target = agg_in.at[side, distance - 3, span]
            receiver = agg_recv.at[side, distance - 3, which * parts + s]
            device = chip_of(z + 2 * side - 1)
        return remote(far_out.at[block, span], target, far_send.at[block], receiver, device)

    def sent(ref, sem):
        return remote(ref, ref, sem, side_recv.at[0, 0], peer)

    def arrived(ref, sem):
        return remote(ref, ref, side_send.at[0], sem, peer)

    def job(distance, turn, which, pumped):
        block, there = at(turn, distance)
        side, _, through = flow(turn)
        start = pl.multiple_of(which * half, 16)

        @pl.when(there)
        def _():
            activate(block, start, half, 0)

        @pl.when(there)
        def _():
            activate(block, start, half, 1)

        if pumped:
            pump()

        @pl.when(there)
        def _():
            rows_here = half_of(which)
            if distance == 1:
                for begin in range(0, width, COLUMN_TILE):
                    merge_out[side, rows_here, begin : begin + COLUMN_TILE] = project(
                        begin, half
                    ).astype(jnp.bfloat16)
                if turn == 0 or which is second_half:
                    for s in range(parts):
                        merge_copy(side, 1 - side, which, s, block).start()
            else:
                for begin in range(0, out_width, COLUMN_TILE):
                    side_out[block, rows_here, begin : begin + COLUMN_TILE] = project(
                        pl.multiple_of(theirs + begin, 128), half
                    ).astype(jnp.bfloat16)
                if distance == last:
                    for s in range(OVER if distance == 2 else 0, parts):
                        side_copy(block, which, s).start()
                for begin in range(0, out_width, COLUMN_TILE):
                    part[block, rows_here, begin : begin + COLUMN_TILE] = project(
                        pl.multiple_of(mine + begin, 128), half
                    )
            if distance == 2:

                @pl.when(jnp.logical_not(through))
                def _():
                    for s in range(OVER):
                        span = span_of(which, s)
                        over_copy(side, block, which, s).start()
                        far_out[block, span] = part[block, span].astype(jnp.bfloat16)
                        far_copy(side, 2, block, which, s).start()

        if pumped:
            pump()

    def merges_at(turn, which):
        block, there = at(turn, 1)
        side = flow(turn)[0]

        @pl.when(there)
        def _():
            for s in range(parts):
                merge_copy(side, 1 - side, which, s, block).start()

    def sides_at(distance, turn, which, going):
        block, there = at(turn, distance)
        through = flow(turn)[2]

        @pl.when(there & (through if going else jnp.logical_not(through)))
        def _():
            for s in range(OVER if distance == 2 and not going else 0, parts):
                side_copy(block, which, s).start()

    def far_sums(distance, more):
        for turn in range(2):
            block, there = at(turn, distance)
            side, _, through = flow(turn)

            @pl.when(there & (through if more else jnp.logical_not(through)))
            def _(block=block, side=side):
                for which in (second_half, first_half):
                    for s in range(OVER if distance == 2 and not more else 0, parts):
                        span = span_of(which, s)
                        side_copy(block, which, s).wait_recv()
                        total = part[block, span] + side_in[block, span].astype(jnp.float32)
                        if more:
                            arrived(
                                agg_in.at[side, distance - 2, span],
                                agg_recv.at[side, distance - 2, which * parts + s],
                            ).wait_recv()
                            total = total + agg_in[side, distance - 2, span].astype(jnp.float32)
                        far_out[block, span] = total.astype(jnp.bfloat16)
                        far_copy(side, distance, block, which, s).start()

    def own_exchange():
        for which in (first_half, second_half):
            for s in range(parts):
                span = span_of(which, s)
                for turn in range(2):

                    @pl.when(at(turn, 1)[1])
                    def _(turn=turn):
                        side = flow(turn)[0]
                        arrived(
                            merge_in.at[side, span], merge_recv.at[side, which * parts + s]
                        ).wait_recv()
                        kept[span] = kept[span] + merge_in[side, span].astype(jnp.float32)

                    if s < OVER and chips > 2:
                        side = flow(turn)[0]
                        block = at(turn, 2)[0]

                        @pl.when(block == jnp.where(side == 1, last, 0))
                        def _(side=side):
                            arrived(
                                over_in.at[side, span], over_recv.at[side, which * OVER + s]
                            ).wait_recv()
                            here = (span, pl.ds(theirs, out_width))
                            kept[here] = kept[here] + over_in[side, span].astype(jnp.float32)

                side_out[z, span] = kept[span, pl.ds(theirs, out_width)].astype(jnp.bfloat16)
                side_copy(z, which, s).start()

    def finish():
        for which in (second_half, first_half):
            for s in range(parts):
                span = span_of(which, s)
                here = (span, pl.ds(mine, out_width))
                if chips > 2:
                    for turn in range(2):

                        @pl.when(at(turn, 2)[1])
                        def _(turn=turn):
                            side = flow(turn)[0]
                            arrived(
                                far_in.at[side, span], far_recv.at[side, which * parts + s]
                            ).wait_recv()
                            kept[here] = kept[here] + far_in[side, span].astype(jnp.float32)

                side_copy(z, which, s).wait_recv()
                out_ref[span] = (kept[here] + side_in[z, span].astype(jnp.float32)).astype(
                    jnp.bfloat16
                )

    for load in loads[:2]:
        load.wait()
    pump()
    activate(z, 0, rows, 0)
    for _ in range(count - 2):
        pump()
    for give in gives[:2]:
        give.wait_recv()
    activate(z, 0, rows, 1)
    pump_all(1)
    outer_x()
    loads[2].wait()
    gives[2].wait_recv()
    for begin in range(0, width, COLUMN_TILE):
        kept[:, begin : begin + COLUMN_TILE] = project(begin, rows)

    outer = range(1, last // 2 + 1)
    job(1, 0, first_half, True)
    for distance in range(1, chips):
        if distance in outer:
            job(distance, 1, first_half, False)
        wait_x(distance, 0)
        job(distance, 0, second_half, distance < last)
        if 1 < distance < last:
            sides_at(distance, 0, second_half, True)
        if distance < last:
            pump_all(distance + 1)
            if distance == 1:
                merges_at(1, first_half)
            job(distance + 1, 0, first_half, True)
            if distance + 1 < last:
                sides_at(distance + 1, 0, first_half, True)
            if 1 < distance:
                sides_at(distance, 0, first_half, False)
        if distance in outer:
            wait_x(distance, 1)
            job(distance, 1, second_half, False)
            if distance > 1:
                for which in (first_half, second_half):
                    for going in (True, False):
                        sides_at(distance, 1, which, going)
    for distance in range(last - 1, 1, -1):
        sides_at(distance, 0, second_half, False)
    if last > 1:
        far_sums(last, False)
    own_exchange()
    for distance in range(last - 1, 1, -1):
        far_sums(distance, False)
        far_sums(distance, True)

    for give in gives:
        give.wait_send()
    for turn in range(2):
        for distance in range(chips):
            if distance < last:

                @pl.when(at(turn, distance)[1] & flow(turn)[2])
                def _(turn=turn, distance=distance):
                    z_sent(turn, distance).wait_send()
                    code_copy(turn, distance).wait_send()

            if distance > 0:

                @pl.when(at(turn, distance)[1])
                def _(turn=turn, distance=distance):
                    x_whole(at(turn, distance)[0], tp).wait_send()

        @pl.when(at(turn, 1)[1])
        def _(turn=turn):
            side = flow(turn)[0]
            sent(merge_out.at[side], merge_send.at[side]).wait_send()

    finish()
    sent(side_out.at[z], side_send.at[z]).wait_send()
    short = 2 * SPANS[OVER] * unit
    for turn in range(2):
        side, _, through = flow(turn)
        for distance in range(2, chips):
            block, there = at(turn, distance)
            whole = there & through if distance == 2 else there

            @pl.when(whole)
            def _(block=block):
                sent(side_out.at[block], side_send.at[block]).wait_send()

            if distance == 2:

                @pl.when(there & jnp.logical_not(through))
                def _(block=block, side=side):
                    rest = side_out.at[block, pl.ds(0, rows - short)]
                    sent(rest, side_send.at[block]).wait_send()
                    sent(side_out.at[block, pl.ds(0, short)], over_send.at[side]).wait_send()

            @pl.when(there)
            def _(block=block):
                sent(far_out.at[block], far_send.at[block]).wait_send()


def fused(tokens, norm_gain, w_gate, w_up, w_down, expert_ids, gate_weights):
    rows, width = tokens.shape
    top_count = expert_ids.shape[1]
    chips = lax.axis_size("ep") // CORES
    experts_all = chips * CORES
    lines = experts_all + -experts_all % 8
    hidden = w_gate.shape[2]
    out_width = width // 2
    last = chips - 1
    aggregates = max(last - 2, 1)
    lanes = rows + -rows % 128
    spans = 2 * (len(SPANS) - 1)
    anywhere = pl.BlockSpec(memory_space=pl.ANY)
    vmem, dma = pltpu.VMEM, pltpu.SemaphoreType.DMA
    return pl.pallas_call(
        functools.partial(fused_kernel, chips),
        out_shape=vmem((rows, out_width), jnp.bfloat16),
        in_specs=[anywhere] * 7,
        out_specs=pl.BlockSpec(memory_space=vmem),
        scratch_shapes=[
            vmem((rows, width), jnp.bfloat16),
            vmem((1, width), jnp.float32),
            vmem((top_count, rows), jnp.int32),
            vmem((top_count, rows), jnp.float32),
            vmem((chips, rows, width), jnp.bfloat16),
            vmem((chips, lines, lanes), jnp.float32),
            vmem((lanes, lines), jnp.float32),
            vmem((CORES, width, hidden), jnp.bfloat16),
            vmem((CORES, width, hidden), jnp.bfloat16),
            vmem((CORES * hidden, width), jnp.bfloat16),
            vmem((rows, CORES * hidden), jnp.bfloat16),
            vmem((rows, width), jnp.float32),
            vmem((chips, rows, out_width), jnp.float32),
            vmem((2, rows, width), jnp.bfloat16),
            vmem((2, rows, width), jnp.bfloat16),
            vmem((chips, rows, out_width), jnp.bfloat16),
            vmem((chips, rows, out_width), jnp.bfloat16),
            vmem((chips, rows, out_width), jnp.bfloat16),
            vmem((2, rows, out_width), jnp.bfloat16),
            vmem((2, aggregates, rows, out_width), jnp.bfloat16),
            vmem((2, rows, out_width), jnp.bfloat16),
            dma((5,)),
            dma((3,)),
            dma((2, 3)),
            dma((chips + 1,)),
            dma((chips,)),
            dma((chips + 1,)),
            dma((chips, len(PIECES) - 1)),
            dma((chips,)),
            dma((chips,)),
            dma((2,)),
            dma((2, spans)),
            dma((chips,)),
            dma((chips, spans)),
            dma((chips,)),
            dma((2, spans)),
            dma((2, aggregates, spans)),
            dma((2,)),
            dma((2, 2 * OVER)),
        ],
        compiler_params=pltpu.CompilerParams(collective_id=0, has_side_effects=True),
    )(tokens, norm_gain[None, :], expert_ids.T, gate_weights.T, w_gate, w_up, w_down)


def step(mesh, *arrays):
    tokens, norm_gain, w_gate, w_up, w_down, expert_ids, gate_weights = arrays
    ep_count, tp_count = mesh.shape["ep"], mesh.shape["tp"]
    rows, top_count = expert_ids.shape
    experts_all = ep_count * w_gate.shape[0]
    capacity = min(rows, rows * top_count * 4 // (3 * experts_all))
    dense = (
        w_gate.shape[0] == 1
        and tp_count == 2
        and ep_count % CORES == 0
        and ep_count > CORES
        and rows <= 2 * capacity
        and rows % (32 * PIECES[-1]) == 0
        and rows % (32 * SPANS[-1]) == 0
    )
    return fused(*arrays) if dense else body(*arrays)


def solution(mesh):
    placed = (
        P(("grp", "ep"), None),
        P(),
        P("ep", None, "tp"),
        P("ep", None, "tp"),
        P("ep", "tp", None),
        P(("grp", "ep"), None),
        P(("grp", "ep"), None),
    )
    return jax.shard_map(
        functools.partial(step, mesh), mesh=mesh, in_specs=placed, out_specs=P(("grp", "ep"), "tp"), check_vma=False
    )
```

```python
import functools

import jax
import jax.numpy as jnp
from jax import lax
from jax.experimental import pallas as pl
from jax.experimental.pallas import tpu as pltpu
from jax.sharding import PartitionSpec as P

epsilon = 1e-06
clamp_limit = 7.0
swish_alpha = 1.702


def rms_norm(tokens, norm_gain):
    widened = tokens.astype(jnp.float32)
    scaled = widened * lax.rsqrt(jnp.mean(widened * widened, axis=-1, keepdims=True) + epsilon)
    return (scaled * norm_gain).astype(jnp.bfloat16)


def body(tokens, norm_gain, w_gate, w_up, w_down, expert_ids, gate_weights):
    tok_rows, model_width = tokens.shape
    top_count = expert_ids.shape[1]
    ep_count = lax.axis_size("ep")
    local_experts = w_gate.shape[0]
    experts_all = local_experts * ep_count
    capacity = min(tok_rows, tok_rows * top_count * 4 // (3 * experts_all))
    normed = rms_norm(tokens, norm_gain)
    flat_ids = expert_ids.reshape(-1)
    onehot = (flat_ids[:, None] == jnp.arange(experts_all, dtype=jnp.int32)[None, :]).astype(
        jnp.int32
    )
    before = jnp.cumsum(onehot, axis=0) - onehot
    slot_index = jnp.sum(before * onehot, axis=1)
    dest_row = flat_ids * capacity + slot_index
    owner_tok = jnp.arange(tok_rows * top_count, dtype=jnp.int32) // top_count
    slot_table = (
        jnp.full((experts_all * capacity,), tok_rows, jnp.int32).at[dest_row].set(owner_tok)
    )
    padded = jnp.concatenate([normed, jnp.zeros((1, model_width), jnp.bfloat16)], axis=0)
    send_buffer = padded[slot_table].reshape(experts_all, capacity, model_width)
    received = lax.all_to_all(send_buffer, "ep", split_axis=0, concat_axis=0, tiled=True)
    expert_rows = received.reshape(ep_count, local_experts, capacity, model_width)
    gate_pre = jnp.einsum("sjcd,jdf->sjcf", expert_rows, w_gate, preferred_element_type=jnp.float32)
    up_pre = jnp.einsum("sjcd,jdf->sjcf", expert_rows, w_up, preferred_element_type=jnp.float32)
    gated = jnp.minimum(gate_pre, clamp_limit)
    linear = jnp.clip(up_pre, -clamp_limit, clamp_limit)
    activated = (gated * jax.nn.sigmoid(swish_alpha * gated) * (linear + 1.0)).astype(jnp.bfloat16)
    partial_value = jnp.einsum(
        "sjcf,jfd->sjcd", activated, w_down, preferred_element_type=jnp.float32
    ).astype(jnp.bfloat16)
    summed = (
        lax.psum_scatter(partial_value, "tp", scatter_dimension=3, tiled=True)
        .astype(jnp.float32)
        .astype(jnp.bfloat16)
    )
    returned = lax.all_to_all(summed, "ep", split_axis=0, concat_axis=0, tiled=True)
    returned = returned.reshape(experts_all * capacity, returned.shape[3])
    picked = returned[dest_row].reshape(tok_rows, top_count, returned.shape[1]).astype(jnp.float32)
    return jnp.sum(picked * gate_weights[:, :, None], axis=1).astype(jnp.bfloat16)


MESH = pl.DeviceIdType.MESH
CORES = 2
PIECES = (0, 1, 3, 5, 6)
SPANS = (0, 1, 2, 3)
OVER = 1
NEAR = 1
HIDDEN_TILE = 256
COLUMN_TILE = 512


def fused_kernel(
    chips,
    tok_hbm,
    gain_hbm,
    ids_hbm,
    gates_hbm,
    wg_hbm,
    wu_hbm,
    wd_hbm,
    out_ref,
    tok_ref,
    gain_ref,
    ids_ref,
    gates_ref,
    rows_all,
    codes,
    gate_cols,
    wg,
    wu,
    wd,
    act,
    kept,
    part,
    merge_out,
    merge_in,
    side_out,
    side_in,
    far_out,
    far_in,
    agg_in,
    over_in,
    near_in,
    input_sem,
    weight_sem,
    pair_sem,
    code_send,
    code_recv,
    z_send,
    z_recv,
    x_send,
    x_recv,
    merge_send,
    merge_recv,
    side_send,
    side_recv,
    far_send,
    far_recv,
    agg_recv,
    over_send,
    over_recv,
    near_send,
    near_recv,
):
    ep, tp = lax.axis_index("ep"), lax.axis_index("tp")
    z, core = lax.div(ep, CORES), lax.rem(ep, CORES)
    rows, width = tok_hbm.shape
    half = rows // 2
    out_width = width // 2
    hidden = wg.shape[2]
    last = chips - 1
    partner = {"ep": z * CORES + 1 - core}
    peer = {"tp": 1 - tp}
    centre = jnp.where(2 * z < last, 1, 0)

    def chip_of(block):
        return {"ep": block * CORES + core}

    def within(block):
        return (block >= 0) & (block < chips)

    def flow(turn):
        side = centre if turn == 0 else 1 - centre
        ahead = z + 1 - 2 * side
        return side, ahead, within(ahead)

    def at(turn, distance):
        block = z + distance * (2 * flow(turn)[0] - 1)
        return block, within(block)

    def half_of(which):
        return pl.ds(pl.multiple_of(which * half, 16), half)

    small = [
        pltpu.make_async_copy(source, target, input_sem.at[i])
        for i, (source, target) in enumerate(
            (
                (gain_hbm, gain_ref),
                (ids_hbm, ids_ref),
                (gates_hbm, gates_ref),
                (tok_hbm.at[half_of(tp)], tok_ref.at[half_of(tp)]),
                (tok_hbm.at[half_of(1 - tp)], tok_ref.at[half_of(1 - tp)]),
            )
        )
    ]
    sources = (wg_hbm.at[0], wu_hbm.at[0], wd_hbm.at[0])
    loads = [
        pltpu.make_async_copy(source, target, weight_sem.at[i])
        for i, (source, target) in enumerate(
            zip(sources, (wg.at[0], wu.at[0], wd.at[pl.ds(0, hidden)]))
        )
    ]

    barrier = pltpu.get_barrier_semaphore()
    for target in (partner, peer):
        pl.semaphore_signal(barrier, inc=1, device_id=target, device_id_type=MESH)
    for turn in range(2):

        @pl.when(flow(turn)[2])
        def _(turn=turn):
            target = chip_of(flow(turn)[1])
            pl.semaphore_signal(barrier, inc=1, device_id=target, device_id_type=MESH)

    for load in small + loads:
        load.start()

    def remote(source, target, send, recv, device):
        return pltpu.make_async_remote_copy(
            src_ref=source,
            dst_ref=target,
            send_sem=send,
            recv_sem=recv,
            device_id=device,
            device_id_type=MESH,
        )

    gives = [
        remote(source, target, pair_sem.at[0, i], pair_sem.at[1, i], partner)
        for i, (source, target) in enumerate(
            zip(sources, (wg.at[1], wu.at[1], wd.at[pl.ds(hidden, hidden)]))
        )
    ]

    def normed(which):
        span = half_of(which)
        widened = tok_ref[span].astype(jnp.float32)
        scaled = widened * lax.rsqrt(jnp.mean(widened * widened, axis=-1, keepdims=True) + epsilon)
        rows_all[z, span] = (scaled * gain_ref[...]).astype(jnp.bfloat16)

    for load in small[:4]:
        load.wait()
    normed(tp)
    line = lax.broadcasted_iota(jnp.int32, (codes.shape[1], rows), 0)
    gate = jnp.zeros(line.shape, jnp.float32)
    for k in range(ids_ref.shape[0]):
        gate = gate + jnp.where(line == ids_ref[k : k + 1, :], gates_ref[k : k + 1, :], 0.0)
    codes[z] = jnp.zeros(codes.shape[1:], jnp.float32)
    codes[z, :, :rows] = gate

    neighbours = 2 + jnp.where(z > 0, 1, 0) + jnp.where(z < last, 1, 0)
    pl.semaphore_wait(barrier, neighbours)

    count = len(PIECES) - 1

    def rows_of(block, which, q):
        unit = half // PIECES[-1]
        start = pl.multiple_of(which * half + PIECES[q] * unit, 16)
        return rows_all.at[block, pl.ds(start, (PIECES[q + 1] - PIECES[q]) * unit)]

    def sender(turn, distance):
        side, _, _ = flow(turn)
        return jnp.where(side == 1, chips, z) if distance == 0 else at(turn, distance)[0]

    def z_copy(turn, distance, q):
        block = at(turn, distance)[0]
        ref = rows_of(block, tp, q)
        device = chip_of(flow(turn)[1])
        return remote(
            ref, ref, z_send.at[sender(turn, distance)], z_recv.at[block, q], device
        )

    def z_sent(turn, distance):
        ref = rows_all.at[z, half_of(tp)]
        return remote(ref, ref, z_send.at[sender(turn, distance)], z_recv.at[z, 0], peer)

    def code_copy(turn, distance):
        block = at(turn, distance)[0]
        device = chip_of(flow(turn)[1])
        return remote(
            codes.at[block],
            codes.at[block],
            code_send.at[sender(turn, distance)],
            code_recv.at[block],
            device,
        )

    def x_copy(block, which, q):
        ref = rows_of(block, which, q)
        return remote(ref, ref, x_send.at[block], x_recv.at[block], peer)

    def x_whole(block, which):
        ref = rows_all.at[block, half_of(which)]
        return remote(ref, ref, x_send.at[block], x_recv.at[block], peer)

    for q in range(count):
        for turn in range(2):

            @pl.when(flow(turn)[2])
            def _(turn=turn, q=q):
                z_copy(turn, 0, q).start()
                if q == 0:
                    code_copy(turn, 0).start()

    for give in gives:
        give.start()
    small[4].wait()
    normed(1 - tp)

    def gather_z(distance, q):
        for turn in range(2):

            @pl.when(at(turn, distance)[1])
            def _(turn=turn):
                z_copy(turn, distance, q).wait_recv()
                if q == 0:
                    code_copy(turn, distance).wait_recv()
                if distance < last:

                    @pl.when(flow(turn)[2])
                    def _():
                        z_copy(turn, distance, q).start()
                        if q == 0:
                            code_copy(turn, distance).start()

                if distance > 1 or turn == 0:
                    x_copy(at(turn, distance)[0], tp, q).start()

    waiting = [(distance, q) for distance in range(1, chips) for q in range(count)]

    def pump():
        if waiting:
            gather_z(*waiting.pop(0))

    def pump_all(distance):
        while waiting and waiting[0][0] <= distance:
            pump()

    def outer_x():
        @pl.when(at(1, 1)[1])
        def _():
            for q in range(count):
                x_copy(at(1, 1)[0], tp, q).start()

    def wait_x(distance, turn):
        @pl.when(at(turn, distance)[1])
        def _():
            x_whole(at(turn, distance)[0], 1 - tp).wait_recv()

    theirs = pl.multiple_of((1 - tp) * out_width, 128)
    mine = pl.multiple_of(tp * out_width, 128)
    parts = len(SPANS) - 1
    unit = half // SPANS[-1]
    first_half, second_half = tp, 1 - tp

    def span_of(which, s):
        start = pl.multiple_of(which * half + SPANS[s] * unit, 16)
        return pl.ds(start, (SPANS[s + 1] - SPANS[s]) * unit)

    def activate(block, start, size, slot):
        if slot == 0:
            gate_cols[...] = jnp.transpose(codes[block])
        span = pl.ds(start, size)
        turned = gate_cols[span]
        lane = lax.broadcasted_iota(jnp.int32, turned.shape, 1)
        owner = ep if slot == 0 else z * CORES + 1 - core
        weight = jnp.sum(jnp.where(lane == owner, turned, 0.0), axis=1, keepdims=True)
        held = rows_all[block, span]
        for begin in range(0, hidden, HIDDEN_TILE):
            columns = slice(begin, begin + HIDDEN_TILE)
            gate_pre = jnp.dot(held, wg[slot, :, columns], preferred_element_type=jnp.float32)
            up_pre = jnp.dot(held, wu[slot, :, columns], preferred_element_type=jnp.float32)
            gated = jnp.minimum(gate_pre, clamp_limit)
            linear = jnp.clip(up_pre, -clamp_limit, clamp_limit)
            value = gated * jax.nn.sigmoid(swish_alpha * gated) * (linear + 1.0) * weight
            act[:size, slot * hidden + begin : slot * hidden + begin + HIDDEN_TILE] = value.astype(
                jnp.bfloat16
            )

    def project(start, size):
        return jnp.dot(
            act[:size], wd[:, pl.ds(start, COLUMN_TILE)], preferred_element_type=jnp.float32
        )

    def merge_copy(side, other, which, s, block):
        span = span_of(which, s)
        return remote(
            merge_out.at[side, span],
            merge_in.at[other, span],
            merge_send.at[side],
            merge_recv.at[other, which * parts + s],
            chip_of(block),
        )

    def side_copy(block, which, s):
        span = span_of(which, s)
        return remote(
            side_out.at[block, span],
            side_in.at[block, span],
            side_send.at[block],
            side_recv.at[block, which * parts + s],
            peer,
        )

    def over_copy(side, block, which, s):
        span = span_of(which, s)
        return remote(
            side_out.at[block, span],
            over_in.at[1 - side, span],
            over_send.at[side],
            over_recv.at[1 - side, which * OVER + s],
            chip_of(block),
        )

    def far_copy(side, distance, block, which, s):
        span = span_of(which, s)
        if distance == 2:
            target = far_in.at[1 - side, span]
            receiver = far_recv.at[1 - side, which * parts + s]
            device = chip_of(block)
        else:
            target = agg_in.at[side, distance - 3, span]
            receiver = agg_recv.at[side, distance - 3, which * parts + s]
            device = chip_of(z + 2 * side - 1)
        return remote(far_out.at[block, span], target, far_send.at[block], receiver, device)

    def near_copy(side, block, which, s):
        span = span_of(which, s)
        return remote(
            far_out.at[block, span],
            near_in.at[1 - side, span],
            near_send.at[side],
            near_recv.at[1 - side, which * NEAR + s],
            chip_of(block),
        )

    def outward(turn):
        block, there = at(turn, 1)
        return there & (block + 1 - 2 * jnp.where(2 * block < last, 1, 0) == z)

    def over_there(turn):
        return at(turn, 2)[0] == jnp.where(flow(turn)[0] == 1, last, 0)

    def sent(ref, sem):
        return remote(ref, ref, sem, side_recv.at[0, 0], peer)

    def arrived(ref, sem):
        return remote(ref, ref, side_send.at[0], sem, peer)

    def outer_starts(side, block, which):
        for s in range(parts):
            if s < NEAR:
                side_copy(block, which, s).start()
            else:
                merge_copy(side, 1 - side, which, s, block).start()

    def job(distance, turn, which, pumped):
        block, there = at(turn, distance)
        side, _, through = flow(turn)
        start = pl.multiple_of(which * half, 16)

        @pl.when(there)
        def _():
            activate(block, start, half, 0)

        @pl.when(there)
        def _():
            activate(block, start, half, 1)

        if pumped:
            pump()

        @pl.when(there)
        def _():
            rows_here = half_of(which)
            if distance == 1:
                for begin in range(0, width, COLUMN_TILE):
                    merge_out[side, rows_here, begin : begin + COLUMN_TILE] = project(
                        begin, half
                    ).astype(jnp.bfloat16)
                if turn == 0:
                    for s in range(parts):
                        merge_copy(side, 1 - side, which, s, block).start()
                else:
                    for s in range(NEAR):
                        span = span_of(which, s)
                        side_out[block, span] = merge_out[side, span, pl.ds(theirs, out_width)]
                        part[block, span] = merge_out[side, span, pl.ds(mine, out_width)].astype(
                            jnp.float32
                        )
                    if which is second_half:
                        outer_starts(side, block, which)
            else:
                for begin in range(0, out_width, COLUMN_TILE):
                    side_out[block, rows_here, begin : begin + COLUMN_TILE] = project(
                        pl.multiple_of(theirs + begin, 128), half
                    ).astype(jnp.bfloat16)
                if distance == last:
                    for s in range(OVER if distance == 2 else 0, parts):
                        side_copy(block, which, s).start()
                for begin in range(0, out_width, COLUMN_TILE):
                    part[block, rows_here, begin : begin + COLUMN_TILE] = project(
                        pl.multiple_of(mine + begin, 128), half
                    )
            if distance == 2:

                @pl.when(jnp.logical_not(through))
                def _():
                    for s in range(OVER):
                        span = span_of(which, s)
                        over_copy(side, block, which, s).start()
                        far_out[block, span] = part[block, span].astype(jnp.bfloat16)
                        far_copy(side, 2, block, which, s).start()

        if pumped:
            pump()

    def outer_at(which):
        block, there = at(1, 1)
        side = flow(1)[0]

        @pl.when(there)
        def _():
            outer_starts(side, block, which)

    def near_sums():
        block, there = at(1, 1)
        side = flow(1)[0]

        @pl.when(there)
        def _():
            for which in (second_half, first_half):
                for s in range(NEAR):
                    span = span_of(which, s)
                    side_copy(block, which, s).wait_recv()
                    total = part[block, span] + side_in[block, span].astype(jnp.float32)
                    far_out[block, span] = total.astype(jnp.bfloat16)
                    near_copy(side, block, which, s).start()

    def sides_at(distance, turn, which, going):
        block, there = at(turn, distance)
        through = flow(turn)[2]

        @pl.when(there & (through if going else jnp.logical_not(through)))
        def _():
            for s in range(OVER if distance == 2 and not going else 0, parts):
                side_copy(block, which, s).start()

    def far_sums(distance, more):
        for turn in range(2):
            block, there = at(turn, distance)
            side, _, through = flow(turn)

            @pl.when(there & (through if more else jnp.logical_not(through)))
            def _(block=block, side=side):
                for which in (second_half, first_half):
                    for s in range(OVER if distance == 2 and not more else 0, parts):
                        span = span_of(which, s)
                        side_copy(block, which, s).wait_recv()
                        total = part[block, span] + side_in[block, span].astype(jnp.float32)
                        if more:
                            arrived(
                                agg_in.at[side, distance - 2, span],
                                agg_recv.at[side, distance - 2, which * parts + s],
                            ).wait_recv()
                            total = total + agg_in[side, distance - 2, span].astype(jnp.float32)
                        far_out[block, span] = total.astype(jnp.bfloat16)
                        far_copy(side, distance, block, which, s).start()

    early = jnp.logical_not(over_there(0) | over_there(1))
    for turn in range(2):
        early = early & (outward(turn) | jnp.logical_not(at(turn, 1)[1]))

    def own_send(which, s):
        span = span_of(which, s)
        side_out[z, span] = kept[span, pl.ds(theirs, out_width)].astype(jnp.bfloat16)
        side_copy(z, which, s).start()

    def own_early(which):
        @pl.when(early)
        def _():
            for s in range(NEAR):
                own_send(which, s)

    def own_span(which, s):
        span = span_of(which, s)
        for turn in range(2):
            merged = at(turn, 1)[1]
            if s < NEAR:
                merged = merged & jnp.logical_not(outward(turn))

            @pl.when(merged)
            def _(turn=turn):
                side = flow(turn)[0]
                arrived(
                    merge_in.at[side, span], merge_recv.at[side, which * parts + s]
                ).wait_recv()
                kept[span] = kept[span] + merge_in[side, span].astype(jnp.float32)

            if s < OVER and chips > 2:

                @pl.when(over_there(turn))
                def _(turn=turn):
                    side = flow(turn)[0]
                    arrived(
                        over_in.at[side, span], over_recv.at[side, which * OVER + s]
                    ).wait_recv()
                    here = (span, pl.ds(theirs, out_width))
                    kept[here] = kept[here] + over_in[side, span].astype(jnp.float32)

        own_send(which, s)

    def own_exchange():
        for which in (first_half, second_half):
            for s in range(parts):
                if s < NEAR:

                    @pl.when(jnp.logical_not(early))
                    def _():
                        own_span(which, s)

                else:
                    own_span(which, s)

    def finish():
        for which in (second_half, first_half):
            for s in range(parts):
                span = span_of(which, s)
                here = (span, pl.ds(mine, out_width))
                if chips > 2:
                    for turn in range(2):

                        @pl.when(at(turn, 2)[1])
                        def _(turn=turn):
                            side = flow(turn)[0]
                            arrived(
                                far_in.at[side, span], far_recv.at[side, which * parts + s]
                            ).wait_recv()
                            kept[here] = kept[here] + far_in[side, span].astype(jnp.float32)

                if s < NEAR:
                    for turn in range(2):

                        @pl.when(outward(turn))
                        def _(turn=turn):
                            side = flow(turn)[0]
                            arrived(
                                near_in.at[side, span], near_recv.at[side, which * NEAR + s]
                            ).wait_recv()
                            kept[here] = kept[here] + near_in[side, span].astype(jnp.float32)

                side_copy(z, which, s).wait_recv()
                out_ref[span] = (kept[here] + side_in[z, span].astype(jnp.float32)).astype(
                    jnp.bfloat16
                )

    for load in loads[:2]:
        load.wait()
    pump()
    activate(z, 0, rows, 0)
    for _ in range(count - 2):
        pump()
    for give in gives[:2]:
        give.wait_recv()
    activate(z, 0, rows, 1)
    pump_all(1)
    outer_x()
    loads[2].wait()
    gives[2].wait_recv()
    for begin in range(0, width, COLUMN_TILE):
        kept[:, begin : begin + COLUMN_TILE] = project(begin, rows)

    outer = range(1, last // 2 + 1)
    job(1, 0, first_half, True)
    for distance in range(1, chips):
        if distance in outer:
            job(distance, 1, first_half, False)
        wait_x(distance, 0)
        job(distance, 0, second_half, distance < last)
        if 1 < distance < last:
            sides_at(distance, 0, second_half, True)
        if distance < last:
            pump_all(distance + 1)
            if distance == 1:
                outer_at(first_half)
            job(distance + 1, 0, first_half, True)
            if distance + 1 < last:
                sides_at(distance + 1, 0, first_half, True)
            if distance + 1 == last:
                own_early(first_half)
        if distance in outer:
            wait_x(distance, 1)
            job(distance, 1, second_half, False)
            if distance > 1:
                for which in (first_half, second_half):
                    for going in (True, False):
                        sides_at(distance, 1, which, going)
    if last == 1:
        own_early(first_half)
    for distance in range(last - 1, 1, -1):
        for which in (first_half, second_half):
            sides_at(distance, 0, which, False)
    own_early(second_half)
    near_sums()
    if last > 1:
        far_sums(last, False)
    own_exchange()
    for distance in range(last - 1, 1, -1):
        far_sums(distance, False)
        far_sums(distance, True)

    for give in gives:
        give.wait_send()
    for turn in range(2):
        for distance in range(chips):
            if distance < last:

                @pl.when(at(turn, distance)[1] & flow(turn)[2])
                def _(turn=turn, distance=distance):
                    z_sent(turn, distance).wait_send()
                    code_copy(turn, distance).wait_send()

            if distance > 0:

                @pl.when(at(turn, distance)[1])
                def _(turn=turn, distance=distance):
                    x_whole(at(turn, distance)[0], tp).wait_send()

        @pl.when(at(turn, 1)[1])
        def _(turn=turn):
            side = flow(turn)[0]
            near_rows = 2 * SPANS[NEAR] * unit if turn == 1 else 0
            whole = merge_out.at[side, pl.ds(0, rows - near_rows)]
            sent(whole, merge_send.at[side]).wait_send()
            if turn == 1:
                block = at(turn, 1)[0]
                sent(side_out.at[block, pl.ds(0, near_rows)], side_send.at[block]).wait_send()
                sent(far_out.at[block, pl.ds(0, near_rows)], near_send.at[side]).wait_send()

    finish()
    sent(side_out.at[z], side_send.at[z]).wait_send()
    short = 2 * SPANS[OVER] * unit
    for turn in range(2):
        side, _, through = flow(turn)
        for distance in range(2, chips):
            block, there = at(turn, distance)
            whole = there & through if distance == 2 else there

            @pl.when(whole)
            def _(block=block):
                sent(side_out.at[block], side_send.at[block]).wait_send()

            if distance == 2:

                @pl.when(there & jnp.logical_not(through))
                def _(block=block, side=side):
                    rest = side_out.at[block, pl.ds(0, rows - short)]
                    sent(rest, side_send.at[block]).wait_send()
                    sent(side_out.at[block, pl.ds(0, short)], over_send.at[side]).wait_send()

            @pl.when(there)
            def _(block=block):
                sent(far_out.at[block], far_send.at[block]).wait_send()


def fused(tokens, norm_gain, w_gate, w_up, w_down, expert_ids, gate_weights):
    rows, width = tokens.shape
    top_count = expert_ids.shape[1]
    chips = lax.axis_size("ep") // CORES
    experts_all = chips * CORES
    lines = experts_all + -experts_all % 8
    hidden = w_gate.shape[2]
    out_width = width // 2
    last = chips - 1
    aggregates = max(last - 2, 1)
    lanes = rows + -rows % 128
    spans = 2 * (len(SPANS) - 1)
    anywhere = pl.BlockSpec(memory_space=pl.ANY)
    vmem, dma = pltpu.VMEM, pltpu.SemaphoreType.DMA
    return pl.pallas_call(
        functools.partial(fused_kernel, chips),
        out_shape=vmem((rows, out_width), jnp.bfloat16),
        in_specs=[anywhere] * 7,
        out_specs=pl.BlockSpec(memory_space=vmem),
        scratch_shapes=[
            vmem((rows, width), jnp.bfloat16),
            vmem((1, width), jnp.float32),
            vmem((top_count, rows), jnp.int32),
            vmem((top_count, rows), jnp.float32),
            vmem((chips, rows, width), jnp.bfloat16),
            vmem((chips, lines, lanes), jnp.float32),
            vmem((lanes, lines), jnp.float32),
            vmem((CORES, width, hidden), jnp.bfloat16),
            vmem((CORES, width, hidden), jnp.bfloat16),
            vmem((CORES * hidden, width), jnp.bfloat16),
            vmem((rows, CORES * hidden), jnp.bfloat16),
            vmem((rows, width), jnp.float32),
            vmem((chips, rows, out_width), jnp.float32),
            vmem((2, rows, width), jnp.bfloat16),
            vmem((2, rows, width), jnp.bfloat16),
            vmem((chips, rows, out_width), jnp.bfloat16),
            vmem((chips, rows, out_width), jnp.bfloat16),
            vmem((chips, rows, out_width), jnp.bfloat16),
            vmem((2, rows, out_width), jnp.bfloat16),
            vmem((2, aggregates, rows, out_width), jnp.bfloat16),
            vmem((2, rows, out_width), jnp.bfloat16),
            vmem((2, rows, out_width), jnp.bfloat16),
            dma((5,)),
            dma((3,)),
            dma((2, 3)),
            dma((chips + 1,)),
            dma((chips,)),
            dma((chips + 1,)),
            dma((chips, len(PIECES) - 1)),
            dma((chips,)),
            dma((chips,)),
            dma((2,)),
            dma((2, spans)),
            dma((chips,)),
            dma((chips, spans)),
            dma((chips,)),
            dma((2, spans)),
            dma((2, aggregates, spans)),
            dma((2,)),
            dma((2, 2 * OVER)),
            dma((2,)),
            dma((2, 2 * NEAR)),
        ],
        compiler_params=pltpu.CompilerParams(collective_id=0, has_side_effects=True),
    )(tokens, norm_gain[None, :], expert_ids.T, gate_weights.T, w_gate, w_up, w_down)


def step(mesh, *arrays):
    tokens, norm_gain, w_gate, w_up, w_down, expert_ids, gate_weights = arrays
    ep_count, tp_count = mesh.shape["ep"], mesh.shape["tp"]
    rows, top_count = expert_ids.shape
    experts_all = ep_count * w_gate.shape[0]
    capacity = min(rows, rows * top_count * 4 // (3 * experts_all))
    dense = (
        w_gate.shape[0] == 1
        and tp_count == 2
        and ep_count % CORES == 0
        and ep_count > CORES
        and rows <= 2 * capacity
        and rows % (32 * PIECES[-1]) == 0
        and rows % (32 * SPANS[-1]) == 0
    )
    return fused(*arrays) if dense else body(*arrays)


def solution(mesh):
    placed = (
        P(("grp", "ep"), None),
        P(),
        P("ep", None, "tp"),
        P("ep", None, "tp"),
        P("ep", "tp", None),
        P(("grp", "ep"), None),
        P(("grp", "ep"), None),
    )
    return jax.shard_map(
        functools.partial(step, mesh), mesh=mesh, in_specs=placed, out_specs=P(("grp", "ep"), "tp"), check_vma=False
    )
```

```python
import functools

import jax
import jax.numpy as jnp
from jax import lax
from jax.experimental import pallas as pl
from jax.experimental.pallas import tpu as pltpu
from jax.sharding import PartitionSpec as P

epsilon = 1e-06
clamp_limit = 7.0
swish_alpha = 1.702


def rms_norm(tokens, norm_gain):
    widened = tokens.astype(jnp.float32)
    scaled = widened * lax.rsqrt(jnp.mean(widened * widened, axis=-1, keepdims=True) + epsilon)
    return (scaled * norm_gain).astype(jnp.bfloat16)


def body(tokens, norm_gain, w_gate, w_up, w_down, expert_ids, gate_weights):
    tok_rows, model_width = tokens.shape
    top_count = expert_ids.shape[1]
    ep_count = lax.axis_size("ep")
    local_experts = w_gate.shape[0]
    experts_all = local_experts * ep_count
    capacity = min(tok_rows, tok_rows * top_count * 4 // (3 * experts_all))
    normed = rms_norm(tokens, norm_gain)
    flat_ids = expert_ids.reshape(-1)
    onehot = (flat_ids[:, None] == jnp.arange(experts_all, dtype=jnp.int32)[None, :]).astype(
        jnp.int32
    )
    before = jnp.cumsum(onehot, axis=0) - onehot
    slot_index = jnp.sum(before * onehot, axis=1)
    dest_row = flat_ids * capacity + slot_index
    owner_tok = jnp.arange(tok_rows * top_count, dtype=jnp.int32) // top_count
    slot_table = (
        jnp.full((experts_all * capacity,), tok_rows, jnp.int32).at[dest_row].set(owner_tok)
    )
    padded = jnp.concatenate([normed, jnp.zeros((1, model_width), jnp.bfloat16)], axis=0)
    send_buffer = padded[slot_table].reshape(experts_all, capacity, model_width)
    received = lax.all_to_all(send_buffer, "ep", split_axis=0, concat_axis=0, tiled=True)
    expert_rows = received.reshape(ep_count, local_experts, capacity, model_width)
    gate_pre = jnp.einsum("sjcd,jdf->sjcf", expert_rows, w_gate, preferred_element_type=jnp.float32)
    up_pre = jnp.einsum("sjcd,jdf->sjcf", expert_rows, w_up, preferred_element_type=jnp.float32)
    gated = jnp.minimum(gate_pre, clamp_limit)
    linear = jnp.clip(up_pre, -clamp_limit, clamp_limit)
    activated = (gated * jax.nn.sigmoid(swish_alpha * gated) * (linear + 1.0)).astype(jnp.bfloat16)
    partial_value = jnp.einsum(
        "sjcf,jfd->sjcd", activated, w_down, preferred_element_type=jnp.float32
    ).astype(jnp.bfloat16)
    summed = (
        lax.psum_scatter(partial_value, "tp", scatter_dimension=3, tiled=True)
        .astype(jnp.float32)
        .astype(jnp.bfloat16)
    )
    returned = lax.all_to_all(summed, "ep", split_axis=0, concat_axis=0, tiled=True)
    returned = returned.reshape(experts_all * capacity, returned.shape[3])
    picked = returned[dest_row].reshape(tok_rows, top_count, returned.shape[1]).astype(jnp.float32)
    return jnp.sum(picked * gate_weights[:, :, None], axis=1).astype(jnp.bfloat16)


MESH = pl.DeviceIdType.MESH
CORES = 2
PIECES = (0, 1, 3, 5, 6)
SPANS = (0, 1, 2, 3)
OVER = 1
NEAR = 1
HIDDEN_TILE = 256
COLUMN_TILE = 512


def fused_kernel(
    chips,
    tok_hbm,
    gain_hbm,
    ids_hbm,
    gates_hbm,
    wg_hbm,
    wu_hbm,
    wd_hbm,
    out_ref,
    tok_ref,
    gain_ref,
    ids_ref,
    gates_ref,
    rows_all,
    codes,
    gate_cols,
    wg,
    wu,
    wd,
    act,
    kept,
    part,
    merge_out,
    merge_in,
    side_out,
    side_in,
    far_out,
    far_in,
    agg_in,
    over_in,
    near_in,
    input_sem,
    weight_sem,
    pair_sem,
    code_send,
    code_recv,
    z_send,
    z_recv,
    x_send,
    x_recv,
    merge_send,
    merge_recv,
    side_send,
    side_recv,
    far_send,
    far_recv,
    agg_recv,
    over_send,
    over_recv,
    near_send,
    near_recv,
):
    ep, tp = lax.axis_index("ep"), lax.axis_index("tp")
    z, core = lax.div(ep, CORES), lax.rem(ep, CORES)
    rows, width = tok_hbm.shape
    half = rows // 2
    out_width = width // 2
    hidden = wg.shape[2]
    last = chips - 1
    partner = {"ep": z * CORES + 1 - core}
    peer = {"tp": 1 - tp}
    centre = jnp.where(2 * z < last, 1, 0)

    def chip_of(block):
        return {"ep": block * CORES + core}

    def within(block):
        return (block >= 0) & (block < chips)

    def flow(turn):
        side = centre if turn == 0 else 1 - centre
        ahead = z + 1 - 2 * side
        return side, ahead, within(ahead)

    def at(turn, distance):
        block = z + distance * (2 * flow(turn)[0] - 1)
        return block, within(block)

    def half_of(which):
        return pl.ds(pl.multiple_of(which * half, 16), half)

    small = [
        pltpu.make_async_copy(source, target, input_sem.at[i])
        for i, (source, target) in enumerate(
            (
                (gain_hbm, gain_ref),
                (ids_hbm, ids_ref),
                (gates_hbm, gates_ref),
                (tok_hbm.at[half_of(tp)], tok_ref.at[half_of(tp)]),
                (tok_hbm.at[half_of(1 - tp)], tok_ref.at[half_of(1 - tp)]),
            )
        )
    ]
    sources = (wg_hbm.at[0], wu_hbm.at[0], wd_hbm.at[0])
    loads = [
        pltpu.make_async_copy(source, target, weight_sem.at[i])
        for i, (source, target) in enumerate(
            zip(sources, (wg.at[0], wu.at[0], wd.at[pl.ds(0, hidden)]))
        )
    ]

    barrier = pltpu.get_barrier_semaphore()
    for target in (partner, peer):
        pl.semaphore_signal(barrier, inc=1, device_id=target, device_id_type=MESH)
    for turn in range(2):

        @pl.when(flow(turn)[2])
        def _(turn=turn):
            target = chip_of(flow(turn)[1])
            pl.semaphore_signal(barrier, inc=1, device_id=target, device_id_type=MESH)

    for load in small:
        load.start()

    def remote(source, target, send, recv, device):
        return pltpu.make_async_remote_copy(
            src_ref=source,
            dst_ref=target,
            send_sem=send,
            recv_sem=recv,
            device_id=device,
            device_id_type=MESH,
        )

    gives = [
        remote(source, target, pair_sem.at[0, i], pair_sem.at[1, i], partner)
        for i, (source, target) in enumerate(
            zip(sources, (wg.at[1], wu.at[1], wd.at[pl.ds(hidden, hidden)]))
        )
    ]

    def normed(which):
        span = half_of(which)
        widened = tok_ref[span].astype(jnp.float32)
        scaled = widened * lax.rsqrt(jnp.mean(widened * widened, axis=-1, keepdims=True) + epsilon)
        rows_all[z, span] = (scaled * gain_ref[...]).astype(jnp.bfloat16)

    for load in small[:4]:
        load.wait()
    for load in loads:
        load.start()
    normed(tp)
    line = lax.broadcasted_iota(jnp.int32, (codes.shape[1], rows), 0)
    gate = jnp.zeros(line.shape, jnp.float32)
    for k in range(ids_ref.shape[0]):
        gate = gate + jnp.where(line == ids_ref[k : k + 1, :], gates_ref[k : k + 1, :], 0.0)
    codes[z] = jnp.zeros(codes.shape[1:], jnp.float32)
    codes[z, :, :rows] = gate

    neighbours = 2 + jnp.where(z > 0, 1, 0) + jnp.where(z < last, 1, 0)
    pl.semaphore_wait(barrier, neighbours)

    count = len(PIECES) - 1

    def rows_of(block, which, q):
        unit = half // PIECES[-1]
        start = pl.multiple_of(which * half + PIECES[q] * unit, 16)
        return rows_all.at[block, pl.ds(start, (PIECES[q + 1] - PIECES[q]) * unit)]

    def sender(turn, distance):
        side, _, _ = flow(turn)
        return jnp.where(side == 1, chips, z) if distance == 0 else at(turn, distance)[0]

    def z_copy(turn, distance, q):
        block = at(turn, distance)[0]
        ref = rows_of(block, tp, q)
        device = chip_of(flow(turn)[1])
        return remote(
            ref, ref, z_send.at[sender(turn, distance)], z_recv.at[block, q], device
        )

    def z_sent(turn, distance):
        ref = rows_all.at[z, half_of(tp)]
        return remote(ref, ref, z_send.at[sender(turn, distance)], z_recv.at[z, 0], peer)

    def code_copy(turn, distance):
        block = at(turn, distance)[0]
        device = chip_of(flow(turn)[1])
        return remote(
            codes.at[block],
            codes.at[block],
            code_send.at[sender(turn, distance)],
            code_recv.at[block],
            device,
        )

    def x_copy(block, which, q):
        ref = rows_of(block, which, q)
        return remote(ref, ref, x_send.at[block], x_recv.at[block], peer)

    def x_whole(block, which):
        ref = rows_all.at[block, half_of(which)]
        return remote(ref, ref, x_send.at[block], x_recv.at[block], peer)

    for q in range(count):
        for turn in range(2):

            @pl.when(flow(turn)[2])
            def _(turn=turn, q=q):
                z_copy(turn, 0, q).start()
                if q == 0:
                    code_copy(turn, 0).start()

    for give in gives:
        give.start()
    small[4].wait()
    normed(1 - tp)

    def gather_z(distance, q):
        for turn in range(2):

            @pl.when(at(turn, distance)[1])
            def _(turn=turn):
                z_copy(turn, distance, q).wait_recv()
                if q == 0:
                    code_copy(turn, distance).wait_recv()
                if distance < last:

                    @pl.when(flow(turn)[2])
                    def _():
                        z_copy(turn, distance, q).start()
                        if q == 0:
                            code_copy(turn, distance).start()

                if distance > 1 or turn == 0:
                    x_copy(at(turn, distance)[0], tp, q).start()

    waiting = [(distance, q) for distance in range(1, chips) for q in range(count)]

    def pump():
        if waiting:
            gather_z(*waiting.pop(0))

    def pump_all(distance):
        while waiting and waiting[0][0] <= distance:
            pump()

    def outer_x():
        @pl.when(at(1, 1)[1])
        def _():
            for q in range(count):
                x_copy(at(1, 1)[0], tp, q).start()

    def wait_x(distance, turn):
        @pl.when(at(turn, distance)[1])
        def _():
            x_whole(at(turn, distance)[0], 1 - tp).wait_recv()

    theirs = pl.multiple_of((1 - tp) * out_width, 128)
    mine = pl.multiple_of(tp * out_width, 128)
    parts = len(SPANS) - 1
    unit = half // SPANS[-1]
    first_half, second_half = tp, 1 - tp

    def span_of(which, s):
        start = pl.multiple_of(which * half + SPANS[s] * unit, 16)
        return pl.ds(start, (SPANS[s + 1] - SPANS[s]) * unit)

    def activate(block, start, size, slot):
        if slot == 0:
            gate_cols[...] = jnp.transpose(codes[block])
        span = pl.ds(start, size)
        turned = gate_cols[span]
        lane = lax.broadcasted_iota(jnp.int32, turned.shape, 1)
        owner = ep if slot == 0 else z * CORES + 1 - core
        weight = jnp.sum(jnp.where(lane == owner, turned, 0.0), axis=1, keepdims=True)
        held = rows_all[block, span]
        for begin in range(0, hidden, HIDDEN_TILE):
            columns = slice(begin, begin + HIDDEN_TILE)
            gate_pre = jnp.dot(held, wg[slot, :, columns], preferred_element_type=jnp.float32)
            up_pre = jnp.dot(held, wu[slot, :, columns], preferred_element_type=jnp.float32)
            gated = jnp.minimum(gate_pre, clamp_limit)
            linear = jnp.clip(up_pre, -clamp_limit, clamp_limit)
            value = gated * jax.nn.sigmoid(swish_alpha * gated) * (linear + 1.0) * weight
            act[:size, slot * hidden + begin : slot * hidden + begin + HIDDEN_TILE] = value.astype(
                jnp.bfloat16
            )

    def project(start, size):
        return jnp.dot(
            act[:size], wd[:, pl.ds(start, COLUMN_TILE)], preferred_element_type=jnp.float32
        )

    def merge_copy(side, other, which, s, block):
        span = span_of(which, s)
        return remote(
            merge_out.at[side, span],
            merge_in.at[other, span],
            merge_send.at[side],
            merge_recv.at[other, which * parts + s],
            chip_of(block),
        )

    def side_copy(block, which, s):
        span = span_of(which, s)
        return remote(
            side_out.at[block, span],
            side_in.at[block, span],
            side_send.at[block],
            side_recv.at[block, which * parts + s],
            peer,
        )

    def over_copy(side, block, which, s):
        span = span_of(which, s)
        return remote(
            side_out.at[block, span],
            over_in.at[1 - side, span],
            over_send.at[side],
            over_recv.at[1 - side, which * OVER + s],
            chip_of(block),
        )

    def far_copy(side, distance, block, which, s):
        span = span_of(which, s)
        if distance == 2:
            target = far_in.at[1 - side, span]
            receiver = far_recv.at[1 - side, which * parts + s]
            device = chip_of(block)
        else:
            target = agg_in.at[side, distance - 3, span]
            receiver = agg_recv.at[side, distance - 3, which * parts + s]
            device = chip_of(z + 2 * side - 1)
        return remote(far_out.at[block, span], target, far_send.at[block], receiver, device)

    def near_copy(side, block, which, s):
        span = span_of(which, s)
        return remote(
            far_out.at[block, span],
            near_in.at[1 - side, span],
            near_send.at[side],
            near_recv.at[1 - side, which * NEAR + s],
            chip_of(block),
        )

    def outward(turn):
        block, there = at(turn, 1)
        return there & (block + 1 - 2 * jnp.where(2 * block < last, 1, 0) == z)

    def over_there(turn):
        return at(turn, 2)[0] == jnp.where(flow(turn)[0] == 1, last, 0)

    def sent(ref, sem):
        return remote(ref, ref, sem, side_recv.at[0, 0], peer)

    def arrived(ref, sem):
        return remote(ref, ref, side_send.at[0], sem, peer)

    def outer_starts(side, block, which):
        for s in range(parts):
            if s < NEAR:
                side_copy(block, which, s).start()
            else:
                merge_copy(side, 1 - side, which, s, block).start()

    def job(distance, turn, which, pumped):
        block, there = at(turn, distance)
        side, _, through = flow(turn)
        start = pl.multiple_of(which * half, 16)

        @pl.when(there)
        def _():
            activate(block, start, half, 0)

        @pl.when(there)
        def _():
            activate(block, start, half, 1)

        if pumped:
            pump()

        @pl.when(there)
        def _():
            rows_here = half_of(which)
            if distance == 1:
                for begin in range(0, width, COLUMN_TILE):
                    merge_out[side, rows_here, begin : begin + COLUMN_TILE] = project(
                        begin, half
                    ).astype(jnp.bfloat16)
                if turn == 0:
                    for s in range(parts):
                        merge_copy(side, 1 - side, which, s, block).start()
                else:
                    for s in range(NEAR):
                        span = span_of(which, s)
                        side_out[block, span] = merge_out[side, span, pl.ds(theirs, out_width)]
                        part[block, span] = merge_out[side, span, pl.ds(mine, out_width)].astype(
                            jnp.float32
                        )
                    if which is second_half:
                        outer_starts(side, block, which)
            else:
                for begin in range(0, out_width, COLUMN_TILE):
                    side_out[block, rows_here, begin : begin + COLUMN_TILE] = project(
                        pl.multiple_of(theirs + begin, 128), half
                    ).astype(jnp.bfloat16)
                if distance == last:
                    for s in range(OVER if distance == 2 else 0, parts):
                        side_copy(block, which, s).start()
                for begin in range(0, out_width, COLUMN_TILE):
                    part[block, rows_here, begin : begin + COLUMN_TILE] = project(
                        pl.multiple_of(mine + begin, 128), half
                    )
            if distance == 2:

                @pl.when(jnp.logical_not(through))
                def _():
                    for s in range(OVER):
                        span = span_of(which, s)
                        over_copy(side, block, which, s).start()
                        far_out[block, span] = part[block, span].astype(jnp.bfloat16)
                        far_copy(side, 2, block, which, s).start()

        if pumped:
            pump()

    def outer_at(which):
        block, there = at(1, 1)
        side = flow(1)[0]

        @pl.when(there)
        def _():
            outer_starts(side, block, which)

    def near_sums():
        block, there = at(1, 1)
        side = flow(1)[0]

        @pl.when(there)
        def _():
            for which in (second_half, first_half):
                for s in range(NEAR):
                    span = span_of(which, s)
                    side_copy(block, which, s).wait_recv()
                    total = part[block, span] + side_in[block, span].astype(jnp.float32)
                    far_out[block, span] = total.astype(jnp.bfloat16)
                    near_copy(side, block, which, s).start()

    def sides_at(distance, turn, which, going):
        block, there = at(turn, distance)
        through = flow(turn)[2]

        @pl.when(there & (through if going else jnp.logical_not(through)))
        def _():
            for s in range(OVER if distance == 2 and not going else 0, parts):
                side_copy(block, which, s).start()

    def far_sums(distance, more, halves):
        for turn in range(2):
            block, there = at(turn, distance)
            side, _, through = flow(turn)

            @pl.when(there & (through if more else jnp.logical_not(through)))
            def _(block=block, side=side):
                for which in halves:
                    for s in range(OVER if distance == 2 and not more else 0, parts):
                        span = span_of(which, s)
                        side_copy(block, which, s).wait_recv()
                        total = part[block, span] + side_in[block, span].astype(jnp.float32)
                        if more:
                            arrived(
                                agg_in.at[side, distance - 2, span],
                                agg_recv.at[side, distance - 2, which * parts + s],
                            ).wait_recv()
                            total = total + agg_in[side, distance - 2, span].astype(jnp.float32)
                        far_out[block, span] = total.astype(jnp.bfloat16)
                        far_copy(side, distance, block, which, s).start()

    early = jnp.logical_not(over_there(0) | over_there(1))
    for turn in range(2):
        early = early & (outward(turn) | jnp.logical_not(at(turn, 1)[1]))

    def own_send(which, s):
        span = span_of(which, s)
        side_out[z, span] = kept[span, pl.ds(theirs, out_width)].astype(jnp.bfloat16)
        side_copy(z, which, s).start()

    def own_early(which):
        @pl.when(early)
        def _():
            for s in range(NEAR):
                own_send(which, s)

    def own_span(which, s):
        span = span_of(which, s)
        for turn in range(2):
            merged = at(turn, 1)[1]
            if s < NEAR:
                merged = merged & jnp.logical_not(outward(turn))

            @pl.when(merged)
            def _(turn=turn):
                side = flow(turn)[0]
                arrived(
                    merge_in.at[side, span], merge_recv.at[side, which * parts + s]
                ).wait_recv()
                kept[span] = kept[span] + merge_in[side, span].astype(jnp.float32)

            if s < OVER and chips > 2:

                @pl.when(over_there(turn))
                def _(turn=turn):
                    side = flow(turn)[0]
                    arrived(
                        over_in.at[side, span], over_recv.at[side, which * OVER + s]
                    ).wait_recv()
                    here = (span, pl.ds(theirs, out_width))
                    kept[here] = kept[here] + over_in[side, span].astype(jnp.float32)

        own_send(which, s)

    def own_exchange():
        for which in (first_half, second_half):
            for s in range(parts):
                if s < NEAR:

                    @pl.when(jnp.logical_not(early))
                    def _():
                        own_span(which, s)

                else:
                    own_span(which, s)

    def finish():
        for which in (second_half, first_half):
            for s in range(parts):
                span = span_of(which, s)
                here = (span, pl.ds(mine, out_width))
                if chips > 2:
                    for turn in range(2):

                        @pl.when(at(turn, 2)[1])
                        def _(turn=turn):
                            side = flow(turn)[0]
                            arrived(
                                far_in.at[side, span], far_recv.at[side, which * parts + s]
                            ).wait_recv()
                            kept[here] = kept[here] + far_in[side, span].astype(jnp.float32)

                if s < NEAR:
                    for turn in range(2):

                        @pl.when(outward(turn))
                        def _(turn=turn):
                            side = flow(turn)[0]
                            arrived(
                                near_in.at[side, span], near_recv.at[side, which * NEAR + s]
                            ).wait_recv()
                            kept[here] = kept[here] + near_in[side, span].astype(jnp.float32)

                side_copy(z, which, s).wait_recv()
                out_ref[span] = (kept[here] + side_in[z, span].astype(jnp.float32)).astype(
                    jnp.bfloat16
                )

    for load in loads[:2]:
        load.wait()
    pump()
    activate(z, 0, rows, 0)
    for _ in range(count - 2):
        pump()
    for give in gives[:2]:
        give.wait_recv()
    activate(z, 0, rows, 1)
    pump_all(1)
    outer_x()
    loads[2].wait()
    gives[2].wait_recv()
    for begin in range(0, width, COLUMN_TILE):
        kept[:, begin : begin + COLUMN_TILE] = project(begin, rows)

    outer = range(1, last // 2 + 1)
    job(1, 0, first_half, True)
    for distance in range(1, chips):
        if distance in outer:
            job(distance, 1, first_half, False)
        wait_x(distance, 0)
        job(distance, 0, second_half, distance < last)
        if 1 < distance < last:
            sides_at(distance, 0, second_half, True)
        if distance < last:
            pump_all(distance + 1)
            if distance == 1:
                outer_at(first_half)
            job(distance + 1, 0, first_half, True)
            if distance + 1 < last:
                sides_at(distance + 1, 0, first_half, True)
            if distance + 1 == last:
                own_early(first_half)
        if distance in outer:
            wait_x(distance, 1)
            job(distance, 1, second_half, False)
            if distance > 1:
                for which in (first_half, second_half):
                    for going in (True, False):
                        sides_at(distance, 1, which, going)
    if last == 1:
        own_early(first_half)
    for distance in range(last - 1, 1, -1):
        for which in (first_half, second_half):
            sides_at(distance, 0, which, False)
    own_early(second_half)
    both = (second_half, first_half)
    if last > 1:
        far_sums(last, False, both)
    own_exchange()
    for distance in range(last - 1, 1, -1):
        far_sums(distance, False, both)
        if distance > 2:
            far_sums(distance, True, both)
    far_sums(2, True, both[:1])
    near_sums()
    far_sums(2, True, both[1:])

    for give in gives:
        give.wait_send()
    for turn in range(2):
        for distance in range(chips):
            if distance < last:

                @pl.when(at(turn, distance)[1] & flow(turn)[2])
                def _(turn=turn, distance=distance):
                    z_sent(turn, distance).wait_send()
                    code_copy(turn, distance).wait_send()

            if distance > 0:

                @pl.when(at(turn, distance)[1])
                def _(turn=turn, distance=distance):
                    x_whole(at(turn, distance)[0], tp).wait_send()

        @pl.when(at(turn, 1)[1])
        def _(turn=turn):
            side = flow(turn)[0]
            near_rows = 2 * SPANS[NEAR] * unit if turn == 1 else 0
            whole = merge_out.at[side, pl.ds(0, rows - near_rows)]
            sent(whole, merge_send.at[side]).wait_send()
            if turn == 1:
                block = at(turn, 1)[0]
                sent(side_out.at[block, pl.ds(0, near_rows)], side_send.at[block]).wait_send()
                sent(far_out.at[block, pl.ds(0, near_rows)], near_send.at[side]).wait_send()

    finish()
    sent(side_out.at[z], side_send.at[z]).wait_send()
    short = 2 * SPANS[OVER] * unit
    for turn in range(2):
        side, _, through = flow(turn)
        for distance in range(2, chips):
            block, there = at(turn, distance)
            whole = there & through if distance == 2 else there

            @pl.when(whole)
            def _(block=block):
                sent(side_out.at[block], side_send.at[block]).wait_send()

            if distance == 2:

                @pl.when(there & jnp.logical_not(through))
                def _(block=block, side=side):
                    rest = side_out.at[block, pl.ds(0, rows - short)]
                    sent(rest, side_send.at[block]).wait_send()
                    sent(side_out.at[block, pl.ds(0, short)], over_send.at[side]).wait_send()

            @pl.when(there)
            def _(block=block):
                sent(far_out.at[block], far_send.at[block]).wait_send()


def fused(tokens, norm_gain, w_gate, w_up, w_down, expert_ids, gate_weights):
    rows, width = tokens.shape
    top_count = expert_ids.shape[1]
    chips = lax.axis_size("ep") // CORES
    experts_all = chips * CORES
    lines = experts_all + -experts_all % 8
    hidden = w_gate.shape[2]
    out_width = width // 2
    last = chips - 1
    aggregates = max(last - 2, 1)
    lanes = rows + -rows % 128
    spans = 2 * (len(SPANS) - 1)
    anywhere = pl.BlockSpec(memory_space=pl.ANY)
    vmem, dma = pltpu.VMEM, pltpu.SemaphoreType.DMA
    return pl.pallas_call(
        functools.partial(fused_kernel, chips),
        out_shape=vmem((rows, out_width), jnp.bfloat16),
        in_specs=[anywhere] * 7,
        out_specs=pl.BlockSpec(memory_space=vmem),
        scratch_shapes=[
            vmem((rows, width), jnp.bfloat16),
            vmem((1, width), jnp.float32),
            vmem((top_count, rows), jnp.int32),
            vmem((top_count, rows), jnp.float32),
            vmem((chips, rows, width), jnp.bfloat16),
            vmem((chips, lines, lanes), jnp.float32),
            vmem((lanes, lines), jnp.float32),
            vmem((CORES, width, hidden), jnp.bfloat16),
            vmem((CORES, width, hidden), jnp.bfloat16),
            vmem((CORES * hidden, width), jnp.bfloat16),
            vmem((rows, CORES * hidden), jnp.bfloat16),
            vmem((rows, width), jnp.float32),
            vmem((chips, rows, out_width), jnp.float32),
            vmem((2, rows, width), jnp.bfloat16),
            vmem((2, rows, width), jnp.bfloat16),
            vmem((chips, rows, out_width), jnp.bfloat16),
            vmem((chips, rows, out_width), jnp.bfloat16),
            vmem((chips, rows, out_width), jnp.bfloat16),
            vmem((2, rows, out_width), jnp.bfloat16),
            vmem((2, aggregates, rows, out_width), jnp.bfloat16),
            vmem((2, rows, out_width), jnp.bfloat16),
            vmem((2, rows, out_width), jnp.bfloat16),
            dma((5,)),
            dma((3,)),
            dma((2, 3)),
            dma((chips + 1,)),
            dma((chips,)),
            dma((chips + 1,)),
            dma((chips, len(PIECES) - 1)),
            dma((chips,)),
            dma((chips,)),
            dma((2,)),
            dma((2, spans)),
            dma((chips,)),
            dma((chips, spans)),
            dma((chips,)),
            dma((2, spans)),
            dma((2, aggregates, spans)),
            dma((2,)),
            dma((2, 2 * OVER)),
            dma((2,)),
            dma((2, 2 * NEAR)),
        ],
        compiler_params=pltpu.CompilerParams(collective_id=0, has_side_effects=True),
    )(tokens, norm_gain[None, :], expert_ids.T, gate_weights.T, w_gate, w_up, w_down)


def step(mesh, *arrays):
    tokens, norm_gain, w_gate, w_up, w_down, expert_ids, gate_weights = arrays
    ep_count, tp_count = mesh.shape["ep"], mesh.shape["tp"]
    rows, top_count = expert_ids.shape
    experts_all = ep_count * w_gate.shape[0]
    capacity = min(rows, rows * top_count * 4 // (3 * experts_all))
    dense = (
        w_gate.shape[0] == 1
        and tp_count == 2
        and ep_count % CORES == 0
        and ep_count > CORES
        and rows <= 2 * capacity
        and rows % (32 * PIECES[-1]) == 0
        and rows % (32 * SPANS[-1]) == 0
    )
    return fused(*arrays) if dense else body(*arrays)


def solution(mesh):
    placed = (
        P(("grp", "ep"), None),
        P(),
        P("ep", None, "tp"),
        P("ep", None, "tp"),
        P("ep", "tp", None),
        P(("grp", "ep"), None),
        P(("grp", "ep"), None),
    )
    return jax.shard_map(
        functools.partial(step, mesh), mesh=mesh, in_specs=placed, out_specs=P(("grp", "ep"), "tp"), check_vma=False
    )
```

```python
import functools

import jax
import jax.numpy as jnp
from jax import lax
from jax.experimental import pallas as pl
from jax.experimental.pallas import tpu as pltpu
from jax.sharding import PartitionSpec as P

epsilon = 1e-06
clamp_limit = 7.0
swish_alpha = 1.702


def rms_norm(tokens, norm_gain):
    widened = tokens.astype(jnp.float32)
    scaled = widened * lax.rsqrt(jnp.mean(widened * widened, axis=-1, keepdims=True) + epsilon)
    return (scaled * norm_gain).astype(jnp.bfloat16)


def body(tokens, norm_gain, w_gate, w_up, w_down, expert_ids, gate_weights):
    tok_rows, model_width = tokens.shape
    top_count = expert_ids.shape[1]
    ep_count = lax.axis_size("ep")
    local_experts = w_gate.shape[0]
    experts_all = local_experts * ep_count
    capacity = min(tok_rows, tok_rows * top_count * 4 // (3 * experts_all))
    normed = rms_norm(tokens, norm_gain)
    flat_ids = expert_ids.reshape(-1)
    onehot = (flat_ids[:, None] == jnp.arange(experts_all, dtype=jnp.int32)[None, :]).astype(
        jnp.int32
    )
    before = jnp.cumsum(onehot, axis=0) - onehot
    slot_index = jnp.sum(before * onehot, axis=1)
    dest_row = flat_ids * capacity + slot_index
    owner_tok = jnp.arange(tok_rows * top_count, dtype=jnp.int32) // top_count
    slot_table = (
        jnp.full((experts_all * capacity,), tok_rows, jnp.int32).at[dest_row].set(owner_tok)
    )
    padded = jnp.concatenate([normed, jnp.zeros((1, model_width), jnp.bfloat16)], axis=0)
    send_buffer = padded[slot_table].reshape(experts_all, capacity, model_width)
    received = lax.all_to_all(send_buffer, "ep", split_axis=0, concat_axis=0, tiled=True)
    expert_rows = received.reshape(ep_count, local_experts, capacity, model_width)
    gate_pre = jnp.einsum("sjcd,jdf->sjcf", expert_rows, w_gate, preferred_element_type=jnp.float32)
    up_pre = jnp.einsum("sjcd,jdf->sjcf", expert_rows, w_up, preferred_element_type=jnp.float32)
    gated = jnp.minimum(gate_pre, clamp_limit)
    linear = jnp.clip(up_pre, -clamp_limit, clamp_limit)
    activated = (gated * jax.nn.sigmoid(swish_alpha * gated) * (linear + 1.0)).astype(jnp.bfloat16)
    partial_value = jnp.einsum(
        "sjcf,jfd->sjcd", activated, w_down, preferred_element_type=jnp.float32
    ).astype(jnp.bfloat16)
    summed = (
        lax.psum_scatter(partial_value, "tp", scatter_dimension=3, tiled=True)
        .astype(jnp.float32)
        .astype(jnp.bfloat16)
    )
    returned = lax.all_to_all(summed, "ep", split_axis=0, concat_axis=0, tiled=True)
    returned = returned.reshape(experts_all * capacity, returned.shape[3])
    picked = returned[dest_row].reshape(tok_rows, top_count, returned.shape[1]).astype(jnp.float32)
    return jnp.sum(picked * gate_weights[:, :, None], axis=1).astype(jnp.bfloat16)


MESH = pl.DeviceIdType.MESH
CORES = 2
PIECES = (0, 1, 3, 5, 6)
SPANS = (0, 1, 2, 3)
OVER = 1
NEAR = 1
HIDDEN_TILE = 256
COLUMN_TILE = 512


def fused_kernel(
    chips,
    tok_hbm,
    gain_hbm,
    ids_hbm,
    gates_hbm,
    wg_hbm,
    wu_hbm,
    wd_hbm,
    out_ref,
    tok_ref,
    gain_ref,
    ids_ref,
    gates_ref,
    rows_all,
    codes,
    gate_cols,
    wg,
    wu,
    wd,
    act,
    kept,
    part,
    merge_out,
    merge_in,
    side_out,
    side_in,
    far_out,
    far_in,
    agg_in,
    over_in,
    near_in,
    input_sem,
    weight_sem,
    pair_sem,
    code_send,
    code_recv,
    z_send,
    z_recv,
    x_send,
    x_recv,
    merge_send,
    merge_recv,
    side_send,
    side_recv,
    far_send,
    far_recv,
    agg_recv,
    over_send,
    over_recv,
    near_send,
    near_recv,
):
    ep, tp = lax.axis_index("ep"), lax.axis_index("tp")
    z, core = lax.div(ep, CORES), lax.rem(ep, CORES)
    rows, width = tok_hbm.shape
    half = rows // 2
    out_width = width // 2
    hidden = wg.shape[2]
    last = chips - 1
    partner = {"ep": z * CORES + 1 - core}
    peer = {"tp": 1 - tp}
    centre = jnp.where(2 * z < last, 1, 0)

    def chip_of(block):
        return {"ep": block * CORES + core}

    def within(block):
        return (block >= 0) & (block < chips)

    def flow(turn):
        side = centre if turn == 0 else 1 - centre
        ahead = z + 1 - 2 * side
        return side, ahead, within(ahead)

    def at(turn, distance):
        block = z + distance * (2 * flow(turn)[0] - 1)
        return block, within(block)

    def half_of(which):
        return pl.ds(pl.multiple_of(which * half, 16), half)

    small = [
        pltpu.make_async_copy(source, target, input_sem.at[i])
        for i, (source, target) in enumerate(
            (
                (gain_hbm, gain_ref),
                (ids_hbm, ids_ref),
                (gates_hbm, gates_ref),
                (tok_hbm.at[half_of(tp)], tok_ref.at[half_of(tp)]),
                (tok_hbm.at[half_of(1 - tp)], tok_ref.at[half_of(1 - tp)]),
            )
        )
    ]
    sources = (wg_hbm.at[0], wu_hbm.at[0], wd_hbm.at[0])
    loads = [
        pltpu.make_async_copy(source, target, weight_sem.at[i])
        for i, (source, target) in enumerate(
            zip(sources, (wg.at[0], wu.at[0], wd.at[pl.ds(0, hidden)]))
        )
    ]

    barrier = pltpu.get_barrier_semaphore()
    for target in (partner, peer):
        pl.semaphore_signal(barrier, inc=1, device_id=target, device_id_type=MESH)
    for turn in range(2):

        @pl.when(flow(turn)[2])
        def _(turn=turn):
            target = chip_of(flow(turn)[1])
            pl.semaphore_signal(barrier, inc=1, device_id=target, device_id_type=MESH)

    for load in small:
        load.start()

    def remote(source, target, send, recv, device):
        return pltpu.make_async_remote_copy(
            src_ref=source,
            dst_ref=target,
            send_sem=send,
            recv_sem=recv,
            device_id=device,
            device_id_type=MESH,
        )

    gives = [
        remote(source, target, pair_sem.at[0, i], pair_sem.at[1, i], partner)
        for i, (source, target) in enumerate(
            zip(sources, (wg.at[1], wu.at[1], wd.at[pl.ds(hidden, hidden)]))
        )
    ]

    def normed(which):
        span = half_of(which)
        widened = tok_ref[span].astype(jnp.float32)
        scaled = widened * lax.rsqrt(jnp.mean(widened * widened, axis=-1, keepdims=True) + epsilon)
        rows_all[z, span] = (scaled * gain_ref[...]).astype(jnp.bfloat16)

    for load in small[:4]:
        load.wait()
    for load in loads:
        load.start()
    normed(tp)
    line = lax.broadcasted_iota(jnp.int32, (codes.shape[1], rows), 0)
    gate = jnp.zeros(line.shape, jnp.float32)
    for k in range(ids_ref.shape[0]):
        gate = gate + jnp.where(line == ids_ref[k : k + 1, :], gates_ref[k : k + 1, :], 0.0)
    codes[z] = jnp.zeros(codes.shape[1:], jnp.float32)
    codes[z, :, :rows] = gate

    neighbours = 2 + jnp.where(z > 0, 1, 0) + jnp.where(z < last, 1, 0)
    pl.semaphore_wait(barrier, neighbours)

    count = len(PIECES) - 1

    def rows_of(block, which, q):
        unit = half // PIECES[-1]
        start = pl.multiple_of(which * half + PIECES[q] * unit, 16)
        return rows_all.at[block, pl.ds(start, (PIECES[q + 1] - PIECES[q]) * unit)]

    def sender(turn, distance):
        side, _, _ = flow(turn)
        return jnp.where(side == 1, chips, z) if distance == 0 else at(turn, distance)[0]

    def z_copy(turn, distance, q):
        block = at(turn, distance)[0]
        ref = rows_of(block, tp, q)
        device = chip_of(flow(turn)[1])
        return remote(
            ref, ref, z_send.at[sender(turn, distance)], z_recv.at[block, q], device
        )

    def z_sent(turn, distance):
        ref = rows_all.at[z, half_of(tp)]
        return remote(ref, ref, z_send.at[sender(turn, distance)], z_recv.at[z, 0], peer)

    def code_copy(turn, distance):
        block = at(turn, distance)[0]
        device = chip_of(flow(turn)[1])
        return remote(
            codes.at[block],
            codes.at[block],
            code_send.at[sender(turn, distance)],
            code_recv.at[block],
            device,
        )

    def x_copy(block, which, q):
        ref = rows_of(block, which, q)
        return remote(ref, ref, x_send.at[block], x_recv.at[block], peer)

    def x_whole(block, which):
        ref = rows_all.at[block, half_of(which)]
        return remote(ref, ref, x_send.at[block], x_recv.at[block], peer)

    for q in range(count):
        for turn in range(2):

            @pl.when(flow(turn)[2])
            def _(turn=turn, q=q):
                z_copy(turn, 0, q).start()
                if q == 0:
                    code_copy(turn, 0).start()

    for give in gives:
        give.start()
    small[4].wait()
    normed(1 - tp)

    def gather_z(distance, q):
        for turn in range(2):

            @pl.when(at(turn, distance)[1])
            def _(turn=turn):
                z_copy(turn, distance, q).wait_recv()
                if q == 0:
                    code_copy(turn, distance).wait_recv()
                if distance < last:

                    @pl.when(flow(turn)[2])
                    def _():
                        z_copy(turn, distance, q).start()
                        if q == 0:
                            code_copy(turn, distance).start()

                if distance > 1 or turn == 0:
                    x_copy(at(turn, distance)[0], tp, q).start()

    waiting = [(distance, q) for distance in range(1, chips) for q in range(count)]

    def pump():
        if waiting:
            gather_z(*waiting.pop(0))

    def pump_all(distance):
        while waiting and waiting[0][0] <= distance:
            pump()

    def outer_x():
        @pl.when(at(1, 1)[1])
        def _():
            for q in range(count):
                x_copy(at(1, 1)[0], tp, q).start()

    def wait_x(distance, turn):
        @pl.when(at(turn, distance)[1])
        def _():
            x_whole(at(turn, distance)[0], 1 - tp).wait_recv()

    theirs = pl.multiple_of((1 - tp) * out_width, 128)
    mine = pl.multiple_of(tp * out_width, 128)
    parts = len(SPANS) - 1
    unit = half // SPANS[-1]
    first_half, second_half = tp, 1 - tp

    def span_of(which, s):
        start = pl.multiple_of(which * half + SPANS[s] * unit, 16)
        return pl.ds(start, (SPANS[s + 1] - SPANS[s]) * unit)

    def activate(block, start, size, slot):
        if slot == 0:
            gate_cols[...] = jnp.transpose(codes[block])
        span = pl.ds(start, size)
        turned = gate_cols[span]
        lane = lax.broadcasted_iota(jnp.int32, turned.shape, 1)
        owner = ep if slot == 0 else z * CORES + 1 - core
        weight = jnp.sum(jnp.where(lane == owner, turned, 0.0), axis=1, keepdims=True)
        held = rows_all[block, span]
        for begin in range(0, hidden, HIDDEN_TILE):
            columns = slice(begin, begin + HIDDEN_TILE)
            gate_pre = jnp.dot(held, wg[slot, :, columns], preferred_element_type=jnp.float32)
            up_pre = jnp.dot(held, wu[slot, :, columns], preferred_element_type=jnp.float32)
            gated = jnp.minimum(gate_pre, clamp_limit)
            linear = jnp.clip(up_pre, -clamp_limit, clamp_limit)
            value = gated * jax.nn.sigmoid(swish_alpha * gated) * (linear + 1.0) * weight
            act[:size, slot * hidden + begin : slot * hidden + begin + HIDDEN_TILE] = value.astype(
                jnp.bfloat16
            )

    def project(start, size):
        return jnp.dot(
            act[:size], wd[:, pl.ds(start, COLUMN_TILE)], preferred_element_type=jnp.float32
        )

    def merge_copy(side, other, which, s, block):
        span = span_of(which, s)
        return remote(
            merge_out.at[side, span],
            merge_in.at[other, span],
            merge_send.at[side],
            merge_recv.at[other, which * parts + s],
            chip_of(block),
        )

    def side_copy(block, which, s):
        span = span_of(which, s)
        return remote(
            side_out.at[block, span],
            side_in.at[block, span],
            side_send.at[block],
            side_recv.at[block, which * parts + s],
            peer,
        )

    def over_copy(side, block, which, s):
        span = span_of(which, s)
        return remote(
            side_out.at[block, span],
            over_in.at[1 - side, span],
            over_send.at[side],
            over_recv.at[1 - side, which * OVER + s],
            chip_of(block),
        )

    def far_copy(side, distance, block, which, s):
        span = span_of(which, s)
        if distance == 2:
            target = far_in.at[1 - side, span]
            receiver = far_recv.at[1 - side, which * parts + s]
            device = chip_of(block)
        else:
            target = agg_in.at[side, distance - 3, span]
            receiver = agg_recv.at[side, distance - 3, which * parts + s]
            device = chip_of(z + 2 * side - 1)
        return remote(far_out.at[block, span], target, far_send.at[block], receiver, device)

    def near_copy(side, block, which, s):
        span = span_of(which, s)
        return remote(
            far_out.at[block, span],
            near_in.at[1 - side, span],
            near_send.at[side],
            near_recv.at[1 - side, which * NEAR + s],
            chip_of(block),
        )

    def outward(turn):
        block, there = at(turn, 1)
        return there & (block + 1 - 2 * jnp.where(2 * block < last, 1, 0) == z)

    def over_there(turn):
        return at(turn, 2)[0] == jnp.where(flow(turn)[0] == 1, last, 0)

    def sent(ref, sem):
        return remote(ref, ref, sem, side_recv.at[0, 0], peer)

    def arrived(ref, sem):
        return remote(ref, ref, side_send.at[0], sem, peer)

    def outer_starts(side, block, which):
        for s in range(parts):
            if s < NEAR:
                side_copy(block, which, s).start()
            else:
                merge_copy(side, 1 - side, which, s, block).start()

    def job(distance, turn, which, pumped):
        block, there = at(turn, distance)
        side, _, through = flow(turn)
        start = pl.multiple_of(which * half, 16)

        @pl.when(there)
        def _():
            activate(block, start, half, 0)

        @pl.when(there)
        def _():
            activate(block, start, half, 1)

        if pumped:
            pump()

        @pl.when(there)
        def _():
            rows_here = half_of(which)
            if distance == 1:
                for begin in range(0, width, COLUMN_TILE):
                    merge_out[side, rows_here, begin : begin + COLUMN_TILE] = project(
                        begin, half
                    ).astype(jnp.bfloat16)
                if turn == 0:
                    for s in range(parts):
                        merge_copy(side, 1 - side, which, s, block).start()
                else:
                    for s in range(NEAR):
                        span = span_of(which, s)
                        side_out[block, span] = merge_out[side, span, pl.ds(theirs, out_width)]
                        part[block, span] = merge_out[side, span, pl.ds(mine, out_width)].astype(
                            jnp.float32
                        )
                    if which is second_half:
                        outer_starts(side, block, which)
            else:
                for begin in range(0, out_width, COLUMN_TILE):
                    side_out[block, rows_here, begin : begin + COLUMN_TILE] = project(
                        pl.multiple_of(theirs + begin, 128), half
                    ).astype(jnp.bfloat16)
                if distance == last:
                    for s in range(OVER if distance == 2 else 0, parts):
                        side_copy(block, which, s).start()
                for begin in range(0, out_width, COLUMN_TILE):
                    part[block, rows_here, begin : begin + COLUMN_TILE] = project(
                        pl.multiple_of(mine + begin, 128), half
                    )
            if distance == 2:

                @pl.when(jnp.logical_not(through))
                def _():
                    for s in range(OVER):
                        span = span_of(which, s)
                        over_copy(side, block, which, s).start()
                        far_out[block, span] = part[block, span].astype(jnp.bfloat16)
                        far_copy(side, 2, block, which, s).start()

        if pumped:
            pump()

    def outer_at(which):
        block, there = at(1, 1)
        side = flow(1)[0]

        @pl.when(there)
        def _():
            outer_starts(side, block, which)

    def near_sums():
        block, there = at(1, 1)
        side = flow(1)[0]

        @pl.when(there)
        def _():
            for which in (second_half, first_half):
                for s in range(NEAR):
                    span = span_of(which, s)
                    side_copy(block, which, s).wait_recv()
                    total = part[block, span] + side_in[block, span].astype(jnp.float32)
                    far_out[block, span] = total.astype(jnp.bfloat16)
                    near_copy(side, block, which, s).start()

    def sides_at(distance, turn, which, going):
        block, there = at(turn, distance)
        through = flow(turn)[2]

        @pl.when(there & (through if going else jnp.logical_not(through)))
        def _():
            for s in range(OVER if distance == 2 and not going else 0, parts):
                side_copy(block, which, s).start()

    def far_sums(distance, more, halves):
        for turn in range(2):
            block, there = at(turn, distance)
            side, _, through = flow(turn)

            @pl.when(there & (through if more else jnp.logical_not(through)))
            def _(block=block, side=side):
                for which in halves:
                    for s in range(OVER if distance == 2 and not more else 0, parts):
                        span = span_of(which, s)
                        side_copy(block, which, s).wait_recv()
                        total = part[block, span] + side_in[block, span].astype(jnp.float32)
                        if more:
                            arrived(
                                agg_in.at[side, distance - 2, span],
                                agg_recv.at[side, distance - 2, which * parts + s],
                            ).wait_recv()
                            total = total + agg_in[side, distance - 2, span].astype(jnp.float32)
                        far_out[block, span] = total.astype(jnp.bfloat16)
                        far_copy(side, distance, block, which, s).start()

    inner = (z > 0) & (z < last)
    early = jnp.logical_not(over_there(0) | over_there(1))
    for turn in range(2):
        early = early & (outward(turn) | jnp.logical_not(at(turn, 1)[1]))

    def own_send(which, s):
        span = span_of(which, s)
        side_out[z, span] = kept[span, pl.ds(theirs, out_width)].astype(jnp.bfloat16)
        side_copy(z, which, s).start()

    def own_early(which):
        @pl.when(early)
        def _():
            for s in range(NEAR):
                own_send(which, s)

    def own_span(which, s):
        span = span_of(which, s)
        for turn in range(2):
            merged = at(turn, 1)[1]
            if s < NEAR:
                merged = merged & jnp.logical_not(outward(turn))

            @pl.when(merged)
            def _(turn=turn):
                side = flow(turn)[0]
                arrived(
                    merge_in.at[side, span], merge_recv.at[side, which * parts + s]
                ).wait_recv()
                kept[span] = kept[span] + merge_in[side, span].astype(jnp.float32)

            if s < OVER and chips > 2:

                @pl.when(over_there(turn))
                def _(turn=turn):
                    side = flow(turn)[0]
                    arrived(
                        over_in.at[side, span], over_recv.at[side, which * OVER + s]
                    ).wait_recv()
                    here = (span, pl.ds(theirs, out_width))
                    kept[here] = kept[here] + over_in[side, span].astype(jnp.float32)

        own_send(which, s)

    def own_exchange():
        for which in (first_half, second_half):
            for s in range(parts):
                if s < NEAR:

                    @pl.when(jnp.logical_not(early))
                    def _():
                        own_span(which, s)

                else:
                    own_span(which, s)

    def finish():
        for which in (second_half, first_half):
            for s in range(parts):
                span = span_of(which, s)
                here = (span, pl.ds(mine, out_width))
                if chips > 2:
                    for turn in range(2):

                        @pl.when(at(turn, 2)[1])
                        def _(turn=turn):
                            side = flow(turn)[0]
                            arrived(
                                far_in.at[side, span], far_recv.at[side, which * parts + s]
                            ).wait_recv()
                            kept[here] = kept[here] + far_in[side, span].astype(jnp.float32)

                if s < NEAR:
                    for turn in range(2):

                        @pl.when(outward(turn))
                        def _(turn=turn):
                            side = flow(turn)[0]
                            arrived(
                                near_in.at[side, span], near_recv.at[side, which * NEAR + s]
                            ).wait_recv()
                            kept[here] = kept[here] + near_in[side, span].astype(jnp.float32)

                side_copy(z, which, s).wait_recv()
                out_ref[span] = (kept[here] + side_in[z, span].astype(jnp.float32)).astype(
                    jnp.bfloat16
                )

    def own_compute(there):
        @pl.when(there)
        def _():
            activate(z, 0, rows, 0)
            activate(z, 0, rows, 1)
            for begin in range(0, width, COLUMN_TILE):
                kept[:, begin : begin + COLUMN_TILE] = project(begin, rows)

    pump_all(1)
    outer_x()
    for load in loads:
        load.wait()
    for give in gives:
        give.wait_recv()

    outer = range(1, last // 2 + 1)
    job(1, 0, first_half, True)
    for distance in range(1, chips):
        if distance in outer:
            job(distance, 1, first_half, False)
        if distance == 2:
            own_compute(inner)
        wait_x(distance, 0)
        job(distance, 0, second_half, distance < last)
        if 1 < distance < last:
            sides_at(distance, 0, second_half, True)
        if distance < last:
            pump_all(distance + 1)
            if distance == 1:
                outer_at(first_half)
            job(distance + 1, 0, first_half, True)
            if distance + 1 < last:
                sides_at(distance + 1, 0, first_half, True)
            if distance + 1 == last:
                own_compute(jnp.logical_not(inner))
                own_early(first_half)
        if distance in outer:
            wait_x(distance, 1)
            job(distance, 1, second_half, False)
            if distance > 1:
                for which in (first_half, second_half):
                    for going in (True, False):
                        sides_at(distance, 1, which, going)
    if last == 1:
        own_early(first_half)
    for distance in range(last - 1, 1, -1):
        for which in (first_half, second_half):
            sides_at(distance, 0, which, False)
    own_early(second_half)
    both = (second_half, first_half)
    if last > 1:
        far_sums(last, False, both)
    own_exchange()
    for distance in range(last - 1, 1, -1):
        far_sums(distance, False, both)
        if distance > 2:
            far_sums(distance, True, both)
    far_sums(2, True, both[:1])
    near_sums()
    far_sums(2, True, both[1:])

    for give in gives:
        give.wait_send()
    for turn in range(2):
        for distance in range(chips):
            if distance < last:

                @pl.when(at(turn, distance)[1] & flow(turn)[2])
                def _(turn=turn, distance=distance):
                    z_sent(turn, distance).wait_send()
                    code_copy(turn, distance).wait_send()

            if distance > 0:

                @pl.when(at(turn, distance)[1])
                def _(turn=turn, distance=distance):
                    x_whole(at(turn, distance)[0], tp).wait_send()

        @pl.when(at(turn, 1)[1])
        def _(turn=turn):
            side = flow(turn)[0]
            near_rows = 2 * SPANS[NEAR] * unit if turn == 1 else 0
            whole = merge_out.at[side, pl.ds(0, rows - near_rows)]
            sent(whole, merge_send.at[side]).wait_send()
            if turn == 1:
                block = at(turn, 1)[0]
                sent(side_out.at[block, pl.ds(0, near_rows)], side_send.at[block]).wait_send()
                sent(far_out.at[block, pl.ds(0, near_rows)], near_send.at[side]).wait_send()

    finish()
    sent(side_out.at[z], side_send.at[z]).wait_send()
    short = 2 * SPANS[OVER] * unit
    for turn in range(2):
        side, _, through = flow(turn)
        for distance in range(2, chips):
            block, there = at(turn, distance)
            whole = there & through if distance == 2 else there

            @pl.when(whole)
            def _(block=block):
                sent(side_out.at[block], side_send.at[block]).wait_send()

            if distance == 2:

                @pl.when(there & jnp.logical_not(through))
                def _(block=block, side=side):
                    rest = side_out.at[block, pl.ds(0, rows - short)]
                    sent(rest, side_send.at[block]).wait_send()
                    sent(side_out.at[block, pl.ds(0, short)], over_send.at[side]).wait_send()

            @pl.when(there)
            def _(block=block):
                sent(far_out.at[block], far_send.at[block]).wait_send()


def fused(tokens, norm_gain, w_gate, w_up, w_down, expert_ids, gate_weights):
    rows, width = tokens.shape
    top_count = expert_ids.shape[1]
    chips = lax.axis_size("ep") // CORES
    experts_all = chips * CORES
    lines = experts_all + -experts_all % 8
    hidden = w_gate.shape[2]
    out_width = width // 2
    last = chips - 1
    aggregates = max(last - 2, 1)
    lanes = rows + -rows % 128
    spans = 2 * (len(SPANS) - 1)
    anywhere = pl.BlockSpec(memory_space=pl.ANY)
    vmem, dma = pltpu.VMEM, pltpu.SemaphoreType.DMA
    return pl.pallas_call(
        functools.partial(fused_kernel, chips),
        out_shape=vmem((rows, out_width), jnp.bfloat16),
        in_specs=[anywhere] * 7,
        out_specs=pl.BlockSpec(memory_space=vmem),
        scratch_shapes=[
            vmem((rows, width), jnp.bfloat16),
            vmem((1, width), jnp.float32),
            vmem((top_count, rows), jnp.int32),
            vmem((top_count, rows), jnp.float32),
            vmem((chips, rows, width), jnp.bfloat16),
            vmem((chips, lines, lanes), jnp.float32),
            vmem((lanes, lines), jnp.float32),
            vmem((CORES, width, hidden), jnp.bfloat16),
            vmem((CORES, width, hidden), jnp.bfloat16),
            vmem((CORES * hidden, width), jnp.bfloat16),
            vmem((rows, CORES * hidden), jnp.bfloat16),
            vmem((rows, width), jnp.float32),
            vmem((chips, rows, out_width), jnp.float32),
            vmem((2, rows, width), jnp.bfloat16),
            vmem((2, rows, width), jnp.bfloat16),
            vmem((chips, rows, out_width), jnp.bfloat16),
            vmem((chips, rows, out_width), jnp.bfloat16),
            vmem((chips, rows, out_width), jnp.bfloat16),
            vmem((2, rows, out_width), jnp.bfloat16),
            vmem((2, aggregates, rows, out_width), jnp.bfloat16),
            vmem((2, rows, out_width), jnp.bfloat16),
            vmem((2, rows, out_width), jnp.bfloat16),
            dma((5,)),
            dma((3,)),
            dma((2, 3)),
            dma((chips + 1,)),
            dma((chips,)),
            dma((chips + 1,)),
            dma((chips, len(PIECES) - 1)),
            dma((chips,)),
            dma((chips,)),
            dma((2,)),
            dma((2, spans)),
            dma((chips,)),
            dma((chips, spans)),
            dma((chips,)),
            dma((2, spans)),
            dma((2, aggregates, spans)),
            dma((2,)),
            dma((2, 2 * OVER)),
            dma((2,)),
            dma((2, 2 * NEAR)),
        ],
        compiler_params=pltpu.CompilerParams(collective_id=0, has_side_effects=True),
    )(tokens, norm_gain[None, :], expert_ids.T, gate_weights.T, w_gate, w_up, w_down)


def step(mesh, *arrays):
    tokens, norm_gain, w_gate, w_up, w_down, expert_ids, gate_weights = arrays
    ep_count, tp_count = mesh.shape["ep"], mesh.shape["tp"]
    rows, top_count = expert_ids.shape
    experts_all = ep_count * w_gate.shape[0]
    capacity = min(rows, rows * top_count * 4 // (3 * experts_all))
    dense = (
        w_gate.shape[0] == 1
        and tp_count == 2
        and ep_count % CORES == 0
        and ep_count > 3 * CORES
        and rows <= 2 * capacity
        and rows % (32 * PIECES[-1]) == 0
        and rows % (32 * SPANS[-1]) == 0
    )
    return fused(*arrays) if dense else body(*arrays)


def solution(mesh):
    placed = (
        P(("grp", "ep"), None),
        P(),
        P("ep", None, "tp"),
        P("ep", None, "tp"),
        P("ep", "tp", None),
        P(("grp", "ep"), None),
        P(("grp", "ep"), None),
    )
    return jax.shard_map(
        functools.partial(step, mesh), mesh=mesh, in_specs=placed, out_specs=P(("grp", "ep"), "tp"), check_vma=False
    )
```

```python
import functools

import jax
import jax.numpy as jnp
from jax import lax
from jax.experimental import pallas as pl
from jax.experimental.pallas import tpu as pltpu
from jax.sharding import PartitionSpec as P

epsilon = 1e-06
clamp_limit = 7.0
swish_alpha = 1.702


def rms_norm(tokens, norm_gain):
    widened = tokens.astype(jnp.float32)
    scaled = widened * lax.rsqrt(jnp.mean(widened * widened, axis=-1, keepdims=True) + epsilon)
    return (scaled * norm_gain).astype(jnp.bfloat16)


def body(tokens, norm_gain, w_gate, w_up, w_down, expert_ids, gate_weights):
    tok_rows, model_width = tokens.shape
    top_count = expert_ids.shape[1]
    ep_count = lax.axis_size("ep")
    local_experts = w_gate.shape[0]
    experts_all = local_experts * ep_count
    capacity = min(tok_rows, tok_rows * top_count * 4 // (3 * experts_all))
    normed = rms_norm(tokens, norm_gain)
    flat_ids = expert_ids.reshape(-1)
    onehot = (flat_ids[:, None] == jnp.arange(experts_all, dtype=jnp.int32)[None, :]).astype(
        jnp.int32
    )
    before = jnp.cumsum(onehot, axis=0) - onehot
    slot_index = jnp.sum(before * onehot, axis=1)
    dest_row = flat_ids * capacity + slot_index
    owner_tok = jnp.arange(tok_rows * top_count, dtype=jnp.int32) // top_count
    slot_table = (
        jnp.full((experts_all * capacity,), tok_rows, jnp.int32).at[dest_row].set(owner_tok)
    )
    padded = jnp.concatenate([normed, jnp.zeros((1, model_width), jnp.bfloat16)], axis=0)
    send_buffer = padded[slot_table].reshape(experts_all, capacity, model_width)
    received = lax.all_to_all(send_buffer, "ep", split_axis=0, concat_axis=0, tiled=True)
    expert_rows = received.reshape(ep_count, local_experts, capacity, model_width)
    gate_pre = jnp.einsum("sjcd,jdf->sjcf", expert_rows, w_gate, preferred_element_type=jnp.float32)
    up_pre = jnp.einsum("sjcd,jdf->sjcf", expert_rows, w_up, preferred_element_type=jnp.float32)
    gated = jnp.minimum(gate_pre, clamp_limit)
    linear = jnp.clip(up_pre, -clamp_limit, clamp_limit)
    activated = (gated * jax.nn.sigmoid(swish_alpha * gated) * (linear + 1.0)).astype(jnp.bfloat16)
    partial_value = jnp.einsum(
        "sjcf,jfd->sjcd", activated, w_down, preferred_element_type=jnp.float32
    ).astype(jnp.bfloat16)
    summed = (
        lax.psum_scatter(partial_value, "tp", scatter_dimension=3, tiled=True)
        .astype(jnp.float32)
        .astype(jnp.bfloat16)
    )
    returned = lax.all_to_all(summed, "ep", split_axis=0, concat_axis=0, tiled=True)
    returned = returned.reshape(experts_all * capacity, returned.shape[3])
    picked = returned[dest_row].reshape(tok_rows, top_count, returned.shape[1]).astype(jnp.float32)
    return jnp.sum(picked * gate_weights[:, :, None], axis=1).astype(jnp.bfloat16)


MESH = pl.DeviceIdType.MESH
CORES = 2
PIECES = (0, 1, 3, 5, 6)
SPANS = (0, 1, 2, 3)
OVER = 1
NEAR = 1
HIDDEN_TILE = 256
COLUMN_TILE = 512


def fused_kernel(
    chips,
    tok_hbm,
    gain_hbm,
    ids_hbm,
    gates_hbm,
    wg_hbm,
    wu_hbm,
    wd_hbm,
    out_ref,
    tok_ref,
    gain_ref,
    ids_ref,
    gates_ref,
    rows_all,
    codes,
    gate_cols,
    wg,
    wu,
    wd,
    act,
    kept,
    part,
    merge_out,
    merge_in,
    side_out,
    side_in,
    far_out,
    far_in,
    agg_in,
    over_in,
    near_in,
    input_sem,
    weight_sem,
    pair_sem,
    code_send,
    code_recv,
    z_send,
    z_recv,
    x_send,
    x_recv,
    merge_send,
    merge_recv,
    side_send,
    side_recv,
    far_send,
    far_recv,
    agg_recv,
    over_send,
    over_recv,
    near_send,
    near_recv,
):
    ep, tp = lax.axis_index("ep"), lax.axis_index("tp")
    z, core = lax.div(ep, CORES), lax.rem(ep, CORES)
    rows, width = tok_hbm.shape
    half = rows // 2
    out_width = width // 2
    hidden = wg.shape[2]
    last = chips - 1
    partner = {"ep": z * CORES + 1 - core}
    peer = {"tp": 1 - tp}
    centre = jnp.where(2 * z < last, 1, 0)

    def chip_of(block):
        return {"ep": block * CORES + core}

    def within(block):
        return (block >= 0) & (block < chips)

    def flow(turn):
        side = centre if turn == 0 else 1 - centre
        ahead = z + 1 - 2 * side
        return side, ahead, within(ahead)

    def at(turn, distance):
        block = z + distance * (2 * flow(turn)[0] - 1)
        return block, within(block)

    def half_of(which):
        return pl.ds(pl.multiple_of(which * half, 16), half)

    small = [
        pltpu.make_async_copy(source, target, input_sem.at[i])
        for i, (source, target) in enumerate(
            (
                (gain_hbm, gain_ref),
                (ids_hbm, ids_ref),
                (gates_hbm, gates_ref),
                (tok_hbm.at[half_of(tp)], tok_ref.at[half_of(tp)]),
                (tok_hbm.at[half_of(1 - tp)], tok_ref.at[half_of(1 - tp)]),
            )
        )
    ]
    sources = (wg_hbm.at[0], wu_hbm.at[0], wd_hbm.at[0])
    loads = [
        pltpu.make_async_copy(source, target, weight_sem.at[i])
        for i, (source, target) in enumerate(
            zip(sources, (wg.at[0], wu.at[0], wd.at[pl.ds(0, hidden)]))
        )
    ]

    barrier = pltpu.get_barrier_semaphore()
    for target in (partner, peer):
        pl.semaphore_signal(barrier, inc=1, device_id=target, device_id_type=MESH)
    for turn in range(2):

        @pl.when(flow(turn)[2])
        def _(turn=turn):
            target = chip_of(flow(turn)[1])
            pl.semaphore_signal(barrier, inc=1, device_id=target, device_id_type=MESH)

    for load in small:
        load.start()

    def remote(source, target, send, recv, device):
        return pltpu.make_async_remote_copy(
            src_ref=source,
            dst_ref=target,
            send_sem=send,
            recv_sem=recv,
            device_id=device,
            device_id_type=MESH,
        )

    gives = [
        remote(source, target, pair_sem.at[0, i], pair_sem.at[1, i], partner)
        for i, (source, target) in enumerate(
            zip(sources, (wg.at[1], wu.at[1], wd.at[pl.ds(hidden, hidden)]))
        )
    ]

    def normed(which):
        span = half_of(which)
        widened = tok_ref[span].astype(jnp.float32)
        scaled = widened * lax.rsqrt(jnp.mean(widened * widened, axis=-1, keepdims=True) + epsilon)
        rows_all[z, span] = (scaled * gain_ref[...]).astype(jnp.bfloat16)

    for load in small[:4]:
        load.wait()
    for load in loads:
        load.start()
    normed(tp)
    line = lax.broadcasted_iota(jnp.int32, (codes.shape[1], rows), 0)
    gate = jnp.zeros(line.shape, jnp.float32)
    for k in range(ids_ref.shape[0]):
        gate = gate + jnp.where(line == ids_ref[k : k + 1, :], gates_ref[k : k + 1, :], 0.0)
    codes[z] = jnp.zeros(codes.shape[1:], jnp.float32)
    codes[z, :, :rows] = gate

    neighbours = 2 + jnp.where(z > 0, 1, 0) + jnp.where(z < last, 1, 0)
    pl.semaphore_wait(barrier, neighbours)

    count = len(PIECES) - 1

    def rows_of(block, which, q):
        unit = half // PIECES[-1]
        start = pl.multiple_of(which * half + PIECES[q] * unit, 16)
        return rows_all.at[block, pl.ds(start, (PIECES[q + 1] - PIECES[q]) * unit)]

    def sender(turn, distance):
        side, _, _ = flow(turn)
        return jnp.where(side == 1, chips, z) if distance == 0 else at(turn, distance)[0]

    def z_copy(turn, distance, q):
        block = at(turn, distance)[0]
        ref = rows_of(block, tp, q)
        device = chip_of(flow(turn)[1])
        return remote(
            ref, ref, z_send.at[sender(turn, distance)], z_recv.at[block, q], device
        )

    def z_sent(turn, distance):
        ref = rows_all.at[z, half_of(tp)]
        return remote(ref, ref, z_send.at[sender(turn, distance)], z_recv.at[z, 0], peer)

    def code_copy(turn, distance):
        block = at(turn, distance)[0]
        device = chip_of(flow(turn)[1])
        return remote(
            codes.at[block],
            codes.at[block],
            code_send.at[sender(turn, distance)],
            code_recv.at[block],
            device,
        )

    def x_copy(block, which, q):
        ref = rows_of(block, which, q)
        return remote(ref, ref, x_send.at[0], x_recv.at[block], peer)

    def x_whole(block, which):
        ref = rows_all.at[block, half_of(which)]
        return remote(ref, ref, x_send.at[0], x_recv.at[block], peer)

    for q in range(count):
        for turn in range(2):

            @pl.when(flow(turn)[2])
            def _(turn=turn, q=q):
                z_copy(turn, 0, q).start()
                if q == 0:
                    code_copy(turn, 0).start()

    for give in gives:
        give.start()
    small[4].wait()
    normed(1 - tp)

    def gather_z(distance, q):
        for turn in range(2):

            @pl.when(at(turn, distance)[1])
            def _(turn=turn):
                z_copy(turn, distance, q).wait_recv()
                if q == 0:
                    code_copy(turn, distance).wait_recv()
                if distance < last:

                    @pl.when(flow(turn)[2])
                    def _():
                        z_copy(turn, distance, q).start()
                        if q == 0:
                            code_copy(turn, distance).start()

                if distance > 1 or turn == 0:
                    x_copy(at(turn, distance)[0], tp, q).start()

    waiting = [(distance, q) for distance in range(1, chips) for q in range(count)]

    def pump():
        if waiting:
            gather_z(*waiting.pop(0))

    def pump_all(distance):
        while waiting and waiting[0][0] <= distance:
            pump()

    def outer_x():
        @pl.when(at(1, 1)[1])
        def _():
            for q in range(count):
                x_copy(at(1, 1)[0], tp, q).start()

    def wait_x(distance, turn):
        @pl.when(at(turn, distance)[1])
        def _():
            x_whole(at(turn, distance)[0], 1 - tp).wait_recv()

    theirs = pl.multiple_of((1 - tp) * out_width, 128)
    mine = pl.multiple_of(tp * out_width, 128)
    parts = len(SPANS) - 1
    unit = half // SPANS[-1]
    first_half, second_half = tp, 1 - tp

    def span_of(which, s):
        start = pl.multiple_of(which * half + SPANS[s] * unit, 16)
        return pl.ds(start, (SPANS[s + 1] - SPANS[s]) * unit)

    def activate(block, start, size, slot):
        if slot == 0:
            gate_cols[...] = jnp.transpose(codes[block])
        span = pl.ds(start, size)
        turned = gate_cols[span]
        lane = lax.broadcasted_iota(jnp.int32, turned.shape, 1)
        owner = ep if slot == 0 else z * CORES + 1 - core
        weight = jnp.sum(jnp.where(lane == owner, turned, 0.0), axis=1, keepdims=True)
        held = rows_all[block, span]
        for begin in range(0, hidden, HIDDEN_TILE):
            columns = slice(begin, begin + HIDDEN_TILE)
            gate_pre = jnp.dot(held, wg[slot, :, columns], preferred_element_type=jnp.float32)
            up_pre = jnp.dot(held, wu[slot, :, columns], preferred_element_type=jnp.float32)
            gated = jnp.minimum(gate_pre, clamp_limit)
            linear = jnp.clip(up_pre, -clamp_limit, clamp_limit)
            value = gated * jax.nn.sigmoid(swish_alpha * gated) * (linear + 1.0) * weight
            act[:size, slot * hidden + begin : slot * hidden + begin + HIDDEN_TILE] = value.astype(
                jnp.bfloat16
            )

    def project(start, size):
        return jnp.dot(
            act[:size], wd[:, pl.ds(start, COLUMN_TILE)], preferred_element_type=jnp.float32
        )

    def merge_copy(side, other, which, s, block):
        span = span_of(which, s)
        return remote(
            merge_out.at[side, span],
            merge_in.at[other, span],
            merge_send.at[side],
            merge_recv.at[other, which * parts + s],
            chip_of(block),
        )

    def side_copy(block, which, s):
        span = span_of(which, s)
        return remote(
            side_out.at[block, span],
            side_in.at[block, span],
            side_send.at[block],
            side_recv.at[block, which * parts + s],
            peer,
        )

    def over_copy(side, block, which, s):
        span = span_of(which, s)
        return remote(
            side_out.at[block, span],
            over_in.at[1 - side, span],
            over_send.at[side],
            over_recv.at[1 - side, which * OVER + s],
            chip_of(block),
        )

    def far_copy(side, distance, block, which, s):
        span = span_of(which, s)
        if distance == 2:
            target = far_in.at[1 - side, span]
            receiver = far_recv.at[1 - side, which * parts + s]
            device = chip_of(block)
        else:
            target = agg_in.at[side, distance - 3, span]
            receiver = agg_recv.at[side, distance - 3, which * parts + s]
            device = chip_of(z + 2 * side - 1)
        return remote(far_out.at[block, span], target, far_send.at[block], receiver, device)

    def near_copy(side, block, which, s):
        span = span_of(which, s)
        return remote(
            far_out.at[block, span],
            near_in.at[1 - side, span],
            near_send.at[side],
            near_recv.at[1 - side, which * NEAR + s],
            chip_of(block),
        )

    def outward(turn):
        block, there = at(turn, 1)
        return there & (block + 1 - 2 * jnp.where(2 * block < last, 1, 0) == z)

    def over_there(turn):
        return at(turn, 2)[0] == jnp.where(flow(turn)[0] == 1, last, 0)

    def sent(ref, sem):
        return remote(ref, ref, sem, side_recv.at[0, 0], peer)

    def arrived(ref, sem):
        return remote(ref, ref, side_send.at[0], sem, peer)

    def outer_starts(side, block, which):
        for s in range(parts):
            if s < NEAR:
                side_copy(block, which, s).start()
            else:
                merge_copy(side, 1 - side, which, s, block).start()

    def job(distance, turn, which, pumped, ready=None):
        block, there = at(turn, distance)
        side, _, through = flow(turn)
        start = pl.multiple_of(which * half, 16)

        @pl.when(there)
        def _():
            activate(block, start, half, 0)

        @pl.when(there)
        def _():
            activate(block, start, half, 1)

        if ready is not None:
            ready()
        if pumped:
            pump()

        @pl.when(there)
        def _():
            rows_here = half_of(which)
            if distance == 1:
                for begin in range(0, width, COLUMN_TILE):
                    merge_out[side, rows_here, begin : begin + COLUMN_TILE] = project(
                        begin, half
                    ).astype(jnp.bfloat16)
                if turn == 0:
                    for s in range(parts):
                        merge_copy(side, 1 - side, which, s, block).start()
                else:
                    for s in range(NEAR):
                        span = span_of(which, s)
                        side_out[block, span] = merge_out[side, span, pl.ds(theirs, out_width)]
                        part[block, span] = merge_out[side, span, pl.ds(mine, out_width)].astype(
                            jnp.float32
                        )
                    if which is second_half:
                        outer_starts(side, block, which)
            else:
                for begin in range(0, out_width, COLUMN_TILE):
                    side_out[block, rows_here, begin : begin + COLUMN_TILE] = project(
                        pl.multiple_of(theirs + begin, 128), half
                    ).astype(jnp.bfloat16)
                if distance == last:
                    for s in range(OVER if distance == 2 else 0, parts):
                        side_copy(block, which, s).start()
                for begin in range(0, out_width, COLUMN_TILE):
                    part[block, rows_here, begin : begin + COLUMN_TILE] = project(
                        pl.multiple_of(mine + begin, 128), half
                    )
            if distance == 2:

                @pl.when(jnp.logical_not(through))
                def _():
                    for s in range(OVER):
                        span = span_of(which, s)
                        over_copy(side, block, which, s).start()
                        far_out[block, span] = part[block, span].astype(jnp.bfloat16)
                        far_copy(side, 2, block, which, s).start()

        if pumped:
            pump()

    def outer_at(which):
        block, there = at(1, 1)
        side = flow(1)[0]

        @pl.when(there)
        def _():
            outer_starts(side, block, which)

    def near_sums():
        block, there = at(1, 1)
        side = flow(1)[0]

        @pl.when(there)
        def _():
            for which in (second_half, first_half):
                for s in range(NEAR):
                    span = span_of(which, s)
                    side_copy(block, which, s).wait_recv()
                    total = part[block, span] + side_in[block, span].astype(jnp.float32)
                    far_out[block, span] = total.astype(jnp.bfloat16)
                    near_copy(side, block, which, s).start()

    def sides_at(distance, turn, which, going):
        block, there = at(turn, distance)
        through = flow(turn)[2]

        @pl.when(there & (through if going else jnp.logical_not(through)))
        def _():
            for s in range(OVER if distance == 2 and not going else 0, parts):
                side_copy(block, which, s).start()

    def far_sums(distance, more, halves):
        for turn in range(2):
            block, there = at(turn, distance)
            side, _, through = flow(turn)

            @pl.when(there & (through if more else jnp.logical_not(through)))
            def _(block=block, side=side):
                for which in halves:
                    for s in range(OVER if distance == 2 and not more else 0, parts):
                        span = span_of(which, s)
                        side_copy(block, which, s).wait_recv()
                        total = part[block, span] + side_in[block, span].astype(jnp.float32)
                        if more:
                            arrived(
                                agg_in.at[side, distance - 2, span],
                                agg_recv.at[side, distance - 2, which * parts + s],
                            ).wait_recv()
                            total = total + agg_in[side, distance - 2, span].astype(jnp.float32)
                        far_out[block, span] = total.astype(jnp.bfloat16)
                        far_copy(side, distance, block, which, s).start()

    inner = (z > 0) & (z < last)
    early = jnp.logical_not(over_there(0) | over_there(1))
    for turn in range(2):
        early = early & (outward(turn) | jnp.logical_not(at(turn, 1)[1]))

    def own_send(which, s):
        span = span_of(which, s)
        side_out[z, span] = kept[span, pl.ds(theirs, out_width)].astype(jnp.bfloat16)
        side_copy(z, which, s).start()

    def own_early(which):
        @pl.when(early)
        def _():
            for s in range(NEAR):
                own_send(which, s)

    def own_span(which, s):
        span = span_of(which, s)
        for turn in range(2):
            merged = at(turn, 1)[1]
            if s < NEAR:
                merged = merged & jnp.logical_not(outward(turn))

            @pl.when(merged)
            def _(turn=turn):
                side = flow(turn)[0]
                arrived(
                    merge_in.at[side, span], merge_recv.at[side, which * parts + s]
                ).wait_recv()
                kept[span] = kept[span] + merge_in[side, span].astype(jnp.float32)

            if s < OVER and chips > 2:

                @pl.when(over_there(turn))
                def _(turn=turn):
                    side = flow(turn)[0]
                    arrived(
                        over_in.at[side, span], over_recv.at[side, which * OVER + s]
                    ).wait_recv()
                    here = (span, pl.ds(theirs, out_width))
                    kept[here] = kept[here] + over_in[side, span].astype(jnp.float32)

        own_send(which, s)

    def own_exchange():
        for which in (first_half, second_half):
            for s in range(parts):
                if s < NEAR:

                    @pl.when(jnp.logical_not(early))
                    def _():
                        own_span(which, s)

                else:
                    own_span(which, s)

    def finish():
        for which in (second_half, first_half):
            for s in range(parts):
                span = span_of(which, s)
                here = (span, pl.ds(mine, out_width))
                if chips > 2:
                    for turn in range(2):

                        @pl.when(at(turn, 2)[1])
                        def _(turn=turn):
                            side = flow(turn)[0]
                            arrived(
                                far_in.at[side, span], far_recv.at[side, which * parts + s]
                            ).wait_recv()
                            kept[here] = kept[here] + far_in[side, span].astype(jnp.float32)

                if s < NEAR:
                    for turn in range(2):

                        @pl.when(outward(turn))
                        def _(turn=turn):
                            side = flow(turn)[0]
                            arrived(
                                near_in.at[side, span], near_recv.at[side, which * NEAR + s]
                            ).wait_recv()
                            kept[here] = kept[here] + near_in[side, span].astype(jnp.float32)

                side_copy(z, which, s).wait_recv()
                out_ref[span] = (kept[here] + side_in[z, span].astype(jnp.float32)).astype(
                    jnp.bfloat16
                )

    def own_compute(there):
        @pl.when(there)
        def _():
            activate(z, 0, rows, 0)
            activate(z, 0, rows, 1)
            for begin in range(0, width, COLUMN_TILE):
                kept[:, begin : begin + COLUMN_TILE] = project(begin, rows)

    pump_all(1)
    outer_x()
    for i in range(2):
        loads[i].wait()
        gives[i].wait_recv()

    outer = range(1, last // 2 + 1)
    def down_ready():
        loads[2].wait()
        gives[2].wait_recv()

    job(1, 0, first_half, True, down_ready)
    for distance in range(1, chips):
        if distance in outer:
            job(distance, 1, first_half, False)
        if distance == 2:
            own_compute(inner)
        wait_x(distance, 0)
        job(distance, 0, second_half, distance < last)
        if 1 < distance < last:
            sides_at(distance, 0, second_half, True)
        if distance < last:
            pump_all(distance + 1)
            if distance == 1:
                outer_at(first_half)
            job(distance + 1, 0, first_half, True)
            if distance + 1 < last:
                sides_at(distance + 1, 0, first_half, True)
            if distance + 1 == last:
                own_compute(jnp.logical_not(inner))
                own_early(first_half)
        if distance in outer:
            wait_x(distance, 1)
            job(distance, 1, second_half, False)
            if distance > 1:
                for which in (first_half, second_half):
                    for going in (True, False):
                        sides_at(distance, 1, which, going)
    if last == 1:
        own_early(first_half)
    for distance in range(last - 1, 1, -1):
        for which in (first_half, second_half):
            sides_at(distance, 0, which, False)
    own_early(second_half)
    both = (second_half, first_half)
    if last > 1:
        far_sums(last, False, both)
    own_exchange()
    for distance in range(last - 1, 1, -1):
        far_sums(distance, False, both)
        if distance > 2:
            far_sums(distance, True, both)
    far_sums(2, True, both[:1])
    near_sums()
    far_sums(2, True, both[1:])

    for give in gives:
        give.wait_send()
    gone = rows_all.at[pl.ds(0, last), half_of(tp)]
    remote(gone, gone, x_send.at[0], x_recv.at[0], peer).wait_send()
    for turn in range(2):
        for distance in range(chips):
            if distance < last:

                @pl.when(at(turn, distance)[1] & flow(turn)[2])
                def _(turn=turn, distance=distance):
                    z_sent(turn, distance).wait_send()
                    code_copy(turn, distance).wait_send()

        @pl.when(at(turn, 1)[1])
        def _(turn=turn):
            side = flow(turn)[0]
            near_rows = 2 * SPANS[NEAR] * unit if turn == 1 else 0
            whole = merge_out.at[side, pl.ds(0, rows - near_rows)]
            sent(whole, merge_send.at[side]).wait_send()
            if turn == 1:
                block = at(turn, 1)[0]
                sent(side_out.at[block, pl.ds(0, near_rows)], side_send.at[block]).wait_send()
                sent(far_out.at[block, pl.ds(0, near_rows)], near_send.at[side]).wait_send()

    finish()
    sent(side_out.at[z], side_send.at[z]).wait_send()
    short = 2 * SPANS[OVER] * unit
    for turn in range(2):
        side, _, through = flow(turn)
        for distance in range(2, chips):
            block, there = at(turn, distance)
            whole = there & through if distance == 2 else there

            @pl.when(whole)
            def _(block=block):
                sent(side_out.at[block], side_send.at[block]).wait_send()

            if distance == 2:

                @pl.when(there & jnp.logical_not(through))
                def _(block=block, side=side):
                    rest = side_out.at[block, pl.ds(0, rows - short)]
                    sent(rest, side_send.at[block]).wait_send()
                    sent(side_out.at[block, pl.ds(0, short)], over_send.at[side]).wait_send()

            @pl.when(there)
            def _(block=block):
                sent(far_out.at[block], far_send.at[block]).wait_send()


def fused(tokens, norm_gain, w_gate, w_up, w_down, expert_ids, gate_weights):
    rows, width = tokens.shape
    top_count = expert_ids.shape[1]
    chips = lax.axis_size("ep") // CORES
    experts_all = chips * CORES
    lines = experts_all + -experts_all % 8
    hidden = w_gate.shape[2]
    out_width = width // 2
    last = chips - 1
    aggregates = max(last - 2, 1)
    lanes = rows + -rows % 128
    spans = 2 * (len(SPANS) - 1)
    anywhere = pl.BlockSpec(memory_space=pl.ANY)
    vmem, dma = pltpu.VMEM, pltpu.SemaphoreType.DMA
    return pl.pallas_call(
        functools.partial(fused_kernel, chips),
        out_shape=vmem((rows, out_width), jnp.bfloat16),
        in_specs=[anywhere] * 7,
        out_specs=pl.BlockSpec(memory_space=vmem),
        scratch_shapes=[
            vmem((rows, width), jnp.bfloat16),
            vmem((1, width), jnp.float32),
            vmem((top_count, rows), jnp.int32),
            vmem((top_count, rows), jnp.float32),
            vmem((chips, rows, width), jnp.bfloat16),
            vmem((chips, lines, lanes), jnp.float32),
            vmem((lanes, lines), jnp.float32),
            vmem((CORES, width, hidden), jnp.bfloat16),
            vmem((CORES, width, hidden), jnp.bfloat16),
            vmem((CORES * hidden, width), jnp.bfloat16),
            vmem((rows, CORES * hidden), jnp.bfloat16),
            vmem((rows, width), jnp.float32),
            vmem((chips, rows, out_width), jnp.float32),
            vmem((2, rows, width), jnp.bfloat16),
            vmem((2, rows, width), jnp.bfloat16),
            vmem((chips, rows, out_width), jnp.bfloat16),
            vmem((chips, rows, out_width), jnp.bfloat16),
            vmem((chips, rows, out_width), jnp.bfloat16),
            vmem((2, rows, out_width), jnp.bfloat16),
            vmem((2, aggregates, rows, out_width), jnp.bfloat16),
            vmem((2, rows, out_width), jnp.bfloat16),
            vmem((2, rows, out_width), jnp.bfloat16),
            dma((5,)),
            dma((3,)),
            dma((2, 3)),
            dma((chips + 1,)),
            dma((chips,)),
            dma((chips + 1,)),
            dma((chips, len(PIECES) - 1)),
            dma((1,)),
            dma((chips,)),
            dma((2,)),
            dma((2, spans)),
            dma((chips,)),
            dma((chips, spans)),
            dma((chips,)),
            dma((2, spans)),
            dma((2, aggregates, spans)),
            dma((2,)),
            dma((2, 2 * OVER)),
            dma((2,)),
            dma((2, 2 * NEAR)),
        ],
        compiler_params=pltpu.CompilerParams(collective_id=0, has_side_effects=True),
    )(tokens, norm_gain[None, :], expert_ids.T, gate_weights.T, w_gate, w_up, w_down)


def step(mesh, *arrays):
    tokens, norm_gain, w_gate, w_up, w_down, expert_ids, gate_weights = arrays
    ep_count, tp_count = mesh.shape["ep"], mesh.shape["tp"]
    rows, top_count = expert_ids.shape
    experts_all = ep_count * w_gate.shape[0]
    capacity = min(rows, rows * top_count * 4 // (3 * experts_all))
    dense = (
        w_gate.shape[0] == 1
        and tp_count == 2
        and ep_count % CORES == 0
        and ep_count > 3 * CORES
        and rows <= 2 * capacity
        and rows % (32 * PIECES[-1]) == 0
        and rows % (32 * SPANS[-1]) == 0
    )
    return fused(*arrays) if dense else body(*arrays)


def solution(mesh):
    placed = (
        P(("grp", "ep"), None),
        P(),
        P("ep", None, "tp"),
        P("ep", None, "tp"),
        P("ep", "tp", None),
        P(("grp", "ep"), None),
        P(("grp", "ep"), None),
    )
    return jax.shard_map(
        functools.partial(step, mesh), mesh=mesh, in_specs=placed, out_specs=P(("grp", "ep"), "tp"), check_vma=False
    )
```
